32 devices in a mesh: sp: 4 (over z), fs: 4 (over y, x), tp: 2 (over core).
Axes of the slice: x: 2, y: 2, z: 4, core: 2. Of those that a mesh axis runs over, the one named last changes fastest.
Arguments:
- tokens: bfloat16 [4, 1024, 2048], P('fs', ('sp', 'tp')), may hold values from -6 to 6
- norm_gain: float32 [2048], replicated, may hold values from 0.1 to 1.9
- w_query: bfloat16 [2048, 1024], P('fs', 'tp'), may hold values from -0.125 to 0.125
- w_key: bfloat16 [2048, 1024], P('fs', 'tp'), may hold values from -0.125 to 0.125
- w_value: bfloat16 [2048, 1024], P('fs', 'tp'), may hold values from -0.125 to 0.125
- w_conv_value: bfloat16 [2048, 1024], P('fs', 'tp'), may hold values from -2 to 2
- w_conv_gate: bfloat16 [2048, 1024], P('fs', 'tp'), may hold values from -0.125 to 0.125
- key_offset: bfloat16 [1024, 16], P('sp', 'tp'), may hold values from -16 to 2
- conv_kernel: float32 [31, 1024], P(None, 'tp'), may hold values from -3 to 3
- conv_gain: float32 [1024], P('tp'), may hold values from 0.1 to 1.9
- w_attn_out: bfloat16 [1024, 2048], P('tp', 'fs'), may hold values from -1 to 1
- w_conv_out: bfloat16 [1024, 2048], P('tp', 'fs'), may hold values from -0.1875 to 0.1875
Outputs:
- mixed: bfloat16 [4, 1024, 2048], P('fs', ('sp', 'tp'))
The draws below stay inside these ranges and needn't reach their ends.
All inputs are finite; a program needn't handle non-finite values.
Results may differ from the reference program's by a relative error of at most 0.0085.
Values may be sent and summed in bfloat16 or wider, within the bound.
A program may use at most 128 MiB of HBM per device.

```python
import math
import jax
import jax.numpy as jnp
from jax import lax

D = 2048
STICK_HEADS = 16
HD = 64
CC = 1024
KW = 31
TOK_DEV = 256
SBW = 1024
SEQUENCE_LENGTH = 1024
BATCH = 4
N_TP = 2


def draw_key_offset(key, part):
    divisions = jax.random.split(jax.random.fold_in(key, 11), 5)
    base_level = jax.random.uniform(divisions[0], (STICK_HEADS,), jnp.float32, -2.0, 5.0)
    block_shift = jax.random.uniform(divisions[1], (SEQUENCE_LENGTH // TOK_DEV, STICK_HEADS), jnp.float32, -0.8, 0.8)
    block_shift = jnp.repeat(block_shift, TOK_DEV, axis=0)
    roughness = jnp.clip(0.3 * jax.random.normal(divisions[2], (SEQUENCE_LENGTH, STICK_HEADS), jnp.float32), -1.0, 1.0)
    signal_height = base_level[None, :] - math.log(SEQUENCE_LENGTH) + block_shift + roughness
    spike_locations = jax.random.randint(divisions[3], (4,), 0, SEQUENCE_LENGTH)
    spike_flags = jnp.any(jnp.arange(SEQUENCE_LENGTH)[:, None] == spike_locations[None, :], axis=1)
    spike_magnitude = jax.random.uniform(divisions[4], (SEQUENCE_LENGTH, STICK_HEADS), jnp.float32, -1.2, 0.0)
    return jnp.where(spike_flags[:, None], spike_magnitude, signal_height).astype(jnp.bfloat16)


def draw_conv_kernel(key, part):
    divisions = jax.random.split(jax.random.fold_in(key, 23), 2)
    ramp = jnp.exp(jnp.linspace(math.log(0.4), math.log(2.0), CC)).astype(jnp.float32)
    entries = jnp.clip(jax.random.normal(divisions[0], (KW, CC), jnp.float32), -4.0, 4.0)
    common_tap = 0.1
    roughness = jax.random.uniform(divisions[1], (CC,), jnp.float32, 0.5, 1.5)
    return (entries * KW ** (-0.5) * ramp[None, :] * roughness[None, :] + common_tap).astype(jnp.float32)


def draw_w_conv_value(key, part):
    divisions = jax.random.split(jax.random.fold_in(key, 37), 3)
    levels = jnp.exp(jnp.linspace(math.log(0.3), math.log(3.0), CC)).astype(jnp.float32)
    noise = jnp.clip(jax.random.normal(divisions[0], (D, CC), jnp.float32), -4.0, 4.0)
    shared = jnp.clip(jax.random.normal(divisions[1], (D,), jnp.float32), -3.0, 3.0)
    roughness = jax.random.uniform(divisions[2], (CC,), jnp.float32, 0.7, 1.0)
    return ((noise + shared[:, None] * (levels * roughness)[None, :]) * D ** (-0.5)).astype(jnp.bfloat16)


def block_levels(stream_key, shape, pieces, smallest, top_value):
    def one(dim, blocks):
        heights = jax.random.uniform(jax.random.fold_in(jax.random.fold_in(stream_key, 6), dim), (blocks,), jnp.float32, smallest / len(pieces), top_value / len(pieces))
        return jnp.repeat(jnp.exp(heights), shape[dim] // blocks).reshape((-1,) + (1,) * (len(shape) - dim - 1))

    factor_of = one(*pieces[0])
    for cut in pieces[1:]:
        factor_of = factor_of * one(*cut)
    return factor_of


def bell_draw(own_key, extent, scale, limit, pieces=(), kind=jnp.bfloat16):
    gain = block_levels(own_key, extent, pieces, -0.22, 0.18) if pieces else 1.0
    values = jax.random.normal(own_key, extent, jnp.float32) * scale * gain
    return jnp.minimum(jnp.maximum(values, -limit), limit).astype(kind)


def setup_inputs(seed: int = 0) -> dict:
    streams_of = jax.random.split(jax.random.key(seed), 13)
    tokens = bell_draw(streams_of[0], (BATCH, SEQUENCE_LENGTH, D), 1.0, 6.0, ((0, 4), (1, 8)))
    norm_gain = jnp.clip(1.0 + 0.18 * jax.random.normal(streams_of[1], (D,), jnp.float32), 0.1, 1.9)
    w_query = bell_draw(streams_of[2], (D, SBW), D ** -0.5, 0.125, ((0, 4), (1, 2)))
    w_key = bell_draw(streams_of[3], (D, SBW), D ** -0.5, 0.125, ((0, 4), (1, 2)))
    w_value = bell_draw(streams_of[4], (D, SBW), D ** -0.5, 0.125, ((0, 4), (1, 2)))
    w_conv_value = draw_w_conv_value(jax.random.fold_in(streams_of[12], 71), 0)
    w_conv_gate = bell_draw(streams_of[6], (D, CC), D ** -0.5, 0.125, ((0, 4), (1, 2)))
    key_offset = draw_key_offset(jax.random.fold_in(streams_of[12], 71), 0)
    conv_kernel = draw_conv_kernel(jax.random.fold_in(streams_of[12], 71), 0)
    conv_gain = jnp.clip(1.0 + 0.18 * jax.random.normal(streams_of[9], (CC,), jnp.float32), 0.1, 1.9)
    w_attn_out = bell_draw(streams_of[10], (SBW, D), (SBW // 32) ** -0.5, 1.0, ((0, 2), (1, 4)))
    w_conv_out = bell_draw(streams_of[11], (CC, D), CC ** -0.5, 0.1875, ((0, 2), (1, 4)))
    return {"tokens": tokens, "norm_gain": norm_gain, "w_query": w_query, "w_key": w_key, "w_value": w_value, "w_conv_value": w_conv_value, "w_conv_gate": w_conv_gate, "key_offset": key_offset, "conv_kernel": conv_kernel, "conv_gain": conv_gain, "w_attn_out": w_attn_out, "w_conv_out": w_conv_out}


def reference(tokens, norm_gain, w_query, w_key, w_value, w_conv_value, w_conv_gate, key_offset, conv_kernel, conv_gain, w_attn_out, w_conv_out):
    floats = tokens.astype(jnp.float32)
    normed = (floats * lax.rsqrt(lax.optimization_barrier(jnp.mean(floats * floats, axis=2, keepdims=True)) + 1e-06) * norm_gain).astype(jnp.bfloat16)
    flat_rows = normed.reshape(BATCH * SEQUENCE_LENGTH, D)

    def project(weight):
        return jnp.dot(flat_rows, weight, preferred_element_type=jnp.float32).astype(jnp.bfloat16).reshape(BATCH, SEQUENCE_LENGTH, weight.shape[1])
    queries = project(w_query)
    key_rows = project(w_key)
    value_rows = project(w_value)
    conv_value = project(w_conv_value)
    conv_gate = project(w_conv_gate)
    offsets = jnp.transpose(key_offset.astype(jnp.float32))
    key_pos = jnp.arange(SEQUENCE_LENGTH, dtype=jnp.int32)
    blocks = SEQUENCE_LENGTH // TOK_DEV
    score_scale = HD ** (-0.5)

    def one_block(index):
        batch_index = index // blocks
        first_row = index % blocks * TOK_DEV
        seq_query = lax.dynamic_index_in_dim(queries, batch_index, 0, keepdims=False)
        query_block = lax.dynamic_slice_in_dim(seq_query, first_row, TOK_DEV, 0).reshape(TOK_DEV, STICK_HEADS, HD)
        seq_keys = lax.dynamic_index_in_dim(key_rows, batch_index, 0, keepdims=False).reshape(SEQUENCE_LENGTH, STICK_HEADS, HD)
        seq_values = lax.dynamic_index_in_dim(value_rows, batch_index, 0, keepdims=False).reshape(SEQUENCE_LENGTH, STICK_HEADS, HD)
        logits = jnp.einsum('qhd,khd->hqk', query_block.astype(jnp.float32), seq_keys.astype(jnp.float32)) * score_scale
        logits = logits + offsets[:, None, :]
        query_pos = first_row + jnp.arange(TOK_DEV, dtype=jnp.int32)
        allowed = key_pos[None, :] < query_pos[:, None]
        log_keep = jnp.where(allowed[None], jax.nn.log_sigmoid(-logits), 0.0)
        between = lax.cumsum(log_keep, axis=2, reverse=True) - log_keep
        weights = jnp.where(allowed[None], jnp.exp(jax.nn.log_sigmoid(logits) + between), 0.0).astype(jnp.bfloat16)
        result = jnp.einsum('hqk,khd->qhd', weights.astype(jnp.float32), seq_values.astype(jnp.float32))
        return result.reshape(TOK_DEV, SBW).astype(jnp.bfloat16)
    attn_heads = lax.map(one_block, jnp.arange(BATCH * blocks, dtype=jnp.int32)).reshape(BATCH, SEQUENCE_LENGTH, SBW)
    gated_input = (conv_value.astype(jnp.float32) * jax.nn.sigmoid(conv_gate.astype(jnp.float32))).astype(jnp.bfloat16)
    padded = jnp.pad(gated_input, ((0, 0), (KW - 1, 0), (0, 0))).astype(jnp.float32)
    conv_sum = jnp.zeros((BATCH, SEQUENCE_LENGTH, CC), jnp.float32)
    for tap_index in range(KW):
        conv_sum = conv_sum + conv_kernel[tap_index] * padded[:, tap_index:tap_index + SEQUENCE_LENGTH]
    mean_val = lax.optimization_barrier(jnp.mean(conv_sum, axis=2, keepdims=True))
    centred = conv_sum - mean_val
    spread = lax.optimization_barrier(jnp.mean(centred * centred, axis=2, keepdims=True))
    conv_hidden = jax.nn.silu(centred * lax.rsqrt(spread + 1e-06) * conv_gain).astype(jnp.bfloat16)
    head_cols = SBW // N_TP
    chan_cols = CC // N_TP
    attn_flat = attn_heads.reshape(BATCH * SEQUENCE_LENGTH, SBW)
    conv_flat = conv_hidden.reshape(BATCH * SEQUENCE_LENGTH, CC)
    total = jnp.zeros((BATCH * SEQUENCE_LENGTH, D), jnp.float32)
    for group in range(N_TP):
        partial_value = jnp.dot(attn_flat[:, group * head_cols:(group + 1) * head_cols], w_attn_out[group * head_cols:(group + 1) * head_cols], preferred_element_type=jnp.float32)
        partial_value = partial_value + jnp.dot(conv_flat[:, group * chan_cols:(group + 1) * chan_cols], w_conv_out[group * chan_cols:(group + 1) * chan_cols], preferred_element_type=jnp.float32)
        total = total + lax.optimization_barrier(partial_value.astype(jnp.bfloat16)).astype(jnp.float32)
    return total.astype(jnp.bfloat16).reshape(BATCH, SEQUENCE_LENGTH, D)
```

```python
import functools

import jax
import jax.numpy as jnp
from jax import lax
from jax.experimental import pallas as pl
from jax.experimental.pallas import tpu as pltpu
from jax.sharding import PartitionSpec as P

HD = 64
CC = 1024
MESH = pl.DeviceIdType.MESH
F32 = jnp.float32
BF16 = jnp.bfloat16


def remote(src, dst, send, recv, **where):
    return pltpu.make_async_remote_copy(
        src_ref=src, dst_ref=dst, send_sem=send, recv_sem=recv, device_id=where, device_id_type=MESH
    )


def greet(peers):
    barrier = pltpu.get_barrier_semaphore()
    for where in peers:
        pl.semaphore_signal(barrier, inc=1, device_id=where, device_id_type=MESH)
    pl.semaphore_wait(barrier, len(peers))


def plane(fs):
    y = (fs + 2) % 4
    return fs + 1 - 2 * (fs % 2), y, y + 1 - 2 * (y % 2)


ANY = pl.BlockSpec(memory_space=pl.ANY)


def aligned(start, size):
    return pl.ds(pl.multiple_of(start, size), size)


def layer_body(n_sp, n_tp, width, heads, taps, blk, *refs):
    tok_in, gain_in, w_ins, off_in, ck_in, cgain_in, wa_in, wc_in = refs[0], refs[1], refs[2:7], *refs[7:12]
    own_out, got_out = refs[12:14]
    tok, w, wout, off_raw, off, ck, gain, cgain = refs[14:22]
    queries, keys, values, gated, carry, running = refs[22:28]
    attn_out, conv_out, stat_out, x_all, stat_all, hidden, part = refs[28:35]
    ld, up_s, up_r, dn_s, dn_r, par_s, par_r, w_s, w_r, off_s, off_r = refs[35:46]
    o_s, o_r, x_s, x_r, st_s, st_r, part_s, part_r, keep_s = refs[46:]
    rows = tok_in.shape[0]
    sub = rows // 2
    depth = w_ins[0].shape[0]
    half = depth // 2
    o_rows, o_cols = wa_in.shape
    quarter = o_rows // 2
    z, fs, tp = lax.axis_index("sp"), lax.axis_index("fs"), lax.axis_index("tp")
    xn, yn, dg = plane(fs)
    n = n_sp * n_tp
    me = z * n_tp + tp

    own_rows = aligned((z * n_tp + tp) * rows, rows)
    loads = [pltpu.make_async_copy(tok_in, tok.at[own_rows], ld.at[0])]
    loads += [
        pltpu.make_async_copy(
            ref.at[:, aligned(z * width, width)],
            w.at[aligned(fs * depth, depth), pl.ds(k * width, width)],
            ld.at[1 + k],
        )
        for k, ref in enumerate(w_ins)
    ]
    loads += [
        pltpu.make_async_copy(wa_in, wout.at[fs, pl.ds(0, o_rows)], ld.at[6]),
        pltpu.make_async_copy(wc_in, wout.at[fs, pl.ds(o_rows, o_rows)], ld.at[7]),
        pltpu.make_async_copy(off_in, off_raw.at[z], ld.at[8]),
        pltpu.make_async_copy(ck_in.at[:, aligned(z * width, width)], ck, ld.at[9]),
        pltpu.make_async_copy(gain_in, gain, ld.at[10]),
        pltpu.make_async_copy(cgain_in, cgain, ld.at[11]),
    ]
    for copy in loads:
        copy.start()
    greet(
        [{"sp": (me + d) % n // n_tp, "tp": (me + d) % n % n_tp} for d in range(1, n)]
        + [{"fs": xn}, {"fs": yn}]
    )

    def piece_rows(block, core, p):
        return tok.at[aligned((block * n_tp + core) * rows + p * sub, sub)]

    def lift(block, dist, p):
        ref = piece_rows(block, tp, p)
        return remote(ref, ref, up_s.at[dist - 1, p], up_r.at[dist - 1, p], sp=(z + 1) % n_sp)

    def sink(block, dist, p):
        ref = piece_rows(block, tp, p)
        return remote(ref, ref, dn_s.at[dist - 1, p], dn_r.at[dist - 1, p], sp=(z + n_sp - 1) % n_sp)

    def across(block, p):
        ref = piece_rows(block, tp, p)
        return remote(ref, ref, par_s.at[block, p], par_r.at[block, p], tp=1 - tp)

    def from_partner(block, p):
        ref = piece_rows(block, 1 - tp, p)
        return remote(ref, ref, par_s.at[block, p], par_r.at[block, p], tp=1 - tp)

    def w_part(owner, h):
        return w.at[aligned(owner * depth + h * half, half)]

    def send_w(owner, h, sem, to):
        return remote(w_part(owner, h), w_part(owner, h), w_s.at[sem], w_r.at[sem], fs=to)

    def send_o(owner, k, sem, to):
        ref = wout.at[owner, pl.ds(k * quarter, quarter)]
        return remote(ref, ref, o_s.at[sem], o_r.at[sem], fs=to)

    loads[0].wait()
    for p in range(2):
        @pl.when(z < n_sp - 1)
        def _():
            lift(z, 1, p).start()

        @pl.when(z > 0)
        def _():
            sink(z, 1, p).start()

    for k in range(5):
        loads[1 + k].wait()
    w_first = [send_w(fs, 0, 0, xn), send_w(fs, 1, 1, yn), send_w(fs, 1, 2, xn), send_w(fs, 0, 3, yn)]
    for copy in w_first:
        copy.start()
    for p in range(2):
        across(z, p).start()
    loads[8].wait()
    offs = [
        remote(off_raw.at[z], off_raw.at[z], off_s.at[d - 1], off_r.at[d - 1], sp=(z + d) % n_sp)
        for d in range(1, n_sp)
    ]
    for copy in offs:
        copy.start()
    w_relay = [send_w(xn, 0, 4, yn), send_w(yn, 1, 5, xn)]
    w_here = [(0, xn, 0), (1, yn, 1), (2, xn, 1), (3, yn, 0), (4, dg, 0), (5, dg, 1)]
    o_first = []
    for a, b in ((0, 2), (1, 3), (2, 0), (3, 1)):
        o_first += [send_o(fs, a, a, xn), send_o(fs, b, 4 + b, yn)]
    o_relay = [send_o(xn, 0, 8, yn), send_o(yn, 2, 10, xn), send_o(xn, 1, 9, yn), send_o(yn, 3, 11, xn)]

    def token_hop(dist, p):
        @pl.when(z >= dist)
        def _():
            block = (z - dist + n_sp) % n_sp
            lift(block, dist, p).wait_recv()
            if dist < n_sp - 1:
                @pl.when(z < n_sp - 1)
                def _():
                    lift(block, dist + 1, p).start()
            across(block, p).start()

        @pl.when(z + dist < n_sp)
        def _():
            block = (z + dist) % n_sp
            sink(block, dist, p).wait_recv()
            if dist < n_sp - 1:
                @pl.when(z > 0)
                def _():
                    sink(block, dist + 1, p).start()
            across(block, p).start()

    def relay_w():
        for s, owner, h in w_here[:2]:
            send_w(owner, h, s, xn).wait_recv()
            w_relay[s].start()
        for copy in loads[6:8]:
            copy.wait()
        for copy in o_first:
            copy.start()

    gated[pl.ds(0, 32), :] = jnp.zeros((32, width), F32)
    for dist in range(1, n_sp - 1):
        token_hop(dist, 0)
        if dist == 1:
            relay_w()
        token_hop(dist, 1)
    if n_sp == 2:
        relay_w()
    for copy in loads[9:]:
        copy.wait()
    for s, owner, h in w_here[2:]:
        send_w(owner, h, s, xn).wait_recv()
    for copy in offs:
        copy.wait()
    off[...] = off_raw[...].astype(F32)

    lane = lax.broadcasted_iota(jnp.int32, (rows, width), 1)

    def project(tile, _):
        at = aligned(tile * rows, rows)
        x = tok[at, :].astype(F32)
        normed = (x * lax.rsqrt(jnp.mean(x * x, axis=1, keepdims=True) + 1e-06) * gain[...]).astype(BF16)
        out = jnp.dot(normed, w[...], preferred_element_type=F32).astype(BF16)
        q = out[:, :width].astype(F32) * HD ** (-0.5)
        for h in range(heads):
            mine = jnp.logical_and(lane >= h * HD, lane < (h + 1) * HD)
            queries[h, at, :] = jnp.where(mine, q, 0.0).astype(BF16)
        keys[at, :] = out[:, width : 2 * width]
        values[at, :] = out[:, 2 * width : 3 * width]
        value = out[:, 3 * width : 4 * width].astype(F32)
        gate = out[:, 4 * width :].astype(F32)
        gated[pl.ds(pl.multiple_of(tile * rows + 32, 32), rows), :] = (
            (value * jax.nn.sigmoid(gate)).astype(BF16).astype(F32)
        )
        return 0

    ones = jnp.full((8, width), 1.0 / width, F32)
    top = lax.broadcasted_iota(jnp.int32, (8, rows), 0) == 0

    def average(x):
        return lax.dot_general(
            ones, x, (((1,), (1,)), ((), ())), precision=lax.Precision.HIGHEST, preferred_element_type=F32
        )

    def convolve(tile, _):
        base = pl.multiple_of(tile * rows, rows)
        window = gated[pl.ds(base, rows + 32), :]
        total = jnp.zeros((rows, width), F32)
        for tap in range(taps):
            lo = 32 - (taps - 1) + tap
            total = total + ck[tap : tap + 1, :] * window[lo : lo + rows]
        local = total - jnp.mean(total, axis=1, keepdims=True)
        conv_out[pl.ds(base, rows), :] = local.astype(BF16)
        stat_out[tile] = jnp.where(top, average(total), average(local * local))
        return 0

    def block_rows(i):
        return aligned(i * blk, blk)

    def ship(k, source, block):
        at = source.at[block_rows(block)]

        @pl.when(block == z)
        def _():
            x_all[k * n_sp + z] = at[...]

        @pl.when(block != z)
        def _():
            remote(at, x_all.at[k * n_sp + z], x_s.at[k, block], x_r.at[k, z], sp=block).start()

    tiles = blk // rows

    def ship_stat(block):
        at = stat_out.at[pl.ds(block * tiles, tiles)]

        @pl.when(block == z)
        def _():
            stat_all[z] = at[...]

        @pl.when(block != z)
        def _():
            remote(at, stat_all.at[z], st_s.at[0, block], st_r.at[z], sp=block).start()

        remote(at, stat_all.at[n_sp + z], st_s.at[1, block], st_r.at[n_sp + z], sp=block, tp=1 - tp).start()

    row = lax.broadcasted_iota(jnp.int32, (blk, blk), 0)
    col = lax.broadcasted_iota(jnp.int32, (blk, blk), 1)
    wide = lax.broadcasted_iota(jnp.int32, (blk, width), 1)

    def attend(i, j, diagonal):
        k = keys[block_rows(j), :]
        v = values[block_rows(j), :]
        after = jnp.where(row >= col, 1.0, 0.0).astype(BF16)
        for h in range(heads):
            q = queries[h, block_rows(i), :]
            s = lax.dot_general(q, k, (((1,), (1,)), ((), ())), preferred_element_type=F32)
            s = s + off[j, pl.ds(z * heads + h, 1), :]
            keep = jnp.minimum(-s, 0.0) - jnp.log(1.0 + jnp.exp(-jnp.abs(s)))
            if diagonal:
                keep = jnp.where(col < row, keep, 0.0)
            high = keep.astype(BF16)
            low = (keep - high.astype(F32)).astype(BF16)
            suffix = jnp.dot(high, after, preferred_element_type=F32)
            suffix = suffix + jnp.dot(low, after, preferred_element_type=F32)
            if diagonal:
                weights = jnp.where(col < row, jnp.exp(s + suffix), 0.0)
                carry[i, h] = suffix[:, :1]
                running[i, h] = jnp.dot(weights.astype(BF16), v, preferred_element_type=F32)
            else:
                before = carry[i, h]
                weights = jnp.exp(s + suffix + before)
                carry[i, h] = before + suffix[:, :1]
                running[i, h] += jnp.dot(weights.astype(BF16), v, preferred_element_type=F32)

        @pl.when(j == 0)
        def _():
            merged = running[i, 0]
            for h in range(1, heads):
                merged = jnp.where(wide >= h * HD, running[i, h], merged)
            attn_out[block_rows(i), :] = merged.astype(BF16)
            ship(0, attn_out, i)

    pairs = jnp.minimum(z, n_sp - 1 - z)

    def step(s, _):
        dist = (s + 1) // 2
        inner = jnp.where(s % 2 == 1, z - dist, z + dist)
        outer = jnp.where(z == pairs, s, n_sp - 1 - s)
        block = jnp.where(s <= 2 * pairs, inner, outer)
        rising = block > z

        @pl.when(jnp.logical_and(s == n_sp - 1, pairs == 0))
        def _():
            for p in range(2):
                token_hop(n_sp - 1, p)

        for p in range(2):
            from_partner(block, p).wait_recv()
        lax.fori_loop(block * n_tp, block * n_tp + n_tp, project, 0)

        def conv_block(u, _):
            target = jnp.where(rising, block, jnp.where(jnp.logical_and(u == 0, s > 0), block + 1, 0))
            lax.fori_loop(target * tiles, target * tiles + tiles, convolve, 0)
            ship(1, conv_out, target)
            ship_stat(target)
            return 0

        falling_count = jnp.where(s > 0, 1, 0) + jnp.where(block == 0, 1, 0)
        lax.fori_loop(0, jnp.where(rising, 1, falling_count), conv_block, 0)
        attend(block, block, True)

        def further(t, _):
            attend(jnp.where(rising, block, block + t), jnp.where(rising, block - t, block), False)
            return 0

        lax.fori_loop(1, s + 1, further, 0)
        return 0

    lax.fori_loop(0, n_sp, step, 0)
    for k in (0, 1):
        send_o(xn, k, k, xn).wait_recv()
        send_o(yn, 2 + k, 6 + k, xn).wait_recv()
    for copy in o_relay:
        copy.start()

    others = [(z + d) % n_sp for d in range(1, n_sp)]

    def stat_from(slot):
        return remote(stat_all.at[slot], stat_all.at[slot], st_s.at[0, z], st_r.at[slot], tp=1 - tp)

    def x_from(k, source):
        ref = x_all.at[k * n_sp + source]
        return remote(ref, ref, x_s.at[k, z], x_r.at[k, source], tp=1 - tp)

    for source in others:
        stat_from(source).wait_recv()
    for source in range(n_sp):
        stat_from(n_sp + source).wait_recv()
    for source in others:
        x_from(1, source).wait_recv()
    square = (lax.broadcasted_iota(jnp.int32, (rows, rows), 0)
              == lax.broadcasted_iota(jnp.int32, (rows, rows), 1)).astype(F32)
    kind = lax.broadcasted_iota(jnp.int32, (rows, n * 8), 1) % 8
    for t in range(tiles):
        flat = stat_all[:, t].reshape(n * 8, rows)
        stats = lax.dot_general(
            square, flat, (((1,), (1,)), ((), ())), precision=lax.Precision.HIGHEST, preferred_element_type=F32
        )
        mean = jnp.sum(jnp.where(kind == 0, stats, 0.0), axis=1, keepdims=True) / n
        off_mean = stats - mean
        spread = jnp.where(kind == 0, off_mean * off_mean, jnp.where(kind == 1, stats, 0.0))
        scale = lax.rsqrt(jnp.sum(spread, axis=1, keepdims=True) / n + 1e-06)
        at = pl.ds(t * rows, rows)
        for g in range(n_sp):
            x = x_all[n_sp + g, at, :].astype(F32) + off_mean[:, 8 * g : 8 * g + 1]
            y = x * scale * cgain[:, g * width : (g + 1) * width]
            hidden[at, (n_sp + g) * width : (n_sp + g + 1) * width] = (y * jax.nn.sigmoid(y)).astype(BF16)
    for source in others:
        x_from(0, source).wait_recv()
    for g in range(n_sp):
        hidden[:, g * width : (g + 1) * width] = x_all[g]

    sent = []
    for index, owner in enumerate((fs, xn, yn, dg)):
        if owner is xn:
            for k in (2, 3):
                send_o(xn, k, k, xn).wait_recv()
        elif owner is yn:
            for k in (0, 1):
                send_o(yn, k, 4 + k, xn).wait_recv()
        elif owner is dg:
            for k in range(4):
                send_o(dg, k, 8 + k, xn).wait_recv()
        part[index] = jnp.dot(hidden[...], wout[owner], preferred_element_type=F32).astype(BF16)
        cols = aligned(owner * o_cols, o_cols)
        keep = pltpu.make_async_copy(
            part.at[index, aligned(tp * rows, rows)], own_out.at[:, cols], keep_s.at[index]
        )
        give = remote(
            part.at[index, aligned((1 - tp) * rows, rows)], got_out.at[:, cols],
            part_s.at[index], part_r.at[index], tp=1 - tp,
        )
        give.start()
        keep.start()
        sent += [keep, give]

    for copy in w_first + w_relay + o_first + o_relay:
        copy.wait_send()
    for p in range(2):
        for dist in range(1, n_sp):
            @pl.when(jnp.logical_and(z < n_sp - 1, z >= dist - 1))
            def _():
                lift(z, dist, p).wait_send()

            @pl.when(jnp.logical_and(z > 0, z + dist - 1 < n_sp))
            def _():
                sink(z, dist, p).wait_send()

        for block in range(n_sp):
            across(block, p).wait_send()
    for block in others:
        for k in range(2):
            remote(x_all.at[k], x_all.at[k], x_s.at[k, block], x_r.at[k, z], tp=1 - tp).wait_send()
        remote(stat_all.at[z], stat_all.at[z], st_s.at[0, block], st_r.at[z], tp=1 - tp).wait_send()
    for block in range(n_sp):
        remote(stat_all.at[z], stat_all.at[z], st_s.at[1, block], st_r.at[z], tp=1 - tp).wait_send()
    for copy in sent:
        copy.wait()


def layer_call(n_sp, n_fs, n_tp, width, heads, blk, tokens, gain, w_ins, off, ck, cgain, wa, wc):
    rows, features = tokens.shape
    depth = w_ins[0].shape[0]
    o_rows, o_cols = wa.shape
    length, n = rows * n_sp * n_tp, n_sp * n_tp
    tiles = blk // rows
    dma = pltpu.SemaphoreType.DMA
    vmem = pltpu.VMEM
    result = jax.ShapeDtypeStruct((rows, n_fs * o_cols), BF16)
    return pl.pallas_call(
        functools.partial(layer_body, n_sp, n_tp, width, heads, ck.shape[0], blk),
        out_shape=[result, result],
        in_specs=[ANY] * 12,
        out_specs=[ANY] * 2,
        scratch_shapes=[
            vmem((length, features), BF16),
            vmem((n_fs * depth, 5 * width), BF16),
            vmem((n_fs, 2 * o_rows, o_cols), BF16),
            vmem((n_sp,) + off.shape, BF16),
            vmem((n_sp,) + off.shape, F32),
            vmem((ck.shape[0], width), F32),
            vmem(gain.shape, F32),
            vmem(cgain.shape, F32),
            vmem((heads, length, width), BF16),
            vmem((length, width), BF16),
            vmem((length, width), BF16),
            vmem((length + 32, width), F32),
            vmem((n_sp, heads, blk, 1), F32),
            vmem((n_sp, heads, blk, width), F32),
            vmem((length, width), BF16),
            vmem((length, width), BF16),
            vmem((length // rows, 8, rows), F32),
            vmem((2 * n_sp, blk, width), BF16),
            vmem((n, tiles, 8, rows), F32),
            vmem((blk, 2 * n_sp * width), BF16),
            vmem((n_fs, blk, o_cols), BF16),
            dma((12,)),
            dma((n_sp - 1, 2)), dma((n_sp - 1, 2)), dma((n_sp - 1, 2)), dma((n_sp - 1, 2)),
            dma((n_sp, 2)), dma((n_sp, 2)),
            dma((6,)), dma((6,)),
            dma((n_sp - 1,)), dma((n_sp - 1,)),
            dma((12,)), dma((12,)),
            dma((2, n_sp)), dma((2, n_sp)),
            dma((2, n_sp)), dma((n,)),
            dma((n_fs,)), dma((n_fs,)), dma((n_fs,)),
        ],
        compiler_params=pltpu.CompilerParams(collective_id=0, has_side_effects=True),
        name="layer",
    )(tokens, gain, *w_ins, off, ck, cgain, wa, wc)


def spread_shards(
    tokens,
    norm_gain,
    w_query,
    w_key,
    w_value,
    w_conv_value,
    w_conv_gate,
    key_offset,
    conv_kernel,
    conv_gain,
    w_attn_out,
    w_conv_out,
):
    n_sp, n_fs, n_tp = (lax.axis_size(a) for a in ("sp", "fs", "tp"))
    width = w_query.shape[1] // n_sp
    own, got = layer_call(
        n_sp, n_fs, n_tp, width, width // HD, key_offset.shape[0], tokens[0], norm_gain[None],
        (w_query, w_key, w_value, w_conv_value, w_conv_gate), jnp.transpose(key_offset),
        conv_kernel, conv_gain[None], w_attn_out, w_conv_out,
    )
    return (own.astype(F32) + got.astype(F32)).astype(BF16)[None]


def shifted(block, axis, distance):
    devices = range(lax.axis_size(axis))
    route = [(i - distance, i) for i in devices if i - distance in devices]
    return lax.ppermute(block, axis, route)


def piece_terms(queries, key_rows, value_rows, offsets, carry_log, allowed):
    head_size = queries.shape[2]
    logits = jnp.einsum(
        "qhd,khd->hqk", queries, key_rows, preferred_element_type=jnp.float32
    ) * head_size ** (-0.5)
    logits = logits + jnp.transpose(offsets.astype(jnp.float32))[:, None, :]
    log_keep = jax.nn.log_sigmoid(-logits)
    if allowed is not None:
        log_keep = jnp.where(allowed[None], log_keep, 0.0)
    between = lax.cumsum(log_keep, axis=2, reverse=True) - log_keep
    weights = jnp.exp(jax.nn.log_sigmoid(logits) + between + carry_log[:, :, None])
    if allowed is not None:
        weights = jnp.where(allowed[None], weights, 0.0)
    result = jnp.einsum(
        "hqk,khd->qhd", weights.astype(jnp.bfloat16), value_rows, preferred_element_type=jnp.float32
    )
    return (result, carry_log + jnp.sum(log_keep, axis=2))


def shards(
    tokens,
    norm_gain,
    w_query,
    w_key,
    w_value,
    w_conv_value,
    w_conv_gate,
    key_offset,
    conv_kernel,
    conv_gain,
    w_attn_out,
    w_conv_out,
):
    gathered = (
        lax.all_gather(w_query, "fs", axis=0, tiled=True),
        lax.all_gather(w_key, "fs", axis=0, tiled=True),
        lax.all_gather(w_value, "fs", axis=0, tiled=True),
        lax.all_gather(w_conv_value, "fs", axis=0, tiled=True),
        lax.all_gather(w_conv_gate, "fs", axis=0, tiled=True),
    )
    floats = lax.all_gather(tokens[0], "tp", axis=0, tiled=True).astype(jnp.float32)
    normed = (
        floats * lax.rsqrt(jnp.mean(floats * floats, axis=1, keepdims=True) + 1e-06) * norm_gain
    ).astype(jnp.bfloat16)
    projected = jnp.concatenate(
        [
            jnp.dot(normed, weight, preferred_element_type=jnp.float32).astype(jnp.bfloat16)
            for weight in gathered
        ],
        axis=1,
    )
    head_cols = w_query.shape[1]
    channels = w_conv_value.shape[1]
    block_len = projected.shape[0]
    local_heads = head_cols // HD
    queries = projected[:, :head_cols].reshape(block_len, local_heads, HD)
    key_flat = projected[:, head_cols : 2 * head_cols]
    value_flat = projected[:, 2 * head_cols : 3 * head_cols]
    conv_value = projected[:, 3 * head_cols : 3 * head_cols + channels]
    conv_gate = projected[:, 3 * head_cols + channels :]
    position = lax.axis_index("sp")
    positions = jnp.arange(block_len, dtype=jnp.int32)
    causal = positions[None, :] < positions[:, None]
    start_log = jnp.zeros((local_heads, block_len), jnp.float32)
    totals, carry_log = piece_terms(
        queries,
        key_flat.reshape(block_len, local_heads, HD),
        value_flat.reshape(block_len, local_heads, HD),
        key_offset,
        start_log,
        causal,
    )

    def visit(hop_count, carried):
        running, running_log, moving = carried
        moving = shifted((moving[0], moving[1], moving[2]), "sp", 1)
        result, next_log = piece_terms(
            queries,
            moving[0].reshape(block_len, local_heads, HD),
            moving[1].reshape(block_len, local_heads, HD),
            moving[2],
            running_log,
            None,
        )
        active = position >= hop_count
        running = jnp.where(active, running + result, running)
        running_log = jnp.where(active, next_log, running_log)
        return (running, running_log, moving)

    totals, carry_log, leftover = lax.fori_loop(
        1, lax.axis_size("sp"), visit, (totals, carry_log, (key_flat, value_flat, key_offset))
    )
    attn_heads = totals.reshape(block_len, head_cols).astype(jnp.bfloat16)
    gated_input = (
        conv_value.astype(jnp.float32) * jax.nn.sigmoid(conv_gate.astype(jnp.float32))
    ).astype(jnp.bfloat16)
    kernel_len = conv_kernel.shape[0]
    edge_rows = shifted(gated_input[block_len - (kernel_len - 1) :], "sp", 1)
    extended = jnp.concatenate([edge_rows, gated_input], axis=0).astype(jnp.float32)
    conv_sum = jnp.zeros((block_len, channels), jnp.float32)
    for tap_index in range(kernel_len):
        conv_sum = conv_sum + conv_kernel[tap_index] * extended[tap_index : tap_index + block_len]
    channel_total = lax.psum(jnp.sum(conv_sum, axis=1), "tp")
    centred = conv_sum - (channel_total / CC)[:, None]
    spread = lax.psum(jnp.sum(centred * centred, axis=1), "tp") / CC
    conv_hidden = jax.nn.silu(centred * lax.rsqrt(spread + 1e-06)[:, None] * conv_gain).astype(
        jnp.bfloat16
    )
    attn_weight, conv_weight = (
        lax.all_gather(w_attn_out, "fs", axis=1, tiled=True),
        lax.all_gather(w_conv_out, "fs", axis=1, tiled=True),
    )
    partial_value = jnp.dot(attn_heads, attn_weight, preferred_element_type=jnp.float32)
    partial_value = partial_value + jnp.dot(
        conv_hidden, conv_weight, preferred_element_type=jnp.float32
    )
    mixed = lax.psum_scatter(
        lax.optimization_barrier(partial_value.astype(jnp.bfloat16))
        .astype(jnp.float32)
        .astype(jnp.bfloat16),
        "tp",
        scatter_dimension=0,
        tiled=True,
    )
    return mixed[None]


def solution(mesh):
    placed = (
        P("fs", ("sp", "tp"), None),
        P(),
        P("fs", "tp"),
        P("fs", "tp"),
        P("fs", "tp"),
        P("fs", "tp"),
        P("fs", "tp"),
        P("sp", "tp"),
        P(None, "tp"),
        P("tp"),
        P("tp", "fs"),
        P("tp", "fs"),
    )

    def fits(tokens, norm_gain, w_query, *rest):
        n_sp, n_fs, n_tp = mesh.shape["sp"], mesh.shape["fs"], mesh.shape["tp"]
        cols = w_query.shape[1] // n_tp
        return n_fs == 4 and n_tp == 2 and n_sp > 1 and rest[5].shape[0] <= 33 and cols % (128 * n_sp) == 0 and rest[2].shape[1] == w_query.shape[1] and (
            tokens.shape[1] % (128 * n_sp * n_tp) == 0
        )

    def program(*args):
        body = spread_shards if fits(*args) else shards
        return mapped(body)(*args)

    def mapped(body):
        return jax.shard_map(
            body, mesh=mesh, in_specs=placed, out_specs=P("fs", ("sp", "tp"), None), check_vma=False
        )

    return program
```

```python
import functools

import jax
import jax.numpy as jnp
from jax import lax
from jax.experimental import pallas as pl
from jax.experimental.pallas import tpu as pltpu
from jax.sharding import PartitionSpec as P

HD = 64
CC = 1024
MESH = pl.DeviceIdType.MESH
F32 = jnp.float32
BF16 = jnp.bfloat16


def remote(src, dst, send, recv, **where):
    return pltpu.make_async_remote_copy(
        src_ref=src, dst_ref=dst, send_sem=send, recv_sem=recv, device_id=where, device_id_type=MESH
    )


def greet(peers):
    barrier = pltpu.get_barrier_semaphore()
    for where in peers:
        pl.semaphore_signal(barrier, inc=1, device_id=where, device_id_type=MESH)
    pl.semaphore_wait(barrier, len(peers))


def plane(fs):
    y = (fs + 2) % 4
    return fs + 1 - 2 * (fs % 2), y, y + 1 - 2 * (y % 2)


ANY = pl.BlockSpec(memory_space=pl.ANY)


def aligned(start, size):
    return pl.ds(pl.multiple_of(start, size), size)


def layer_body(n_sp, n_tp, width, heads, taps, blk, *refs):
    tok_in, gain_in, w_ins, off_in, ck_in, cgain_in, wa_in, wc_in = refs[0], refs[1], refs[2:7], *refs[7:12]
    own_out, got_out = refs[12:14]
    tok, w, wout, off_raw, off, ck, gain, cgain = refs[14:22]
    queries, keys, values, gated, carry, running = refs[22:28]
    attn_out, conv_out, stat_out, x_all, stat_all, hidden, part = refs[28:35]
    ld, up_s, up_r, dn_s, dn_r, par_s, par_r, w_s, w_r, off_s, off_r = refs[35:46]
    o_s, o_r, x_s, x_r, st_s, st_r, part_s, part_r, keep_s = refs[46:]
    rows = tok_in.shape[0]
    sub = rows // 2
    depth = w_ins[0].shape[0]
    half = depth // 2
    o_rows, o_cols = wa_in.shape
    quarter = o_rows // 2
    z, fs, tp = lax.axis_index("sp"), lax.axis_index("fs"), lax.axis_index("tp")
    xn, yn, dg = plane(fs)
    n = n_sp * n_tp
    me = z * n_tp + tp

    own_rows = aligned((z * n_tp + tp) * rows, rows)
    loads = [pltpu.make_async_copy(tok_in, tok.at[own_rows], ld.at[0])]
    loads += [
        pltpu.make_async_copy(
            ref.at[:, aligned(z * width, width)],
            w.at[aligned(fs * depth, depth), pl.ds(k * width, width)],
            ld.at[1 + k],
        )
        for k, ref in enumerate(w_ins)
    ]
    loads += [
        pltpu.make_async_copy(wa_in, wout.at[fs, pl.ds(0, o_rows)], ld.at[6]),
        pltpu.make_async_copy(wc_in, wout.at[fs, pl.ds(o_rows, o_rows)], ld.at[7]),
        pltpu.make_async_copy(off_in, off_raw.at[z], ld.at[8]),
        pltpu.make_async_copy(ck_in.at[:, aligned(z * width, width)], ck, ld.at[9]),
        pltpu.make_async_copy(gain_in, gain, ld.at[10]),
        pltpu.make_async_copy(cgain_in, cgain, ld.at[11]),
    ]
    for copy in loads:
        copy.start()
    greet(
        [{"sp": (me + d) % n // n_tp, "tp": (me + d) % n % n_tp} for d in range(1, n)]
        + [{"fs": xn}, {"fs": yn}]
    )

    def piece_rows(block, core, p):
        return tok.at[aligned((block * n_tp + core) * rows + p * sub, sub)]

    def lift(block, dist, p):
        ref = piece_rows(block, tp, p)
        return remote(ref, ref, up_s.at[dist - 1, p], up_r.at[dist - 1, p], sp=(z + 1) % n_sp)

    def sink(block, dist, p):
        ref = piece_rows(block, tp, p)
        return remote(ref, ref, dn_s.at[dist - 1, p], dn_r.at[dist - 1, p], sp=(z + n_sp - 1) % n_sp)

    def across(block, p):
        ref = piece_rows(block, tp, p)
        return remote(ref, ref, par_s.at[block, p], par_r.at[block, p], tp=1 - tp)

    def from_partner(block, p):
        ref = piece_rows(block, 1 - tp, p)
        return remote(ref, ref, par_s.at[block, p], par_r.at[block, p], tp=1 - tp)

    def w_part(owner, h):
        return w.at[aligned(owner * depth + h * half, half)]

    def send_w(owner, h, sem, to):
        return remote(w_part(owner, h), w_part(owner, h), w_s.at[sem], w_r.at[sem], fs=to)

    def send_o(owner, k, sem, to):
        ref = wout.at[owner, pl.ds(k * quarter, quarter)]
        return remote(ref, ref, o_s.at[sem], o_r.at[sem], fs=to)

    loads[0].wait()
    for p in range(2):
        @pl.when(z < n_sp - 1)
        def _():
            lift(z, 1, p).start()

        @pl.when(z > 0)
        def _():
            sink(z, 1, p).start()

    for k in range(5):
        loads[1 + k].wait()
    w_first = [send_w(fs, 0, 0, xn), send_w(fs, 1, 1, yn), send_w(fs, 1, 2, xn), send_w(fs, 0, 3, yn)]
    for copy in w_first:
        copy.start()
    for p in range(2):
        across(z, p).start()
    loads[8].wait()
    offs = [
        remote(off_raw.at[z], off_raw.at[z], off_s.at[d - 1], off_r.at[d - 1], sp=(z + d) % n_sp)
        for d in range(1, n_sp)
    ]
    for copy in offs:
        copy.start()
    w_relay = [send_w(xn, 0, 4, yn), send_w(yn, 1, 5, xn)]
    w_here = [(0, xn, 0), (1, yn, 1), (2, xn, 1), (3, yn, 0), (4, dg, 0), (5, dg, 1)]
    o_first = []
    for a, b in ((0, 2), (1, 3), (2, 0), (3, 1)):
        o_first += [send_o(fs, a, a, xn), send_o(fs, b, 4 + b, yn)]
    o_relay = [send_o(xn, 0, 8, yn), send_o(yn, 2, 10, xn), send_o(xn, 1, 9, yn), send_o(yn, 3, 11, xn)]

    def token_hop(dist, p):
        @pl.when(z >= dist)
        def _():
            block = (z - dist + n_sp) % n_sp
            lift(block, dist, p).wait_recv()
            if dist < n_sp - 1:
                @pl.when(z < n_sp - 1)
                def _():
                    lift(block, dist + 1, p).start()
            across(block, p).start()

        @pl.when(z + dist < n_sp)
        def _():
            block = (z + dist) % n_sp
            sink(block, dist, p).wait_recv()
            if dist < n_sp - 1:
                @pl.when(z > 0)
                def _():
                    sink(block, dist + 1, p).start()
            across(block, p).start()

    def relay_w():
        for s, owner, h in w_here[:2]:
            send_w(owner, h, s, xn).wait_recv()
            w_relay[s].start()
        for copy in loads[6:8]:
            copy.wait()
        for copy in o_first:
            copy.start()

    gated[pl.ds(0, 32), :] = jnp.zeros((32, width), F32)
    for dist in range(1, n_sp - 1):
        token_hop(dist, 0)
        if dist == 1:
            relay_w()
        token_hop(dist, 1)
    if n_sp == 2:
        relay_w()
    for copy in loads[9:]:
        copy.wait()
    for s, owner, h in w_here[2:]:
        send_w(owner, h, s, xn).wait_recv()
    for copy in offs:
        copy.wait()
    off[...] = off_raw[...].astype(F32)

    lane = lax.broadcasted_iota(jnp.int32, (rows, width), 1)

    def project(tile, _):
        at = aligned(tile * rows, rows)
        x = tok[at, :].astype(F32)
        normed = (x * lax.rsqrt(jnp.mean(x * x, axis=1, keepdims=True) + 1e-06) * gain[...]).astype(BF16)
        out = jnp.dot(normed, w[...], preferred_element_type=F32).astype(BF16)
        q = out[:, :width].astype(F32) * HD ** (-0.5)
        for h in range(heads):
            mine = jnp.logical_and(lane >= h * HD, lane < (h + 1) * HD)
            queries[h, at, :] = jnp.where(mine, q, 0.0).astype(BF16)
        keys[at, :] = out[:, width : 2 * width]
        values[at, :] = out[:, 2 * width : 3 * width]
        value = out[:, 3 * width : 4 * width].astype(F32)
        gate = out[:, 4 * width :].astype(F32)
        gated[pl.ds(pl.multiple_of(tile * rows + 32, 32), rows), :] = (
            (value * jax.nn.sigmoid(gate)).astype(BF16).astype(F32)
        )
        return 0

    ones = jnp.full((8, width), 1.0 / width, F32)
    top = lax.broadcasted_iota(jnp.int32, (8, rows), 0) == 0

    def average(x):
        return lax.dot_general(
            ones, x, (((1,), (1,)), ((), ())), precision=lax.Precision.HIGHEST, preferred_element_type=F32
        )

    def convolve(tile, _):
        base = pl.multiple_of(tile * rows, rows)
        total = jnp.zeros((rows, width), F32)
        for tap in range(taps):
            total = total + ck[tap : tap + 1, :] * gated[pl.ds(base + (33 - taps + tap), rows), :]
        local = total - jnp.mean(total, axis=1, keepdims=True)
        conv_out[pl.ds(base, rows), :] = local.astype(BF16)
        stat_out[tile] = jnp.where(top, average(total), average(local * local))
        return 0

    def block_rows(i):
        return aligned(i * blk, blk)

    def ship(k, source, block):
        at = source.at[block_rows(block)]

        @pl.when(block == z)
        def _():
            x_all[k * n_sp + z] = at[...]

        @pl.when(block != z)
        def _():
            remote(at, x_all.at[k * n_sp + z], x_s.at[k, block], x_r.at[k, z], sp=block).start()

    tiles = blk // rows

    def ship_stat(block):
        at = stat_out.at[pl.ds(block * tiles, tiles)]

        @pl.when(block == z)
        def _():
            stat_all[z] = at[...]

        @pl.when(block != z)
        def _():
            remote(at, stat_all.at[z], st_s.at[0, block], st_r.at[z], sp=block).start()

        remote(at, stat_all.at[n_sp + z], st_s.at[1, block], st_r.at[n_sp + z], sp=block, tp=1 - tp).start()

    row = lax.broadcasted_iota(jnp.int32, (blk, blk), 0)
    col = lax.broadcasted_iota(jnp.int32, (blk, blk), 1)
    wide = lax.broadcasted_iota(jnp.int32, (blk, width), 1)

    def attend(i, j, diagonal):
        k = keys[block_rows(j), :]
        v = values[block_rows(j), :]
        after = jnp.where(row >= col, 1.0, 0.0).astype(BF16)
        for h in range(heads):
            q = queries[h, block_rows(i), :]
            s = lax.dot_general(q, k, (((1,), (1,)), ((), ())), preferred_element_type=F32)
            s = s + off[j, pl.ds(z * heads + h, 1), :]
            keep = jnp.minimum(-s, 0.0) - jnp.log(1.0 + jnp.exp(-jnp.abs(s)))
            if diagonal:
                keep = jnp.where(col < row, keep, 0.0)
            suffix = jnp.dot(keep.astype(BF16), after, preferred_element_type=F32)
            if diagonal:
                weights = jnp.where(col < row, jnp.exp(s + suffix), 0.0)
                carry[i, h] = suffix[:, :1]
                running[i, h] = jnp.dot(weights.astype(BF16), v, preferred_element_type=F32)
            else:
                before = carry[i, h]
                weights = jnp.exp(s + suffix + before)
                carry[i, h] = before + suffix[:, :1]
                running[i, h] += jnp.dot(weights.astype(BF16), v, preferred_element_type=F32)

        @pl.when(j == 0)
        def _():
            merged = running[i, 0]
            for h in range(1, heads):
                merged = jnp.where(wide >= h * HD, running[i, h], merged)
            attn_out[block_rows(i), :] = merged.astype(BF16)
            ship(0, attn_out, i)

    pairs = jnp.minimum(z, n_sp - 1 - z)

    def step(s, _):
        dist = (s + 1) // 2
        inner = jnp.where(s % 2 == 1, z - dist, z + dist)
        outer = jnp.where(z == pairs, s, n_sp - 1 - s)
        block = jnp.where(s <= 2 * pairs, inner, outer)
        rising = block > z

        @pl.when(s == n_sp - 1)
        def _():
            for k in (0, 1):
                send_o(xn, k, k, xn).wait_recv()
                send_o(yn, 2 + k, 6 + k, xn).wait_recv()
            for copy in o_relay:
                copy.start()

        @pl.when(jnp.logical_and(s == n_sp - 1, pairs == 0))
        def _():
            for p in range(2):
                token_hop(n_sp - 1, p)

        for p in range(2):
            from_partner(block, p).wait_recv()
        lax.fori_loop(block * n_tp, block * n_tp + n_tp, project, 0)

        lax.fori_loop(block * tiles + 1, block * tiles + tiles, convolve, 0)

        def conv_block(u, _):
            target = jnp.where(rising, block, jnp.where(jnp.logical_and(u == 0, s > 0), block + 1, 0))
            convolve(target * tiles, 0)
            ship(1, conv_out, target)
            ship_stat(target)
            return 0

        falling_count = jnp.where(s > 0, 1, 0) + jnp.where(block == 0, 1, 0)
        lax.fori_loop(0, jnp.where(rising, 1, falling_count), conv_block, 0)
        attend(block, block, True)

        def further(t, _):
            attend(jnp.where(rising, block, block + t), jnp.where(rising, block - t, block), False)
            return 0

        lax.fori_loop(1, s + 1, further, 0)
        return 0

    lax.fori_loop(0, n_sp, step, 0)

    others = [(z + d) % n_sp for d in range(1, n_sp)]

    def stat_from(slot):
        return remote(stat_all.at[slot], stat_all.at[slot], st_s.at[0, z], st_r.at[slot], tp=1 - tp)

    def x_from(k, source):
        ref = x_all.at[k * n_sp + source]
        return remote(ref, ref, x_s.at[k, z], x_r.at[k, source], tp=1 - tp)

    for source in others:
        stat_from(source).wait_recv()
    for source in range(n_sp):
        stat_from(n_sp + source).wait_recv()
    for source in others:
        x_from(1, source).wait_recv()
    square = (lax.broadcasted_iota(jnp.int32, (rows, rows), 0)
              == lax.broadcasted_iota(jnp.int32, (rows, rows), 1)).astype(F32)
    kind = lax.broadcasted_iota(jnp.int32, (rows, n * 8), 1) % 8
    for t in range(tiles):
        flat = stat_all[:, t].reshape(n * 8, rows)
        stats = lax.dot_general(
            square, flat, (((1,), (1,)), ((), ())), precision=lax.Precision.HIGHEST, preferred_element_type=F32
        )
        mean = jnp.sum(jnp.where(kind == 0, stats, 0.0), axis=1, keepdims=True) / n
        off_mean = stats - mean
        spread = jnp.where(kind == 0, off_mean * off_mean, jnp.where(kind == 1, stats, 0.0))
        scale = lax.rsqrt(jnp.sum(spread, axis=1, keepdims=True) / n + 1e-06)
        at = pl.ds(t * rows, rows)
        for g in range(n_sp):
            x = x_all[n_sp + g, at, :].astype(F32) + off_mean[:, 8 * g : 8 * g + 1]
            y = x * scale * cgain[:, g * width : (g + 1) * width]
            hidden[at, (n_sp + g) * width : (n_sp + g + 1) * width] = (y * jax.nn.sigmoid(y)).astype(BF16)
    for source in others:
        x_from(0, source).wait_recv()
    for g in range(n_sp):
        hidden[:, g * width : (g + 1) * width] = x_all[g]

    sent = []
    for index, owner in enumerate((fs, xn, yn, dg)):
        if owner is xn:
            for k in (2, 3):
                send_o(xn, k, k, xn).wait_recv()
        elif owner is yn:
            for k in (0, 1):
                send_o(yn, k, 4 + k, xn).wait_recv()
        elif owner is dg:
            for k in range(4):
                send_o(dg, k, 8 + k, xn).wait_recv()
        part[index] = jnp.dot(hidden[...], wout[owner], preferred_element_type=F32).astype(BF16)
        cols = aligned(owner * o_cols, o_cols)
        keep = pltpu.make_async_copy(
            part.at[index, aligned(tp * rows, rows)], own_out.at[:, cols], keep_s.at[index]
        )
        give = remote(
            part.at[index, aligned((1 - tp) * rows, rows)], got_out.at[:, cols],
            part_s.at[index], part_r.at[index], tp=1 - tp,
        )
        give.start()
        keep.start()
        sent += [keep, give]

    for copy in w_first + w_relay + o_first + o_relay:
        copy.wait_send()
    for p in range(2):
        for dist in range(1, n_sp):
            @pl.when(jnp.logical_and(z < n_sp - 1, z >= dist - 1))
            def _():
                lift(z, dist, p).wait_send()

            @pl.when(jnp.logical_and(z > 0, z + dist - 1 < n_sp))
            def _():
                sink(z, dist, p).wait_send()

        for block in range(n_sp):
            across(block, p).wait_send()
    for block in others:
        for k in range(2):
            remote(x_all.at[k], x_all.at[k], x_s.at[k, block], x_r.at[k, z], tp=1 - tp).wait_send()
        remote(stat_all.at[z], stat_all.at[z], st_s.at[0, block], st_r.at[z], tp=1 - tp).wait_send()
    for block in range(n_sp):
        remote(stat_all.at[z], stat_all.at[z], st_s.at[1, block], st_r.at[z], tp=1 - tp).wait_send()
    for copy in sent:
        copy.wait()


def layer_call(n_sp, n_fs, n_tp, width, heads, blk, tokens, gain, w_ins, off, ck, cgain, wa, wc):
    rows, features = tokens.shape
    depth = w_ins[0].shape[0]
    o_rows, o_cols = wa.shape
    length, n = rows * n_sp * n_tp, n_sp * n_tp
    tiles = blk // rows
    dma = pltpu.SemaphoreType.DMA
    vmem = pltpu.VMEM
    result = jax.ShapeDtypeStruct((rows, n_fs * o_cols), BF16)
    return pl.pallas_call(
        functools.partial(layer_body, n_sp, n_tp, width, heads, ck.shape[0], blk),
        out_shape=[result, result],
        in_specs=[ANY] * 12,
        out_specs=[ANY] * 2,
        scratch_shapes=[
            vmem((length, features), BF16),
            vmem((n_fs * depth, 5 * width), BF16),
            vmem((n_fs, 2 * o_rows, o_cols), BF16),
            vmem((n_sp,) + off.shape, BF16),
            vmem((n_sp,) + off.shape, F32),
            vmem((ck.shape[0], width), F32),
            vmem(gain.shape, F32),
            vmem(cgain.shape, F32),
            vmem((heads, length, width), BF16),
            vmem((length, width), BF16),
            vmem((length, width), BF16),
            vmem((length + 32, width), F32),
            vmem((n_sp, heads, blk, 1), F32),
            vmem((n_sp, heads, blk, width), F32),
            vmem((length, width), BF16),
            vmem((length, width), BF16),
            vmem((length // rows, 8, rows), F32),
            vmem((2 * n_sp, blk, width), BF16),
            vmem((n, tiles, 8, rows), F32),
            vmem((blk, 2 * n_sp * width), BF16),
            vmem((n_fs, blk, o_cols), BF16),
            dma((12,)),
            dma((n_sp - 1, 2)), dma((n_sp - 1, 2)), dma((n_sp - 1, 2)), dma((n_sp - 1, 2)),
            dma((n_sp, 2)), dma((n_sp, 2)),
            dma((6,)), dma((6,)),
            dma((n_sp - 1,)), dma((n_sp - 1,)),
            dma((12,)), dma((12,)),
            dma((2, n_sp)), dma((2, n_sp)),
            dma((2, n_sp)), dma((n,)),
            dma((n_fs,)), dma((n_fs,)), dma((n_fs,)),
        ],
        compiler_params=pltpu.CompilerParams(collective_id=0, has_side_effects=True),
        name="layer",
    )(tokens, gain, *w_ins, off, ck, cgain, wa, wc)


def spread_shards(
    tokens,
    norm_gain,
    w_query,
    w_key,
    w_value,
    w_conv_value,
    w_conv_gate,
    key_offset,
    conv_kernel,
    conv_gain,
    w_attn_out,
    w_conv_out,
):
    n_sp, n_fs, n_tp = (lax.axis_size(a) for a in ("sp", "fs", "tp"))
    width = w_query.shape[1] // n_sp
    own, got = layer_call(
        n_sp, n_fs, n_tp, width, width // HD, key_offset.shape[0], tokens[0], norm_gain[None],
        (w_query, w_key, w_value, w_conv_value, w_conv_gate), jnp.transpose(key_offset),
        conv_kernel, conv_gain[None], w_attn_out, w_conv_out,
    )
    return (own.astype(F32) + got.astype(F32)).astype(BF16)[None]


def shifted(block, axis, distance):
    devices = range(lax.axis_size(axis))
    route = [(i - distance, i) for i in devices if i - distance in devices]
    return lax.ppermute(block, axis, route)


def piece_terms(queries, key_rows, value_rows, offsets, carry_log, allowed):
    head_size = queries.shape[2]
    logits = jnp.einsum(
        "qhd,khd->hqk", queries, key_rows, preferred_element_type=jnp.float32
    ) * head_size ** (-0.5)
    logits = logits + jnp.transpose(offsets.astype(jnp.float32))[:, None, :]
    log_keep = jax.nn.log_sigmoid(-logits)
    if allowed is not None:
        log_keep = jnp.where(allowed[None], log_keep, 0.0)
    between = lax.cumsum(log_keep, axis=2, reverse=True) - log_keep
    weights = jnp.exp(jax.nn.log_sigmoid(logits) + between + carry_log[:, :, None])
    if allowed is not None:
        weights = jnp.where(allowed[None], weights, 0.0)
    result = jnp.einsum(
        "hqk,khd->qhd", weights.astype(jnp.bfloat16), value_rows, preferred_element_type=jnp.float32
    )
    return (result, carry_log + jnp.sum(log_keep, axis=2))


def shards(
    tokens,
    norm_gain,
    w_query,
    w_key,
    w_value,
    w_conv_value,
    w_conv_gate,
    key_offset,
    conv_kernel,
    conv_gain,
    w_attn_out,
    w_conv_out,
):
    gathered = (
        lax.all_gather(w_query, "fs", axis=0, tiled=True),
        lax.all_gather(w_key, "fs", axis=0, tiled=True),
        lax.all_gather(w_value, "fs", axis=0, tiled=True),
        lax.all_gather(w_conv_value, "fs", axis=0, tiled=True),
        lax.all_gather(w_conv_gate, "fs", axis=0, tiled=True),
    )
    floats = lax.all_gather(tokens[0], "tp", axis=0, tiled=True).astype(jnp.float32)
    normed = (
        floats * lax.rsqrt(jnp.mean(floats * floats, axis=1, keepdims=True) + 1e-06) * norm_gain
    ).astype(jnp.bfloat16)
    projected = jnp.concatenate(
        [
            jnp.dot(normed, weight, preferred_element_type=jnp.float32).astype(jnp.bfloat16)
            for weight in gathered
        ],
        axis=1,
    )
    head_cols = w_query.shape[1]
    channels = w_conv_value.shape[1]
    block_len = projected.shape[0]
    local_heads = head_cols // HD
    queries = projected[:, :head_cols].reshape(block_len, local_heads, HD)
    key_flat = projected[:, head_cols : 2 * head_cols]
    value_flat = projected[:, 2 * head_cols : 3 * head_cols]
    conv_value = projected[:, 3 * head_cols : 3 * head_cols + channels]
    conv_gate = projected[:, 3 * head_cols + channels :]
    position = lax.axis_index("sp")
    positions = jnp.arange(block_len, dtype=jnp.int32)
    causal = positions[None, :] < positions[:, None]
    start_log = jnp.zeros((local_heads, block_len), jnp.float32)
    totals, carry_log = piece_terms(
        queries,
        key_flat.reshape(block_len, local_heads, HD),
        value_flat.reshape(block_len, local_heads, HD),
        key_offset,
        start_log,
        causal,
    )

    def visit(hop_count, carried):
        running, running_log, moving = carried
        moving = shifted((moving[0], moving[1], moving[2]), "sp", 1)
        result, next_log = piece_terms(
            queries,
            moving[0].reshape(block_len, local_heads, HD),
            moving[1].reshape(block_len, local_heads, HD),
            moving[2],
            running_log,
            None,
        )
        active = position >= hop_count
        running = jnp.where(active, running + result, running)
        running_log = jnp.where(active, next_log, running_log)
        return (running, running_log, moving)

    totals, carry_log, leftover = lax.fori_loop(
        1, lax.axis_size("sp"), visit, (totals, carry_log, (key_flat, value_flat, key_offset))
    )
    attn_heads = totals.reshape(block_len, head_cols).astype(jnp.bfloat16)
    gated_input = (
        conv_value.astype(jnp.float32) * jax.nn.sigmoid(conv_gate.astype(jnp.float32))
    ).astype(jnp.bfloat16)
    kernel_len = conv_kernel.shape[0]
    edge_rows = shifted(gated_input[block_len - (kernel_len - 1) :], "sp", 1)
    extended = jnp.concatenate([edge_rows, gated_input], axis=0).astype(jnp.float32)
    conv_sum = jnp.zeros((block_len, channels), jnp.float32)
    for tap_index in range(kernel_len):
        conv_sum = conv_sum + conv_kernel[tap_index] * extended[tap_index : tap_index + block_len]
    channel_total = lax.psum(jnp.sum(conv_sum, axis=1), "tp")
    centred = conv_sum - (channel_total / CC)[:, None]
    spread = lax.psum(jnp.sum(centred * centred, axis=1), "tp") / CC
    conv_hidden = jax.nn.silu(centred * lax.rsqrt(spread + 1e-06)[:, None] * conv_gain).astype(
        jnp.bfloat16
    )
    attn_weight, conv_weight = (
        lax.all_gather(w_attn_out, "fs", axis=1, tiled=True),
        lax.all_gather(w_conv_out, "fs", axis=1, tiled=True),
    )
    partial_value = jnp.dot(attn_heads, attn_weight, preferred_element_type=jnp.float32)
    partial_value = partial_value + jnp.dot(
        conv_hidden, conv_weight, preferred_element_type=jnp.float32
    )
    mixed = lax.psum_scatter(
        lax.optimization_barrier(partial_value.astype(jnp.bfloat16))
        .astype(jnp.float32)
        .astype(jnp.bfloat16),
        "tp",
        scatter_dimension=0,
        tiled=True,
    )
    return mixed[None]


def solution(mesh):
    placed = (
        P("fs", ("sp", "tp"), None),
        P(),
        P("fs", "tp"),
        P("fs", "tp"),
        P("fs", "tp"),
        P("fs", "tp"),
        P("fs", "tp"),
        P("sp", "tp"),
        P(None, "tp"),
        P("tp"),
        P("tp", "fs"),
        P("tp", "fs"),
    )

    def fits(tokens, norm_gain, w_query, *rest):
        n_sp, n_fs, n_tp = mesh.shape["sp"], mesh.shape["fs"], mesh.shape["tp"]
        cols = w_query.shape[1] // n_tp
        return n_fs == 4 and n_tp == 2 and n_sp > 1 and rest[5].shape[0] <= 33 and cols % (128 * n_sp) == 0 and rest[2].shape[1] == w_query.shape[1] and (
            tokens.shape[1] % (128 * n_sp * n_tp) == 0
        )

    def program(*args):
        body = spread_shards if fits(*args) else shards
        return mapped(body)(*args)

    def mapped(body):
        return jax.shard_map(
            body, mesh=mesh, in_specs=placed, out_specs=P("fs", ("sp", "tp"), None), check_vma=False
        )

    return program
```

```python
import functools

import jax
import jax.numpy as jnp
from jax import lax
from jax.experimental import pallas as pl
from jax.experimental.pallas import tpu as pltpu
from jax.sharding import PartitionSpec as P

HD = 64
CC = 1024
MESH = pl.DeviceIdType.MESH
F32 = jnp.float32
BF16 = jnp.bfloat16


def remote(src, dst, send, recv, **where):
    return pltpu.make_async_remote_copy(
        src_ref=src, dst_ref=dst, send_sem=send, recv_sem=recv, device_id=where, device_id_type=MESH
    )


def greet(peers):
    barrier = pltpu.get_barrier_semaphore()
    for where in peers:
        pl.semaphore_signal(barrier, inc=1, device_id=where, device_id_type=MESH)
    pl.semaphore_wait(barrier, len(peers))


def plane(fs):
    y = (fs + 2) % 4
    return fs + 1 - 2 * (fs % 2), y, y + 1 - 2 * (y % 2)


ANY = pl.BlockSpec(memory_space=pl.ANY)


LOG2E = 1.4426950408889634


def aligned(start, size):
    return pl.ds(pl.multiple_of(start, size), size)


def layer_body(n_sp, n_tp, width, heads, taps, blk, *refs):
    tok_in, gain_in, w_ins, off_in, ck_in, cgain_in, wa_in, wc_in = refs[0], refs[1], refs[2:7], *refs[7:12]
    own_out, got_out = refs[12:14]
    tok, w, wout, off_raw, off, ck, gain, cgain = refs[14:22]
    queries, keys, values, gated, carry, running = refs[22:28]
    attn_out, conv_out, stat_out, x_all, stat_all, hidden, part = refs[28:35]
    ld, up_s, up_r, dn_s, dn_r, par_s, par_r, w_s, w_r, off_s, off_r = refs[35:46]
    o_s, o_r, x_s, x_r, st_s, st_r, part_s, part_r, keep_s = refs[46:]
    rows = tok_in.shape[0]
    tiles = blk // rows
    sub = rows // 2
    depth = w_ins[0].shape[0]
    half = depth // 2
    o_rows, o_cols = wa_in.shape
    eighth = o_rows // 4
    z, fs, tp = lax.axis_index("sp"), lax.axis_index("fs"), lax.axis_index("tp")
    xn, yn, dg = plane(fs)
    n = n_sp * n_tp
    me = z * n_tp + tp

    own_rows = aligned((z * n_tp + tp) * rows, rows)
    loads = [pltpu.make_async_copy(tok_in, tok.at[own_rows], ld.at[0])]
    loads += [
        pltpu.make_async_copy(
            ref.at[:, aligned(z * width, width)],
            w.at[aligned(fs * depth, depth), pl.ds(k * width, width)],
            ld.at[1 + k],
        )
        for k, ref in enumerate(w_ins)
    ]
    loads += [
        pltpu.make_async_copy(wa_in, wout.at[fs, pl.ds(0, o_rows)], ld.at[6]),
        pltpu.make_async_copy(wc_in, wout.at[fs, pl.ds(o_rows, o_rows)], ld.at[7]),
        pltpu.make_async_copy(off_in, off_raw.at[z], ld.at[8]),
        pltpu.make_async_copy(ck_in.at[:, aligned(z * width, width)], ck, ld.at[9]),
        pltpu.make_async_copy(gain_in, gain, ld.at[10]),
        pltpu.make_async_copy(cgain_in, cgain, ld.at[11]),
    ]
    for copy in loads:
        copy.start()
    greet(
        [{"sp": (me + d) % n // n_tp, "tp": (me + d) % n % n_tp} for d in range(1, n)]
        + [{"fs": xn}, {"fs": yn}]
    )

    def piece_rows(block, core, p):
        return tok.at[aligned((block * n_tp + core) * rows + p * sub, sub)]

    def lift(block, dist, p):
        ref = piece_rows(block, tp, p)
        return remote(ref, ref, up_s.at[dist - 1, p], up_r.at[dist - 1, p], sp=(z + 1) % n_sp)

    def sink(block, dist, p):
        ref = piece_rows(block, tp, p)
        return remote(ref, ref, dn_s.at[dist - 1, p], dn_r.at[dist - 1, p], sp=(z + n_sp - 1) % n_sp)

    def across(block, p):
        ref = piece_rows(block, tp, p)
        return remote(ref, ref, par_s.at[block, p], par_r.at[block, p], tp=1 - tp)

    def from_partner(block, p):
        ref = piece_rows(block, 1 - tp, p)
        return remote(ref, ref, par_s.at[block, p], par_r.at[block, p], tp=1 - tp)

    def w_part(owner, h):
        return w.at[aligned(owner * depth + h * half, half)]

    def send_w(owner, h, sem, to):
        return remote(w_part(owner, h), w_part(owner, h), w_s.at[sem], w_r.at[sem], fs=to)

    def send_o(owner, k, sem, to):
        ref = wout.at[owner, aligned(k * eighth, eighth)]
        return remote(ref, ref, o_s.at[sem], o_r.at[sem], fs=to)

    loads[0].wait()
    for p in range(2):
        @pl.when(z < n_sp - 1)
        def _():
            lift(z, 1, p).start()

        @pl.when(z > 0)
        def _():
            sink(z, 1, p).start()

    for k in range(5):
        loads[1 + k].wait()
    w_first = [send_w(fs, 0, 0, xn), send_w(fs, 1, 1, yn), send_w(fs, 1, 2, xn), send_w(fs, 0, 3, yn)]
    for copy in w_first:
        copy.start()
    for p in range(2):
        across(z, p).start()
    loads[8].wait()
    offs = [
        remote(off_raw.at[z], off_raw.at[z], off_s.at[d - 1], off_r.at[d - 1], sp=(z + d) % n_sp)
        for d in range(1, n_sp)
    ]
    for copy in offs:
        copy.start()
    w_relay = [send_w(xn, 0, 4, yn), send_w(yn, 1, 5, xn)]
    w_here = [(0, xn, 0), (1, yn, 1), (2, xn, 1), (3, yn, 0), (4, dg, 0), (5, dg, 1)]
    mate = z + 1 - 2 * (z % 2)
    lead = jnp.where(jnp.logical_or(z == 0, z == n_sp - 1), 0, 3)
    o_first, o_later = [], []
    for k in (lead, 1, 2, 3 - lead):
        o_first += [send_o(fs, k, k, xn), send_o(fs, 4 + k, 12 + k, yn)]
    for k in range(4):
        o_later += [send_o(fs, 4 + k, 4 + k, xn), send_o(fs, k, 8 + k, yn)]

    def relay_o(k):
        send_o(xn, k, k, xn).wait_recv()
        send_o(yn, 4 + k, 12 + k, xn).wait_recv()
        send_o(xn, k, 16 + k, yn).start()
        send_o(yn, 4 + k, 20 + k, xn).start()

    def share_o(k, sem):
        ref = wout.at[dg, aligned(k * eighth, eighth)]
        return remote(ref, ref, o_s.at[sem], o_r.at[sem], sp=mate)

    def token_hop(dist, p):
        @pl.when(z >= dist)
        def _():
            block = (z - dist + n_sp) % n_sp
            lift(block, dist, p).wait_recv()
            if dist < n_sp - 1:
                @pl.when(z < n_sp - 1)
                def _():
                    lift(block, dist + 1, p).start()
            across(block, p).start()

        @pl.when(z + dist < n_sp)
        def _():
            block = (z + dist) % n_sp
            sink(block, dist, p).wait_recv()
            if dist < n_sp - 1:
                @pl.when(z > 0)
                def _():
                    sink(block, dist + 1, p).start()
            across(block, p).start()

    def relay_w():
        for s, owner, h in w_here[:2]:
            send_w(owner, h, s, xn).wait_recv()
            w_relay[s].start()
        for copy in loads[6:8]:
            copy.wait()
        for copy in o_first:
            copy.start()

    gated[pl.ds(0, 32), :] = jnp.zeros((32, width), F32)
    for dist in range(1, n_sp - 1):
        token_hop(dist, 0)
        if dist == 1:
            relay_w()
        token_hop(dist, 1)
    if n_sp == 2:
        relay_w()
    for copy in loads[9:]:
        copy.wait()
    for s, owner, h in w_here[2:]:
        send_w(owner, h, s, xn).wait_recv()
    for copy in offs:
        copy.wait()
    off[...] = off_raw[...].astype(F32) * LOG2E

    lane = lax.broadcasted_iota(jnp.int32, (rows, width), 1)

    def project(tile, _):
        at = aligned(tile * rows, rows)
        x = tok[at, :].astype(F32)
        normed = (x * lax.rsqrt(jnp.mean(x * x, axis=1, keepdims=True) + 1e-06) * gain[...]).astype(BF16)
        out = jnp.dot(normed, w[...], preferred_element_type=F32).astype(BF16)
        q = out[:, :width].astype(F32) * HD ** (-0.5)
        for h in range(heads):
            mine = jnp.logical_and(lane >= h * HD, lane < (h + 1) * HD)
            queries[tile // tiles, pl.ds(pl.multiple_of(h * blk + tile % tiles * rows, rows), rows), :] = (
                jnp.where(mine, q, 0.0).astype(BF16)
            )
        keys[at, :] = out[:, width : 2 * width]
        values[at, :] = out[:, 2 * width : 3 * width]
        value = out[:, 3 * width : 4 * width].astype(F32)
        gate = out[:, 4 * width :].astype(F32)
        gated[pl.ds(pl.multiple_of(tile * rows + 32, 32), rows), :] = (
            (value * jax.nn.sigmoid(gate)).astype(BF16).astype(F32)
        )
        return 0

    def convolve(tile, _):
        base = pl.multiple_of(tile * rows, rows)
        total = jnp.zeros((rows, width), F32)
        for phase in range(8):
            span = rows + 8 if phase else rows
            lined = jnp.zeros((span, width), F32)
            for tap in range((phase + taps - 33) % 8, taps, 8):
                lined = lined + ck[tap : tap + 1, :] * gated[pl.ds(base + (33 - taps + tap - phase), span), :]
            total = total + lined[phase : phase + rows]
        mean = jnp.mean(total, axis=1, keepdims=True)
        local = total - mean
        conv_out[pl.ds(base, rows), :] = local.astype(BF16)
        spread = jnp.mean(local * local, axis=1, keepdims=True)
        stat_out[tile] = jnp.transpose(jnp.where(lane == 0, mean, spread))[:8]
        return 0

    def block_rows(i):
        return aligned(i * blk, blk)

    def ship(k, source, block):
        at = source.at[block_rows(block)]

        @pl.when(block == z)
        def _():
            x_all[k * n_sp + z] = at[...]

        @pl.when(block != z)
        def _():
            remote(at, x_all.at[k * n_sp + z], x_s.at[k, block], x_r.at[k, z], sp=block).start()


    def ship_stat(block):
        at = stat_out.at[pl.ds(block * tiles, tiles)]

        @pl.when(block == z)
        def _():
            stat_all[z] = at[...]

        @pl.when(block != z)
        def _():
            remote(at, stat_all.at[z], st_s.at[0, block], st_r.at[z], sp=block).start()

        remote(at, stat_all.at[n_sp + z], st_s.at[1, block], st_r.at[n_sp + z], sp=block, tp=1 - tp).start()

    wide = lax.broadcasted_iota(jnp.int32, (blk, width), 1)
    row = lax.broadcasted_iota(jnp.int32, (blk, blk), 0)
    col = lax.broadcasted_iota(jnp.int32, (blk, blk), 1)
    stacked = (heads, blk, blk)
    earlier = lax.broadcasted_iota(jnp.int32, stacked, 2) < lax.broadcasted_iota(jnp.int32, stacked, 1)
    earlier = earlier.reshape(heads * blk, blk)

    def attend(i, j, diagonal):
        k = keys[block_rows(j), :]
        v = values[block_rows(j), :]
        after = jnp.where(row >= col, 1.0, 0.0).astype(BF16)
        s = lax.dot_general(queries[i], k, (((1,), (1,)), ((), ())), preferred_element_type=F32)
        shift = jnp.concatenate(
            [jnp.broadcast_to(off[j, pl.ds(z * heads + h, 1), :], (blk, blk)) for h in range(heads)], axis=0
        )
        s = s * LOG2E + shift
        keep = jnp.minimum(-s, 0.0) - jnp.log2(1.0 + jnp.exp2(-jnp.abs(s)))
        if diagonal:
            keep = jnp.where(earlier, keep, 0.0)
        suffix = jnp.dot(keep.astype(BF16), after, preferred_element_type=F32)
        if diagonal:
            weights = jnp.where(earlier, jnp.exp2(s + suffix), 0.0)
            carry[i] = suffix[:, :1]
            running[i] = jnp.dot(weights.astype(BF16), v, preferred_element_type=F32)
        else:
            before = carry[i]
            weights = jnp.exp2(s + suffix + before)
            carry[i] = before + suffix[:, :1]
            running[i] += jnp.dot(weights.astype(BF16), v, preferred_element_type=F32)

        @pl.when(j == 0)
        def _():
            merged = running[i, :blk]
            for h in range(1, heads):
                merged = jnp.where(wide >= h * HD, running[i, h * blk : (h + 1) * blk], merged)
            attn_out[block_rows(i), :] = merged.astype(BF16)
            ship(0, attn_out, i)

    pairs = jnp.minimum(z, n_sp - 1 - z)

    def step(s, _):
        dist = (s + 1) // 2
        inner = jnp.where(s % 2 == 1, z - dist, z + dist)
        outer = jnp.where(z == pairs, s, n_sp - 1 - s)
        block = jnp.where(s <= 2 * pairs, inner, outer)
        rising = block > z

        @pl.when(s == n_sp - 1)
        def _():
            for k in (1, 2):
                relay_o(k)

        @pl.when(s == n_sp - 2)
        def _():
            relay_o(lead)
            for copy in o_later:
                copy.start()

        @pl.when(jnp.logical_and(s == n_sp - 1, pairs == 0))
        def _():
            for p in range(2):
                token_hop(n_sp - 1, p)

        for p in range(2):
            from_partner(block, p).wait_recv()
        lax.fori_loop(block * n_tp, block * n_tp + n_tp, project, 0)

        lax.fori_loop(block * tiles + 1, block * tiles + tiles, convolve, 0)

        def conv_block(u, _):
            target = jnp.where(rising, block, jnp.where(jnp.logical_and(u == 0, s > 0), block + 1, 0))
            convolve(target * tiles, 0)
            ship(1, conv_out, target)
            ship_stat(target)
            return 0

        falling_count = jnp.where(s > 0, 1, 0) + jnp.where(block == 0, 1, 0)
        lax.fori_loop(0, jnp.where(rising, 1, falling_count), conv_block, 0)
        attend(block, block, True)

        def further(t, _):
            attend(jnp.where(rising, block, block + t), jnp.where(rising, block - t, block), False)
            return 0

        lax.fori_loop(1, s + 1, further, 0)
        return 0

    lax.fori_loop(0, n_sp, step, 0)

    for k, sem in ((0, 24), (4, 25)):
        send_o(dg, k + lead, 16 + k + lead, xn).wait_recv()
        share_o(k + lead, sem).start()
    others = [(z + d) % n_sp for d in range(1, n_sp)]

    def stat_from(slot):
        return remote(stat_all.at[slot], stat_all.at[slot], st_s.at[0, z], st_r.at[slot], tp=1 - tp)

    def x_from(k, source):
        ref = x_all.at[k * n_sp + source]
        return remote(ref, ref, x_s.at[k, z], x_r.at[k, source], tp=1 - tp)

    for source in others:
        stat_from(source).wait_recv()
    for source in range(n_sp):
        stat_from(n_sp + source).wait_recv()
    for source in others:
        x_from(1, source).wait_recv()
    kind = lax.broadcasted_iota(jnp.int32, (rows, n * 8), 1) % 8
    for t in range(tiles):
        stats = jnp.transpose(stat_all[:, t].reshape(n * 8, rows))
        mean = jnp.sum(jnp.where(kind == 0, stats, 0.0), axis=1, keepdims=True) / n
        off_mean = stats - mean
        spread = jnp.where(kind == 0, off_mean * off_mean, jnp.where(kind == 1, stats, 0.0))
        scale = lax.rsqrt(jnp.sum(spread, axis=1, keepdims=True) / n + 1e-06)
        at = pl.ds(t * rows, rows)
        for g in range(n_sp):
            x = x_all[n_sp + g, at, :].astype(F32) + off_mean[:, 8 * g : 8 * g + 1]
            y = x * scale * cgain[:, g * width : (g + 1) * width]
            hidden[at, (n_sp + g) * width : (n_sp + g + 1) * width] = (y * jax.nn.sigmoid(y)).astype(BF16)
    for source in others:
        x_from(0, source).wait_recv()
    for g in range(n_sp):
        hidden[:, g * width : (g + 1) * width] = x_all[g]

    sent = []
    for index, owner in enumerate((fs, xn, yn, dg)):
        if owner is xn:
            for k in (3 - lead, 4, 5, 6, 7):
                send_o(xn, k, k, xn).wait_recv()
        elif owner is yn:
            for k in (0, 1, 2, 3, 7 - lead):
                send_o(yn, k, 8 + k, xn).wait_recv()
        elif owner is dg:
            for k in (1, 2, 5, 6):
                send_o(dg, k, 16 + k, xn).wait_recv()
            for k, sem in ((0, 24), (4, 25)):
                share_o(k + 3 - lead, sem).wait_recv()
        part[index] = jnp.dot(hidden[...], wout[owner], preferred_element_type=F32).astype(BF16)
        cols = aligned(owner * o_cols, o_cols)
        keep = pltpu.make_async_copy(
            part.at[index, aligned(tp * rows, rows)], own_out.at[:, cols], keep_s.at[index]
        )
        give = remote(
            part.at[index, aligned((1 - tp) * rows, rows)], got_out.at[:, cols],
            part_s.at[index], part_r.at[index], tp=1 - tp,
        )
        give.start()
        keep.start()
        sent += [keep, give]

    for copy in w_first + w_relay + o_first + o_later:
        copy.wait_send()
    for k in (lead, 1, 2):
        send_o(xn, k, 16 + k, yn).wait_send()
        send_o(yn, 4 + k, 20 + k, xn).wait_send()
    for k, sem in ((0, 24), (4, 25)):
        share_o(k + lead, sem).wait_send()
    for p in range(2):
        for dist in range(1, n_sp):
            @pl.when(jnp.logical_and(z < n_sp - 1, z >= dist - 1))
            def _():
                lift(z, dist, p).wait_send()

            @pl.when(jnp.logical_and(z > 0, z + dist - 1 < n_sp))
            def _():
                sink(z, dist, p).wait_send()

        for block in range(n_sp):
            across(block, p).wait_send()
    for block in others:
        for k in range(2):
            remote(x_all.at[k], x_all.at[k], x_s.at[k, block], x_r.at[k, z], tp=1 - tp).wait_send()
        remote(stat_all.at[z], stat_all.at[z], st_s.at[0, block], st_r.at[z], tp=1 - tp).wait_send()
    for block in range(n_sp):
        remote(stat_all.at[z], stat_all.at[z], st_s.at[1, block], st_r.at[z], tp=1 - tp).wait_send()
    for copy in sent:
        copy.wait()


def layer_call(n_sp, n_fs, n_tp, width, heads, blk, tokens, gain, w_ins, off, ck, cgain, wa, wc):
    rows, features = tokens.shape
    depth = w_ins[0].shape[0]
    o_rows, o_cols = wa.shape
    length, n = rows * n_sp * n_tp, n_sp * n_tp
    tiles = blk // rows
    dma = pltpu.SemaphoreType.DMA
    vmem = pltpu.VMEM
    result = jax.ShapeDtypeStruct((rows, n_fs * o_cols), BF16)
    return pl.pallas_call(
        functools.partial(layer_body, n_sp, n_tp, width, heads, ck.shape[0], blk),
        out_shape=[result, result],
        in_specs=[ANY] * 12,
        out_specs=[ANY] * 2,
        scratch_shapes=[
            vmem((length, features), BF16),
            vmem((n_fs * depth, 5 * width), BF16),
            vmem((n_fs, 2 * o_rows, o_cols), BF16),
            vmem((n_sp,) + off.shape, BF16),
            vmem((n_sp,) + off.shape, F32),
            vmem((ck.shape[0], width), F32),
            vmem(gain.shape, F32),
            vmem(cgain.shape, F32),
            vmem((n_sp, heads * blk, width), BF16),
            vmem((length, width), BF16),
            vmem((length, width), BF16),
            vmem((length + 32, width), F32),
            vmem((n_sp, heads * blk, 1), F32),
            vmem((n_sp, heads * blk, width), F32),
            vmem((length, width), BF16),
            vmem((length, width), BF16),
            vmem((length // rows, 8, rows), F32),
            vmem((2 * n_sp, blk, width), BF16),
            vmem((n, tiles, 8, rows), F32),
            vmem((blk, 2 * n_sp * width), BF16),
            vmem((n_fs, blk, o_cols), BF16),
            dma((12,)),
            dma((n_sp - 1, 2)), dma((n_sp - 1, 2)), dma((n_sp - 1, 2)), dma((n_sp - 1, 2)),
            dma((n_sp, 2)), dma((n_sp, 2)),
            dma((6,)), dma((6,)),
            dma((n_sp - 1,)), dma((n_sp - 1,)),
            dma((26,)), dma((26,)),
            dma((2, n_sp)), dma((2, n_sp)),
            dma((2, n_sp)), dma((n,)),
            dma((n_fs,)), dma((n_fs,)), dma((n_fs,)),
        ],
        compiler_params=pltpu.CompilerParams(collective_id=0, has_side_effects=True),
        name="layer",
    )(tokens, gain, *w_ins, off, ck, cgain, wa, wc)


def spread_shards(
    tokens,
    norm_gain,
    w_query,
    w_key,
    w_value,
    w_conv_value,
    w_conv_gate,
    key_offset,
    conv_kernel,
    conv_gain,
    w_attn_out,
    w_conv_out,
):
    n_sp, n_fs, n_tp = (lax.axis_size(a) for a in ("sp", "fs", "tp"))
    width = w_query.shape[1] // n_sp
    own, got = layer_call(
        n_sp, n_fs, n_tp, width, width // HD, key_offset.shape[0], tokens[0], norm_gain[None],
        (w_query, w_key, w_value, w_conv_value, w_conv_gate), jnp.transpose(key_offset),
        conv_kernel, conv_gain[None], w_attn_out, w_conv_out,
    )
    return (own.astype(F32) + got.astype(F32)).astype(BF16)[None]


def shifted(block, axis, distance):
    devices = range(lax.axis_size(axis))
    route = [(i - distance, i) for i in devices if i - distance in devices]
    return lax.ppermute(block, axis, route)


def piece_terms(queries, key_rows, value_rows, offsets, carry_log, allowed):
    head_size = queries.shape[2]
    logits = jnp.einsum(
        "qhd,khd->hqk", queries, key_rows, preferred_element_type=jnp.float32
    ) * head_size ** (-0.5)
    logits = logits + jnp.transpose(offsets.astype(jnp.float32))[:, None, :]
    log_keep = jax.nn.log_sigmoid(-logits)
    if allowed is not None:
        log_keep = jnp.where(allowed[None], log_keep, 0.0)
    between = lax.cumsum(log_keep, axis=2, reverse=True) - log_keep
    weights = jnp.exp(jax.nn.log_sigmoid(logits) + between + carry_log[:, :, None])
    if allowed is not None:
        weights = jnp.where(allowed[None], weights, 0.0)
    result = jnp.einsum(
        "hqk,khd->qhd", weights.astype(jnp.bfloat16), value_rows, preferred_element_type=jnp.float32
    )
    return (result, carry_log + jnp.sum(log_keep, axis=2))


def shards(
    tokens,
    norm_gain,
    w_query,
    w_key,
    w_value,
    w_conv_value,
    w_conv_gate,
    key_offset,
    conv_kernel,
    conv_gain,
    w_attn_out,
    w_conv_out,
):
    gathered = (
        lax.all_gather(w_query, "fs", axis=0, tiled=True),
        lax.all_gather(w_key, "fs", axis=0, tiled=True),
        lax.all_gather(w_value, "fs", axis=0, tiled=True),
        lax.all_gather(w_conv_value, "fs", axis=0, tiled=True),
        lax.all_gather(w_conv_gate, "fs", axis=0, tiled=True),
    )
    floats = lax.all_gather(tokens[0], "tp", axis=0, tiled=True).astype(jnp.float32)
    normed = (
        floats * lax.rsqrt(jnp.mean(floats * floats, axis=1, keepdims=True) + 1e-06) * norm_gain
    ).astype(jnp.bfloat16)
    projected = jnp.concatenate(
        [
            jnp.dot(normed, weight, preferred_element_type=jnp.float32).astype(jnp.bfloat16)
            for weight in gathered
        ],
        axis=1,
    )
    head_cols = w_query.shape[1]
    channels = w_conv_value.shape[1]
    block_len = projected.shape[0]
    local_heads = head_cols // HD
    queries = projected[:, :head_cols].reshape(block_len, local_heads, HD)
    key_flat = projected[:, head_cols : 2 * head_cols]
    value_flat = projected[:, 2 * head_cols : 3 * head_cols]
    conv_value = projected[:, 3 * head_cols : 3 * head_cols + channels]
    conv_gate = projected[:, 3 * head_cols + channels :]
    position = lax.axis_index("sp")
    positions = jnp.arange(block_len, dtype=jnp.int32)
    causal = positions[None, :] < positions[:, None]
    start_log = jnp.zeros((local_heads, block_len), jnp.float32)
    totals, carry_log = piece_terms(
        queries,
        key_flat.reshape(block_len, local_heads, HD),
        value_flat.reshape(block_len, local_heads, HD),
        key_offset,
        start_log,
        causal,
    )

    def visit(hop_count, carried):
        running, running_log, moving = carried
        moving = shifted((moving[0], moving[1], moving[2]), "sp", 1)
        result, next_log = piece_terms(
            queries,
            moving[0].reshape(block_len, local_heads, HD),
            moving[1].reshape(block_len, local_heads, HD),
            moving[2],
            running_log,
            None,
        )
        active = position >= hop_count
        running = jnp.where(active, running + result, running)
        running_log = jnp.where(active, next_log, running_log)
        return (running, running_log, moving)

    totals, carry_log, leftover = lax.fori_loop(
        1, lax.axis_size("sp"), visit, (totals, carry_log, (key_flat, value_flat, key_offset))
    )
    attn_heads = totals.reshape(block_len, head_cols).astype(jnp.bfloat16)
    gated_input = (
        conv_value.astype(jnp.float32) * jax.nn.sigmoid(conv_gate.astype(jnp.float32))
    ).astype(jnp.bfloat16)
    kernel_len = conv_kernel.shape[0]
    edge_rows = shifted(gated_input[block_len - (kernel_len - 1) :], "sp", 1)
    extended = jnp.concatenate([edge_rows, gated_input], axis=0).astype(jnp.float32)
    conv_sum = jnp.zeros((block_len, channels), jnp.float32)
    for tap_index in range(kernel_len):
        conv_sum = conv_sum + conv_kernel[tap_index] * extended[tap_index : tap_index + block_len]
    channel_total = lax.psum(jnp.sum(conv_sum, axis=1), "tp")
    centred = conv_sum - (channel_total / CC)[:, None]
    spread = lax.psum(jnp.sum(centred * centred, axis=1), "tp") / CC
    conv_hidden = jax.nn.silu(centred * lax.rsqrt(spread + 1e-06)[:, None] * conv_gain).astype(
        jnp.bfloat16
    )
    attn_weight, conv_weight = (
        lax.all_gather(w_attn_out, "fs", axis=1, tiled=True),
        lax.all_gather(w_conv_out, "fs", axis=1, tiled=True),
    )
    partial_value = jnp.dot(attn_heads, attn_weight, preferred_element_type=jnp.float32)
    partial_value = partial_value + jnp.dot(
        conv_hidden, conv_weight, preferred_element_type=jnp.float32
    )
    mixed = lax.psum_scatter(
        lax.optimization_barrier(partial_value.astype(jnp.bfloat16))
        .astype(jnp.float32)
        .astype(jnp.bfloat16),
        "tp",
        scatter_dimension=0,
        tiled=True,
    )
    return mixed[None]


def solution(mesh):
    placed = (
        P("fs", ("sp", "tp"), None),
        P(),
        P("fs", "tp"),
        P("fs", "tp"),
        P("fs", "tp"),
        P("fs", "tp"),
        P("fs", "tp"),
        P("sp", "tp"),
        P(None, "tp"),
        P("tp"),
        P("tp", "fs"),
        P("tp", "fs"),
    )

    def fits(tokens, norm_gain, w_query, *rest):
        n_sp, n_fs, n_tp = mesh.shape["sp"], mesh.shape["fs"], mesh.shape["tp"]
        cols = w_query.shape[1] // n_tp
        return n_fs == 4 and n_tp == 2 and n_sp == 4 and rest[5].shape[0] <= 33 and cols % (128 * n_sp) == 0 and rest[2].shape[1] == w_query.shape[1] and (
            tokens.shape[1] % (128 * n_sp * n_tp) == 0
        )

    def program(*args):
        body = spread_shards if fits(*args) else shards
        return mapped(body)(*args)

    def mapped(body):
        return jax.shard_map(
            body, mesh=mesh, in_specs=placed, out_specs=P("fs", ("sp", "tp"), None), check_vma=False
        )

    return program
```

```python
import functools

import jax
import jax.numpy as jnp
from jax import lax
from jax.experimental import pallas as pl
from jax.experimental.pallas import tpu as pltpu
from jax.sharding import PartitionSpec as P

HD = 64
CC = 1024
MESH = pl.DeviceIdType.MESH
F32 = jnp.float32
BF16 = jnp.bfloat16


def remote(src, dst, send, recv, **where):
    return pltpu.make_async_remote_copy(
        src_ref=src, dst_ref=dst, send_sem=send, recv_sem=recv, device_id=where, device_id_type=MESH
    )


def greet(peers):
    barrier = pltpu.get_barrier_semaphore()
    for where in peers:
        pl.semaphore_signal(barrier, inc=1, device_id=where, device_id_type=MESH)
    pl.semaphore_wait(barrier, len(peers))


def plane(fs):
    y = (fs + 2) % 4
    return fs + 1 - 2 * (fs % 2), y, y + 1 - 2 * (y % 2)


ANY = pl.BlockSpec(memory_space=pl.ANY)


LOG2E = 1.4426950408889634


def aligned(start, size):
    return pl.ds(pl.multiple_of(start, size), size)


def layer_body(n_sp, n_tp, width, heads, taps, blk, *refs):
    tok_in, gain_in, w_ins, off_in, ck_in, cgain_in, wa_in, wc_in = refs[0], refs[1], refs[2:7], *refs[7:12]
    own_out, got_out = refs[12:14]
    tok, w, wout, off_raw, off, ck, gain, cgain = refs[14:22]
    queries, keys, values, gated, carry, running = refs[22:28]
    attn_out, conv_out, stat_out, x_all, stat_all, hidden, part = refs[28:35]
    ld, up_s, up_r, dn_s, dn_r, par_s, par_r, w_s, w_r, off_s, off_r = refs[35:46]
    o_s, o_r, x_s, x_r, st_s, st_r, part_s, part_r = refs[46:]
    rows = tok_in.shape[0]
    tiles = blk // rows
    sub = rows // 2
    depth = w_ins[0].shape[0]
    half = depth // 2
    o_rows, o_cols = wa_in.shape
    share = o_rows * 5 // 16 // 16 * 16
    small = o_rows // 2 - share
    z, fs, tp = lax.axis_index("sp"), lax.axis_index("fs"), lax.axis_index("tp")
    xn, yn, dg = plane(fs)
    n = n_sp * n_tp
    me = z * n_tp + tp

    own_rows = aligned((z * n_tp + tp) * rows, rows)
    loads = [pltpu.make_async_copy(tok_in, tok.at[own_rows], ld.at[0])]
    loads += [
        pltpu.make_async_copy(
            ref.at[:, aligned(z * width, width)],
            w.at[aligned(fs * depth, depth), pl.ds(k * width, width)],
            ld.at[1 + k],
        )
        for k, ref in enumerate(w_ins)
    ]
    loads += [
        pltpu.make_async_copy(wa_in, wout.at[fs, pl.ds(0, o_rows)], ld.at[6]),
        pltpu.make_async_copy(wc_in, wout.at[fs, pl.ds(o_rows, o_rows)], ld.at[7]),
        pltpu.make_async_copy(off_in, off_raw.at[z], ld.at[8]),
        pltpu.make_async_copy(ck_in.at[:, aligned(z * width, width)], ck, ld.at[9]),
        pltpu.make_async_copy(gain_in, gain, ld.at[10]),
        pltpu.make_async_copy(cgain_in, cgain, ld.at[11]),
    ]
    for copy in loads:
        copy.start()
    greet(
        [{"sp": (me + d) % n // n_tp, "tp": (me + d) % n % n_tp} for d in range(1, n)]
        + [{"fs": xn}, {"fs": yn}]
    )

    def piece_rows(block, core, p):
        return tok.at[aligned((block * n_tp + core) * rows + p * sub, sub)]

    def lift(block, dist, p):
        ref = piece_rows(block, tp, p)
        return remote(ref, ref, up_s.at[dist - 1, p], up_r.at[dist - 1, p], sp=(z + 1) % n_sp)

    def sink(block, dist, p):
        ref = piece_rows(block, tp, p)
        return remote(ref, ref, dn_s.at[dist - 1, p], dn_r.at[dist - 1, p], sp=(z + n_sp - 1) % n_sp)

    def across(block, p):
        ref = piece_rows(block, tp, p)
        return remote(ref, ref, par_s.at[block, p], par_r.at[block, p], tp=1 - tp)

    def from_partner(block, p):
        ref = piece_rows(block, 1 - tp, p)
        return remote(ref, ref, par_s.at[block, p], par_r.at[block, p], tp=1 - tp)

    def w_part(owner, h):
        return w.at[aligned(owner * depth + h * half, half)]

    def send_w(owner, h, sem, to):
        return remote(w_part(owner, h), w_part(owner, h), w_s.at[sem], w_r.at[sem], fs=to)

    mate = z + 1 - 2 * (z % 2)
    edge = jnp.logical_or(z == 0, z == n_sp - 1)

    def o_piece(owner, side, q):
        far = share + 2 * small
        start = (jnp.where(edge, 0, far), share, share + small, jnp.where(edge, far, 0))[q]
        size = share if q in (0, 3) else small
        return wout.at[owner, pl.ds(pl.multiple_of(side * o_rows + start, 16), size)]

    def send_o(owner, side, q, sem, **to):
        ref = o_piece(owner, side, q)
        return remote(ref, ref, o_s.at[sem], o_r.at[sem], **to)

    def send_side(owner, side, sem, to):
        ref = wout.at[owner, pl.ds(side * o_rows, o_rows)]
        return remote(ref, ref, o_s.at[sem], o_r.at[sem], fs=to)

    loads[0].wait()
    for p in range(2):
        @pl.when(z < n_sp - 1)
        def _():
            lift(z, 1, p).start()

        @pl.when(z > 0)
        def _():
            sink(z, 1, p).start()

    for k in range(5):
        loads[1 + k].wait()
    w_first = [send_w(fs, 0, 0, xn), send_w(fs, 1, 1, yn), send_w(fs, 1, 2, xn), send_w(fs, 0, 3, yn)]
    for copy in w_first:
        copy.start()
    for p in range(2):
        across(z, p).start()
    loads[8].wait()
    offs = [
        remote(off_raw.at[z], off_raw.at[z], off_s.at[d - 1], off_r.at[d - 1], sp=(z + d) % n_sp)
        for d in range(1, n_sp)
    ]
    for copy in offs:
        copy.start()
    w_relay = [send_w(xn, 0, 4, yn), send_w(yn, 1, 5, xn)]
    w_here = [(0, xn, 0), (1, yn, 1), (2, xn, 1), (3, yn, 0), (4, dg, 0), (5, dg, 1)]
    o_first = []
    for q in range(3):
        o_first += [send_o(fs, 0, q, q, fs=xn), send_o(fs, 1, q, 4 + q, fs=yn)]
    o_later = [send_o(fs, 0, 3, 3, fs=xn), send_o(fs, 1, 3, 7, fs=yn), send_side(fs, 1, 8, xn), send_side(fs, 0, 9, yn)]
    o_relay = [(send_o(xn, 0, q, 10 + q, fs=yn), send_o(yn, 1, q, 13 + q, fs=xn)) for q in range(3)]
    o_share = [send_o(dg, side, 0, 16 + side, sp=mate) for side in range(2)]

    def relay_o(q):
        send_o(xn, 0, q, q, fs=xn).wait_recv()
        send_o(yn, 1, q, 4 + q, fs=xn).wait_recv()
        for copy in o_relay[q]:
            copy.start()

    def share_o():
        for side in range(2):
            send_o(dg, side, 0, 10 + 3 * side, fs=xn).wait_recv()
            o_share[side].start()

    def token_hop(dist, p):
        @pl.when(z >= dist)
        def _():
            block = (z - dist + n_sp) % n_sp
            lift(block, dist, p).wait_recv()
            if dist < n_sp - 1:
                @pl.when(z < n_sp - 1)
                def _():
                    lift(block, dist + 1, p).start()
            across(block, p).start()

        @pl.when(z + dist < n_sp)
        def _():
            block = (z + dist) % n_sp
            sink(block, dist, p).wait_recv()
            if dist < n_sp - 1:
                @pl.when(z > 0)
                def _():
                    sink(block, dist + 1, p).start()
            across(block, p).start()

    def relay_w():
        for s, owner, h in w_here[:2]:
            send_w(owner, h, s, xn).wait_recv()
            w_relay[s].start()
        for copy in loads[6:8]:
            copy.wait()
        for copy in o_first:
            copy.start()

    gated[pl.ds(0, 32), :] = jnp.zeros((32, width), F32)
    for dist in range(1, n_sp - 1):
        token_hop(dist, 0)
        if dist == 1:
            relay_w()
        token_hop(dist, 1)
    if n_sp == 2:
        relay_w()
    for copy in loads[9:]:
        copy.wait()
    for s, owner, h in w_here[2:]:
        send_w(owner, h, s, xn).wait_recv()
    for copy in offs:
        copy.wait()
    off[...] = off_raw[...].astype(F32) * LOG2E

    lane = lax.broadcasted_iota(jnp.int32, (rows, width), 1)

    def project(block, p):
        def spots(c):
            return c * rows + p * sub

        x = jnp.concatenate(
            [tok[aligned(block * blk + spots(c), sub), :] for c in range(n_tp)], axis=0
        ).astype(F32)
        normed = (x * lax.rsqrt(jnp.mean(x * x, axis=1, keepdims=True) + 1e-06) * gain[...]).astype(BF16)
        out = jnp.dot(normed, w[...], preferred_element_type=F32).astype(BF16)
        q = out[:, :width].astype(F32) * HD ** (-0.5)
        masked = [
            jnp.where(jnp.logical_and(lane >= h * HD, lane < (h + 1) * HD), q, 0.0).astype(BF16) for h in range(heads)
        ]
        value = out[:, 3 * width : 4 * width].astype(F32)
        gate = out[:, 4 * width :].astype(F32)
        fresh = (value * jax.nn.sigmoid(gate)).astype(BF16).astype(F32)
        for c in range(n_tp):
            part_of = slice(c * sub, (c + 1) * sub)
            at = aligned(block * blk + spots(c), sub)
            for h in range(heads):
                queries[block, aligned(h * blk + spots(c), sub), :] = masked[h][part_of]
            keys[at, :] = out[part_of, width : 2 * width]
            values[at, :] = out[part_of, 2 * width : 3 * width]
            gated[pl.ds(pl.multiple_of(block * blk + spots(c) + 32, 32), sub), :] = fresh[part_of]

    def convolve(tile, _):
        base = pl.multiple_of(tile * rows, rows)
        total = jnp.zeros((rows, width), F32)
        for phase in range(8):
            span = rows + 8 if phase else rows
            lined = jnp.zeros((span, width), F32)
            for tap in range((phase + taps - 33) % 8, taps, 8):
                lined = lined + ck[tap : tap + 1, :] * gated[pl.ds(base + (33 - taps + tap - phase), span), :]
            total = total + lined[phase : phase + rows]
        mean = jnp.mean(total, axis=1, keepdims=True)
        local = total - mean
        conv_out[pl.ds(base, rows), :] = local.astype(BF16)
        spread = jnp.mean(local * local, axis=1, keepdims=True)
        stat_out[tile] = jnp.transpose(jnp.where(lane == 0, mean, spread))[:8]
        return 0

    def block_rows(i):
        return aligned(i * blk, blk)


    def ship(k, source, block):
        at = source.at[block_rows(block)]

        @pl.when(block == z)
        def _():
            x_all[k * n_sp + z] = at[...]

        @pl.when(block != z)
        def _():
            remote(at, x_all.at[k * n_sp + z], x_s.at[k, block], x_r.at[k, z], sp=block).start()


    def ship_stat(block):
        at = stat_out.at[pl.ds(block * tiles, tiles)]

        @pl.when(block == z)
        def _():
            stat_all[z] = at[...]

        @pl.when(block != z)
        def _():
            remote(at, stat_all.at[z], st_s.at[0, block], st_r.at[z], sp=block).start()

        remote(at, stat_all.at[n_sp + z], st_s.at[1, block], st_r.at[n_sp + z], sp=block, tp=1 - tp).start()

    wide = lax.broadcasted_iota(jnp.int32, (blk, width), 1)
    row = lax.broadcasted_iota(jnp.int32, (blk, blk), 0)
    col = lax.broadcasted_iota(jnp.int32, (blk, blk), 1)
    stacked = (heads, blk, blk)
    earlier = lax.broadcasted_iota(jnp.int32, stacked, 2) < lax.broadcasted_iota(jnp.int32, stacked, 1)
    earlier = earlier.reshape(heads * blk, blk)

    def attend(i, j, diagonal):
        k = keys[block_rows(j), :]
        v = values[block_rows(j), :]
        after = jnp.where(row >= col, 1.0, 0.0).astype(BF16)
        s = lax.dot_general(queries[i], k, (((1,), (1,)), ((), ())), preferred_element_type=F32)
        shift = jnp.concatenate(
            [jnp.broadcast_to(off[j, pl.ds(z * heads + h, 1), :], (blk, blk)) for h in range(heads)], axis=0
        )
        s = s * LOG2E + shift
        keep = jnp.minimum(-s, 0.0) - jnp.log2(1.0 + jnp.exp2(-jnp.abs(s)))
        if diagonal:
            keep = jnp.where(earlier, keep, 0.0)
        suffix = jnp.dot(keep.astype(BF16), after, preferred_element_type=F32)
        if diagonal:
            weights = jnp.where(earlier, jnp.exp2(s + suffix), 0.0)
            carry[i] = suffix[:, :1]
            running[i] = jnp.dot(weights.astype(BF16), v, preferred_element_type=F32)
        else:
            before = carry[i]
            weights = jnp.exp2(s + suffix + before)
            carry[i] = before + suffix[:, :1]
            running[i] += jnp.dot(weights.astype(BF16), v, preferred_element_type=F32)

        @pl.when(j == 0)
        def _():
            merged = running[i, :blk]
            for h in range(1, heads):
                merged = jnp.where(wide >= h * HD, running[i, h * blk : (h + 1) * blk], merged)
            attn_out[block_rows(i), :] = merged.astype(BF16)
            ship(0, attn_out, i)

    def step(s, _):
        rising = z < n_sp - 1
        block = jnp.where(rising, s, n_sp - 1 - s)

        def half_block(p, _):
            @pl.when(jnp.logical_and(s == n_sp - 1, edge))
            def _():
                @pl.when(p == 1)
                def _():
                    share_o()

                token_hop(n_sp - 1, p)

            from_partner(block, p).wait_recv()
            project(block, p)
            return 0

        lax.fori_loop(0, 2, half_block, 0)

        @pl.when(s == n_sp - 3)
        def _():
            relay_o(0)
            for copy in o_later:
                copy.start()

        @pl.when(s == n_sp - 2)
        def _():
            for q in (1, 2):
                relay_o(q)

        lax.fori_loop(block * tiles + 1, block * tiles + tiles, convolve, 0)

        def conv_block(u, _):
            target = jnp.where(rising, block, jnp.where(jnp.logical_and(u == 0, s > 0), block + 1, 0))
            convolve(target * tiles, 0)
            ship(1, conv_out, target)
            ship_stat(target)
            return 0

        falling_count = jnp.where(s > 0, 1, 0) + jnp.where(block == 0, 1, 0)
        lax.fori_loop(0, jnp.where(rising, 1, falling_count), conv_block, 0)
        attend(block, block, True)

        def further(t, _):
            attend(jnp.where(rising, block, block + t), jnp.where(rising, block - t, block), False)
            return 0

        lax.fori_loop(1, s + 1, further, 0)
        return 0

    lax.fori_loop(0, n_sp, step, 0)


    @pl.when(jnp.logical_not(edge))
    def _():
        share_o()

    others = [(z + d) % n_sp for d in range(1, n_sp)]

    def stat_from(slot):
        return remote(stat_all.at[slot], stat_all.at[slot], st_s.at[0, z], st_r.at[slot], tp=1 - tp)

    def x_from(k, source):
        ref = x_all.at[k * n_sp + source]
        return remote(ref, ref, x_s.at[k, z], x_r.at[k, source], tp=1 - tp)

    for source in others:
        stat_from(source).wait_recv()
    for source in range(n_sp):
        stat_from(n_sp + source).wait_recv()
    for source in others:
        x_from(1, source).wait_recv()
    kind = lax.broadcasted_iota(jnp.int32, (rows, n * 8), 1) % 8
    for t in range(tiles):
        stats = jnp.transpose(stat_all[:, t].reshape(n * 8, rows))
        mean = jnp.sum(jnp.where(kind == 0, stats, 0.0), axis=1, keepdims=True) / n
        off_mean = stats - mean
        spread = jnp.where(kind == 0, off_mean * off_mean, jnp.where(kind == 1, stats, 0.0))
        scale = lax.rsqrt(jnp.sum(spread, axis=1, keepdims=True) / n + 1e-06)
        at = pl.ds(t * rows, rows)
        for g in range(n_sp):
            x = x_all[n_sp + g, at, :].astype(F32) + off_mean[:, 8 * g : 8 * g + 1]
            y = x * scale * cgain[:, g * width : (g + 1) * width]
            hidden[at, (n_sp + g) * width : (n_sp + g + 1) * width] = (y * jax.nn.sigmoid(y)).astype(BF16)
    for source in others:
        x_from(0, source).wait_recv()
    for g in range(n_sp):
        hidden[:, g * width : (g + 1) * width] = x_all[g]

    sent = []
    for index, owner in enumerate((fs, xn, yn, dg)):
        if owner is xn:
            send_o(xn, 0, 3, 3, fs=xn).wait_recv()
            send_side(xn, 1, 8, xn).wait_recv()
        elif owner is yn:
            send_o(yn, 1, 3, 7, fs=xn).wait_recv()
            send_side(yn, 0, 9, xn).wait_recv()
        elif owner is dg:
            for side in range(2):
                for q in (1, 2):
                    send_o(dg, side, q, 10 + 3 * side + q, fs=xn).wait_recv()
                send_o(dg, side, 3, 16 + side, sp=mate).wait_recv()
        part[index] = jnp.dot(hidden[...], wout[owner], preferred_element_type=F32).astype(BF16)
        cols = aligned(owner * o_cols, o_cols)
        give = remote(
            part.at[index, aligned((1 - tp) * rows, rows)], got_out.at[:, cols],
            part_s.at[index], part_r.at[index], tp=1 - tp,
        )
        give.start()
        own_out[:, cols] = part[index, aligned(tp * rows, rows), :]
        sent.append(give)

    for copy in w_first + w_relay + o_first + o_later + o_share:
        copy.wait_send()
    for pair in o_relay:
        for copy in pair:
            copy.wait_send()
    for p in range(2):
        for dist in range(1, n_sp):
            @pl.when(jnp.logical_and(z < n_sp - 1, z >= dist - 1))
            def _():
                lift(z, dist, p).wait_send()

            @pl.when(jnp.logical_and(z > 0, z + dist - 1 < n_sp))
            def _():
                sink(z, dist, p).wait_send()

        for block in range(n_sp):
            across(block, p).wait_send()
    for block in others:
        for k in range(2):
            remote(x_all.at[k], x_all.at[k], x_s.at[k, block], x_r.at[k, z], tp=1 - tp).wait_send()
        remote(stat_all.at[z], stat_all.at[z], st_s.at[0, block], st_r.at[z], tp=1 - tp).wait_send()
    for block in range(n_sp):
        remote(stat_all.at[z], stat_all.at[z], st_s.at[1, block], st_r.at[z], tp=1 - tp).wait_send()
    for copy in sent:
        copy.wait()


def layer_call(n_sp, n_fs, n_tp, width, heads, blk, tokens, gain, w_ins, off, ck, cgain, wa, wc):
    rows, features = tokens.shape
    depth = w_ins[0].shape[0]
    o_rows, o_cols = wa.shape
    length, n = rows * n_sp * n_tp, n_sp * n_tp
    tiles = blk // rows
    dma = pltpu.SemaphoreType.DMA
    vmem = pltpu.VMEM
    result = vmem((rows, n_fs * o_cols), BF16)
    return pl.pallas_call(
        functools.partial(layer_body, n_sp, n_tp, width, heads, ck.shape[0], blk),
        out_shape=[result, result],
        in_specs=[ANY] * 12,
        out_specs=[pl.BlockSpec(memory_space=pltpu.VMEM)] * 2,
        scratch_shapes=[
            vmem((length, features), BF16),
            vmem((n_fs * depth, 5 * width), BF16),
            vmem((n_fs, 2 * o_rows, o_cols), BF16),
            vmem((n_sp,) + off.shape, BF16),
            vmem((n_sp,) + off.shape, F32),
            vmem((ck.shape[0], width), F32),
            vmem(gain.shape, F32),
            vmem(cgain.shape, F32),
            vmem((n_sp, heads * blk, width), BF16),
            vmem((length, width), BF16),
            vmem((length, width), BF16),
            vmem((length + 32, width), F32),
            vmem((n_sp, heads * blk, 1), F32),
            vmem((n_sp, heads * blk, width), F32),
            vmem((length, width), BF16),
            vmem((length, width), BF16),
            vmem((length // rows, 8, rows), F32),
            vmem((2 * n_sp, blk, width), BF16),
            vmem((n, tiles, 8, rows), F32),
            vmem((blk, 2 * n_sp * width), BF16),
            vmem((n_fs, blk, o_cols), BF16),
            dma((12,)),
            dma((n_sp - 1, 2)), dma((n_sp - 1, 2)), dma((n_sp - 1, 2)), dma((n_sp - 1, 2)),
            dma((n_sp, 2)), dma((n_sp, 2)),
            dma((6,)), dma((6,)),
            dma((n_sp - 1,)), dma((n_sp - 1,)),
            dma((18,)), dma((18,)),
            dma((2, n_sp)), dma((2, n_sp)),
            dma((2, n_sp)), dma((n,)),
            dma((n_fs,)), dma((n_fs,)),
        ],
        compiler_params=pltpu.CompilerParams(collective_id=0, has_side_effects=True),
        name="layer",
    )(tokens, gain, *w_ins, off, ck, cgain, wa, wc)


def spread_shards(
    tokens,
    norm_gain,
    w_query,
    w_key,
    w_value,
    w_conv_value,
    w_conv_gate,
    key_offset,
    conv_kernel,
    conv_gain,
    w_attn_out,
    w_conv_out,
):
    n_sp, n_fs, n_tp = (lax.axis_size(a) for a in ("sp", "fs", "tp"))
    width = w_query.shape[1] // n_sp
    own, got = layer_call(
        n_sp, n_fs, n_tp, width, width // HD, key_offset.shape[0], tokens[0], norm_gain[None],
        (w_query, w_key, w_value, w_conv_value, w_conv_gate), jnp.transpose(key_offset),
        conv_kernel, conv_gain[None], w_attn_out, w_conv_out,
    )
    return (own.astype(F32) + got.astype(F32)).astype(BF16)[None]


def shifted(block, axis, distance):
    devices = range(lax.axis_size(axis))
    route = [(i - distance, i) for i in devices if i - distance in devices]
    return lax.ppermute(block, axis, route)


def piece_terms(queries, key_rows, value_rows, offsets, carry_log, allowed):
    head_size = queries.shape[2]
    logits = jnp.einsum(
        "qhd,khd->hqk", queries, key_rows, preferred_element_type=jnp.float32
    ) * head_size ** (-0.5)
    logits = logits + jnp.transpose(offsets.astype(jnp.float32))[:, None, :]
    log_keep = jax.nn.log_sigmoid(-logits)
    if allowed is not None:
        log_keep = jnp.where(allowed[None], log_keep, 0.0)
    between = lax.cumsum(log_keep, axis=2, reverse=True) - log_keep
    weights = jnp.exp(jax.nn.log_sigmoid(logits) + between + carry_log[:, :, None])
    if allowed is not None:
        weights = jnp.where(allowed[None], weights, 0.0)
    result = jnp.einsum(
        "hqk,khd->qhd", weights.astype(jnp.bfloat16), value_rows, preferred_element_type=jnp.float32
    )
    return (result, carry_log + jnp.sum(log_keep, axis=2))


def shards(
    tokens,
    norm_gain,
    w_query,
    w_key,
    w_value,
    w_conv_value,
    w_conv_gate,
    key_offset,
    conv_kernel,
    conv_gain,
    w_attn_out,
    w_conv_out,
):
    gathered = (
        lax.all_gather(w_query, "fs", axis=0, tiled=True),
        lax.all_gather(w_key, "fs", axis=0, tiled=True),
        lax.all_gather(w_value, "fs", axis=0, tiled=True),
        lax.all_gather(w_conv_value, "fs", axis=0, tiled=True),
        lax.all_gather(w_conv_gate, "fs", axis=0, tiled=True),
    )
    floats = lax.all_gather(tokens[0], "tp", axis=0, tiled=True).astype(jnp.float32)
    normed = (
        floats * lax.rsqrt(jnp.mean(floats * floats, axis=1, keepdims=True) + 1e-06) * norm_gain
    ).astype(jnp.bfloat16)
    projected = jnp.concatenate(
        [
            jnp.dot(normed, weight, preferred_element_type=jnp.float32).astype(jnp.bfloat16)
            for weight in gathered
        ],
        axis=1,
    )
    head_cols = w_query.shape[1]
    channels = w_conv_value.shape[1]
    block_len = projected.shape[0]
    local_heads = head_cols // HD
    queries = projected[:, :head_cols].reshape(block_len, local_heads, HD)
    key_flat = projected[:, head_cols : 2 * head_cols]
    value_flat = projected[:, 2 * head_cols : 3 * head_cols]
    conv_value = projected[:, 3 * head_cols : 3 * head_cols + channels]
    conv_gate = projected[:, 3 * head_cols + channels :]
    position = lax.axis_index("sp")
    positions = jnp.arange(block_len, dtype=jnp.int32)
    causal = positions[None, :] < positions[:, None]
    start_log = jnp.zeros((local_heads, block_len), jnp.float32)
    totals, carry_log = piece_terms(
        queries,
        key_flat.reshape(block_len, local_heads, HD),
        value_flat.reshape(block_len, local_heads, HD),
        key_offset,
        start_log,
        causal,
    )

    def visit(hop_count, carried):
        running, running_log, moving = carried
        moving = shifted((moving[0], moving[1], moving[2]), "sp", 1)
        result, next_log = piece_terms(
            queries,
            moving[0].reshape(block_len, local_heads, HD),
            moving[1].reshape(block_len, local_heads, HD),
            moving[2],
            running_log,
            None,
        )
        active = position >= hop_count
        running = jnp.where(active, running + result, running)
        running_log = jnp.where(active, next_log, running_log)
        return (running, running_log, moving)

    totals, carry_log, leftover = lax.fori_loop(
        1, lax.axis_size("sp"), visit, (totals, carry_log, (key_flat, value_flat, key_offset))
    )
    attn_heads = totals.reshape(block_len, head_cols).astype(jnp.bfloat16)
    gated_input = (
        conv_value.astype(jnp.float32) * jax.nn.sigmoid(conv_gate.astype(jnp.float32))
    ).astype(jnp.bfloat16)
    kernel_len = conv_kernel.shape[0]
    edge_rows = shifted(gated_input[block_len - (kernel_len - 1) :], "sp", 1)
    extended = jnp.concatenate([edge_rows, gated_input], axis=0).astype(jnp.float32)
    conv_sum = jnp.zeros((block_len, channels), jnp.float32)
    for tap_index in range(kernel_len):
        conv_sum = conv_sum + conv_kernel[tap_index] * extended[tap_index : tap_index + block_len]
    channel_total = lax.psum(jnp.sum(conv_sum, axis=1), "tp")
    centred = conv_sum - (channel_total / CC)[:, None]
    spread = lax.psum(jnp.sum(centred * centred, axis=1), "tp") / CC
    conv_hidden = jax.nn.silu(centred * lax.rsqrt(spread + 1e-06)[:, None] * conv_gain).astype(
        jnp.bfloat16
    )
    attn_weight, conv_weight = (
        lax.all_gather(w_attn_out, "fs", axis=1, tiled=True),
        lax.all_gather(w_conv_out, "fs", axis=1, tiled=True),
    )
    partial_value = jnp.dot(attn_heads, attn_weight, preferred_element_type=jnp.float32)
    partial_value = partial_value + jnp.dot(
        conv_hidden, conv_weight, preferred_element_type=jnp.float32
    )
    mixed = lax.psum_scatter(
        lax.optimization_barrier(partial_value.astype(jnp.bfloat16))
        .astype(jnp.float32)
        .astype(jnp.bfloat16),
        "tp",
        scatter_dimension=0,
        tiled=True,
    )
    return mixed[None]


def solution(mesh):
    placed = (
        P("fs", ("sp", "tp"), None),
        P(),
        P("fs", "tp"),
        P("fs", "tp"),
        P("fs", "tp"),
        P("fs", "tp"),
        P("fs", "tp"),
        P("sp", "tp"),
        P(None, "tp"),
        P("tp"),
        P("tp", "fs"),
        P("tp", "fs"),
    )

    def fits(tokens, norm_gain, w_query, *rest):
        n_sp, n_fs, n_tp = mesh.shape["sp"], mesh.shape["fs"], mesh.shape["tp"]
        cols = w_query.shape[1] // n_tp
        return n_fs == 4 and n_tp == 2 and n_sp == 4 and rest[5].shape[0] <= 33 and cols % (128 * n_sp) == 0 and rest[2].shape[1] == w_query.shape[1] and (
            tokens.shape[1] % (128 * n_sp * n_tp) == 0
        )

    def program(*args):
        body = spread_shards if fits(*args) else shards
        return mapped(body)(*args)

    def mapped(body):
        return jax.shard_map(
            body, mesh=mesh, in_specs=placed, out_specs=P("fs", ("sp", "tp"), None), check_vma=False
        )

    return program
```

```python
import functools

import jax
import jax.numpy as jnp
from jax import lax
from jax.experimental import pallas as pl
from jax.experimental.pallas import tpu as pltpu
from jax.sharding import PartitionSpec as P

HD = 64
CC = 1024
MESH = pl.DeviceIdType.MESH
F32 = jnp.float32
BF16 = jnp.bfloat16


def remote(src, dst, send, recv, **where):
    return pltpu.make_async_remote_copy(
        src_ref=src, dst_ref=dst, send_sem=send, recv_sem=recv, device_id=where, device_id_type=MESH
    )


def greet(peers):
    barrier = pltpu.get_barrier_semaphore()
    for where in peers:
        pl.semaphore_signal(barrier, inc=1, device_id=where, device_id_type=MESH)
    pl.semaphore_wait(barrier, len(peers))


def plane(fs):
    y = (fs + 2) % 4
    return fs + 1 - 2 * (fs % 2), y, y + 1 - 2 * (y % 2)


ANY = pl.BlockSpec(memory_space=pl.ANY)


LOG2E = 1.4426950408889634


def aligned(start, size):
    return pl.ds(pl.multiple_of(start, size), size)


def layer_body(n_sp, n_tp, width, heads, taps, blk, *refs):
    tok_in, gain_in, w_ins, off_in, ck_in, cgain_in, wa_in, wc_in = refs[0], refs[1], refs[2:7], *refs[7:12]
    own_out, got_out = refs[12:14]
    tok, w, wout, off_raw, off, ck, gain, cgain = refs[14:22]
    queries, keys, values, gated, carry, running = refs[22:28]
    attn_out, conv_out, stat_out, x_all, stat_all, hidden, part = refs[28:35]
    ld, up_s, up_r, dn_s, dn_r, par_s, par_r, w_s, w_r, off_s, off_r = refs[35:46]
    o_s, o_r, x_s, x_r, st_s, st_r, part_s, part_r = refs[46:]
    rows = tok_in.shape[0]
    tiles = blk // rows
    sub = rows // 2
    depth = w_ins[0].shape[0]
    half = depth // 2
    o_rows, o_cols = wa_in.shape
    share = o_rows * 5 // 16 // 16 * 16
    small = o_rows // 2 - share
    z, fs, tp = lax.axis_index("sp"), lax.axis_index("fs"), lax.axis_index("tp")
    xn, yn, dg = plane(fs)
    n = n_sp * n_tp
    me = z * n_tp + tp

    own_rows = aligned((z * n_tp + tp) * rows, rows)
    loads = [pltpu.make_async_copy(tok_in, tok.at[own_rows], ld.at[0])]
    loads += [
        pltpu.make_async_copy(
            ref.at[:, aligned(z * width, width)],
            w.at[aligned(fs * depth, depth), pl.ds(k * width, width)],
            ld.at[1 + k],
        )
        for k, ref in enumerate(w_ins)
    ]
    loads += [
        pltpu.make_async_copy(wa_in, wout.at[fs, pl.ds(0, o_rows)], ld.at[6]),
        pltpu.make_async_copy(wc_in, wout.at[fs, pl.ds(o_rows, o_rows)], ld.at[7]),
        pltpu.make_async_copy(off_in, off_raw.at[z], ld.at[8]),
        pltpu.make_async_copy(ck_in.at[:, aligned(z * width, width)], ck, ld.at[9]),
        pltpu.make_async_copy(gain_in, gain, ld.at[10]),
        pltpu.make_async_copy(cgain_in, cgain, ld.at[11]),
    ]
    for copy in loads:
        copy.start()
    barrier = pltpu.get_barrier_semaphore()

    def hello(**where):
        pl.semaphore_signal(barrier, inc=1, device_id=where, device_id_type=MESH)

    hello(fs=xn)
    hello(fs=yn)
    hello(tp=1 - tp)

    @pl.when(z > 0)
    def _():
        hello(sp=z - 1)

    @pl.when(z < n_sp - 1)
    def _():
        hello(sp=z + 1)

    pl.semaphore_wait(barrier, 4 + jnp.where(jnp.logical_and(z > 0, z < n_sp - 1), 1, 0))

    def piece_rows(block, core, p):
        return tok.at[aligned((block * n_tp + core) * rows + p * sub, sub)]

    def lift(block, dist, p):
        ref = piece_rows(block, tp, p)
        return remote(ref, ref, up_s.at[dist - 1, p], up_r.at[dist - 1, p], sp=(z + 1) % n_sp)

    def sink(block, dist, p):
        ref = piece_rows(block, tp, p)
        return remote(ref, ref, dn_s.at[dist - 1, p], dn_r.at[dist - 1, p], sp=(z + n_sp - 1) % n_sp)

    def lift_off(block, dist):
        ref = off_raw.at[block]
        return remote(ref, ref, off_s.at[0, dist - 1], off_r.at[0, dist - 1], sp=(z + 1) % n_sp)

    def sink_off(block, dist):
        ref = off_raw.at[block]
        return remote(ref, ref, off_s.at[1, dist - 1], off_r.at[1, dist - 1], sp=(z + n_sp - 1) % n_sp)

    def across(block, p):
        ref = piece_rows(block, tp, p)
        return remote(ref, ref, par_s.at[block, p], par_r.at[block, p], tp=1 - tp)

    def from_partner(block, p):
        ref = piece_rows(block, 1 - tp, p)
        return remote(ref, ref, par_s.at[block, p], par_r.at[block, p], tp=1 - tp)

    def w_part(owner, h):
        return w.at[aligned(owner * depth + h * half, half)]

    def send_w(owner, h, sem, to):
        return remote(w_part(owner, h), w_part(owner, h), w_s.at[sem], w_r.at[sem], fs=to)

    mate = z + 1 - 2 * (z % 2)
    edge = jnp.logical_or(z == 0, z == n_sp - 1)

    def o_piece(owner, side, q):
        far = share + 2 * small
        start = (jnp.where(edge, 0, far), share, share + small, jnp.where(edge, far, 0))[q]
        size = share if q in (0, 3) else small
        return wout.at[owner, pl.ds(pl.multiple_of(side * o_rows + start, 16), size)]

    def send_o(owner, side, q, sem, **to):
        ref = o_piece(owner, side, q)
        return remote(ref, ref, o_s.at[sem], o_r.at[sem], **to)

    def send_side(owner, side, sem, to):
        ref = wout.at[owner, pl.ds(side * o_rows, o_rows)]
        return remote(ref, ref, o_s.at[sem], o_r.at[sem], fs=to)

    loads[0].wait()
    for p in range(2):
        @pl.when(z < n_sp - 1)
        def _():
            lift(z, 1, p).start()

        @pl.when(z > 0)
        def _():
            sink(z, 1, p).start()

    for k in range(5):
        loads[1 + k].wait()
    w_first = [send_w(fs, 0, 0, xn), send_w(fs, 1, 1, yn), send_w(fs, 1, 2, xn), send_w(fs, 0, 3, yn)]
    for copy in w_first:
        copy.start()
    for p in range(2):
        across(z, p).start()
    loads[8].wait()

    @pl.when(z < n_sp - 1)
    def _():
        lift_off(z, 1).start()

    @pl.when(z > 0)
    def _():
        sink_off(z, 1).start()

    w_relay = [send_w(xn, 0, 4, yn), send_w(yn, 1, 5, xn)]
    w_here = [(0, xn, 0), (1, yn, 1), (2, xn, 1), (3, yn, 0), (4, dg, 0), (5, dg, 1)]
    o_first = []
    for q in range(3):
        o_first += [send_o(fs, 0, q, q, fs=xn), send_o(fs, 1, q, 4 + q, fs=yn)]
    o_later = [send_o(fs, 0, 3, 3, fs=xn), send_o(fs, 1, 3, 7, fs=yn), send_side(fs, 1, 8, xn), send_side(fs, 0, 9, yn)]
    o_relay = [(send_o(xn, 0, q, 10 + q, fs=yn), send_o(yn, 1, q, 13 + q, fs=xn)) for q in range(3)]
    o_share = [send_o(dg, side, 0, 16 + side, sp=mate) for side in range(2)]

    def relay_o(q):
        send_o(xn, 0, q, q, fs=xn).wait_recv()
        send_o(yn, 1, q, 4 + q, fs=xn).wait_recv()
        for copy in o_relay[q]:
            copy.start()

    def share_o():
        for side in range(2):
            send_o(dg, side, 0, 10 + 3 * side, fs=xn).wait_recv()
            o_share[side].start()

    def token_hop(dist, p):
        @pl.when(z >= dist)
        def _():
            block = (z - dist + n_sp) % n_sp
            lift(block, dist, p).wait_recv()
            if dist < n_sp - 1:
                @pl.when(z < n_sp - 1)
                def _():
                    lift(block, dist + 1, p).start()
            across(block, p).start()

        @pl.when(z + dist < n_sp)
        def _():
            block = (z + dist) % n_sp
            sink(block, dist, p).wait_recv()
            if dist < n_sp - 1:
                @pl.when(z > 0)
                def _():
                    sink(block, dist + 1, p).start()
            across(block, p).start()

    def offset_hop(dist):
        @pl.when(z >= dist)
        def _():
            block = (z - dist + n_sp) % n_sp
            lift_off(block, dist).wait_recv()
            if dist < n_sp - 1:
                @pl.when(z < n_sp - 1)
                def _():
                    lift_off(block, dist + 1).start()

        @pl.when(z + dist < n_sp)
        def _():
            block = (z + dist) % n_sp
            sink_off(block, dist).wait_recv()
            if dist < n_sp - 1:
                @pl.when(z > 0)
                def _():
                    sink_off(block, dist + 1).start()

    def relay_w():
        for s, owner, h in w_here[:2]:
            send_w(owner, h, s, xn).wait_recv()
            w_relay[s].start()
        for copy in loads[6:8]:
            copy.wait()
        for copy in o_first:
            copy.start()

    gated[pl.ds(0, 32), :] = jnp.zeros((32, width), F32)
    for dist in range(1, n_sp - 1):
        token_hop(dist, 0)
        offset_hop(dist)
        if dist == 1:
            relay_w()
        token_hop(dist, 1)
    if n_sp == 2:
        relay_w()
    for copy in loads[9:]:
        copy.wait()
    for s, owner, h in w_here[2:]:
        send_w(owner, h, s, xn).wait_recv()

    lane = lax.broadcasted_iota(jnp.int32, (rows, width), 1)

    def project(block, p):
        def spots(c):
            return c * rows + p * sub

        x = jnp.concatenate(
            [tok[aligned(block * blk + spots(c), sub), :] for c in range(n_tp)], axis=0
        ).astype(F32)
        normed = (x * lax.rsqrt(jnp.mean(x * x, axis=1, keepdims=True) + 1e-06) * gain[...]).astype(BF16)
        out = jnp.dot(normed, w[...], preferred_element_type=F32).astype(BF16)
        q = out[:, :width].astype(F32) * HD ** (-0.5)
        masked = [
            jnp.where(jnp.logical_and(lane >= h * HD, lane < (h + 1) * HD), q, 0.0).astype(BF16) for h in range(heads)
        ]
        value = out[:, 3 * width : 4 * width].astype(F32)
        gate = out[:, 4 * width :].astype(F32)
        fresh = (value * jax.nn.sigmoid(gate)).astype(BF16).astype(F32)
        for c in range(n_tp):
            part_of = slice(c * sub, (c + 1) * sub)
            at = aligned(block * blk + spots(c), sub)
            for h in range(heads):
                queries[block, aligned(h * blk + spots(c), sub), :] = masked[h][part_of]
            keys[at, :] = out[part_of, width : 2 * width]
            values[at, :] = out[part_of, 2 * width : 3 * width]
            gated[pl.ds(pl.multiple_of(block * blk + spots(c) + 32, 32), sub), :] = fresh[part_of]

    def convolve(tile, _):
        base = pl.multiple_of(tile * rows, rows)
        total = jnp.zeros((rows, width), F32)
        for phase in range(8):
            span = rows + 8 if phase else rows
            lined = jnp.zeros((span, width), F32)
            for tap in range((phase + taps - 33) % 8, taps, 8):
                lined = lined + ck[tap : tap + 1, :] * gated[pl.ds(base + (33 - taps + tap - phase), span), :]
            total = total + lined[phase : phase + rows]
        mean = jnp.mean(total, axis=1, keepdims=True)
        local = total - mean
        conv_out[pl.ds(base, rows), :] = local.astype(BF16)
        spread = jnp.mean(local * local, axis=1, keepdims=True)
        stat_out[tile] = jnp.transpose(jnp.where(lane == 0, mean, spread))[:8]
        return 0

    def block_rows(i):
        return aligned(i * blk, blk)


    def ship(k, source, block):
        at = source.at[block_rows(block)]

        @pl.when(block == z)
        def _():
            x_all[k * n_sp + z] = at[...]

        @pl.when(block != z)
        def _():
            remote(at, x_all.at[k * n_sp + z], x_s.at[k, block], x_r.at[k, z], sp=block).start()


    def ship_stat(block):
        at = stat_out.at[pl.ds(block * tiles, tiles)]

        @pl.when(block == z)
        def _():
            stat_all[z] = at[...]

        @pl.when(block != z)
        def _():
            remote(at, stat_all.at[z], st_s.at[0, block], st_r.at[z], sp=block).start()

        remote(at, stat_all.at[n_sp + z], st_s.at[1, block], st_r.at[n_sp + z], sp=block, tp=1 - tp).start()

    wide = lax.broadcasted_iota(jnp.int32, (blk, width), 1)
    row = lax.broadcasted_iota(jnp.int32, (blk, blk), 0)
    col = lax.broadcasted_iota(jnp.int32, (blk, blk), 1)
    stacked = (heads, blk, blk)
    earlier = lax.broadcasted_iota(jnp.int32, stacked, 2) < lax.broadcasted_iota(jnp.int32, stacked, 1)
    earlier = earlier.reshape(heads * blk, blk)

    def attend(i, j, diagonal):
        k = keys[block_rows(j), :]
        v = values[block_rows(j), :]
        after = jnp.where(row >= col, 1.0, 0.0).astype(BF16)
        s = lax.dot_general(queries[i], k, (((1,), (1,)), ((), ())), preferred_element_type=F32)
        shift = jnp.concatenate(
            [jnp.broadcast_to(off[j, pl.ds(z * heads + h, 1), :], (blk, blk)) for h in range(heads)], axis=0
        )
        s = s * LOG2E + shift
        keep = jnp.minimum(-s, 0.0) - jnp.log2(1.0 + jnp.exp2(-jnp.abs(s)))
        if diagonal:
            keep = jnp.where(earlier, keep, 0.0)
        suffix = jnp.dot(keep.astype(BF16), after, preferred_element_type=F32)
        if diagonal:
            weights = jnp.where(earlier, jnp.exp2(s + suffix), 0.0)
            carry[i] = suffix[:, :1]
            running[i] = jnp.dot(weights.astype(BF16), v, preferred_element_type=F32)
        else:
            before = carry[i]
            weights = jnp.exp2(s + suffix + before)
            carry[i] = before + suffix[:, :1]
            running[i] += jnp.dot(weights.astype(BF16), v, preferred_element_type=F32)

        @pl.when(j == 0)
        def _():
            merged = running[i, :blk]
            for h in range(1, heads):
                merged = jnp.where(wide >= h * HD, running[i, h * blk : (h + 1) * blk], merged)
            attn_out[block_rows(i), :] = merged.astype(BF16)
            ship(0, attn_out, i)

    def step(s, _):
        rising = z < n_sp - 2
        block = jnp.where(rising, s, n_sp - 1 - s)

        def half_block(p, _):
            @pl.when(jnp.logical_and(s == n_sp - 1, edge))
            def _():
                @pl.when(p == 1)
                def _():
                    share_o()

                token_hop(n_sp - 1, p)

            from_partner(block, p).wait_recv()
            project(block, p)
            return 0

        lax.fori_loop(0, 2, half_block, 0)

        @pl.when(jnp.logical_and(s == n_sp - 1, edge))
        def _():
            offset_hop(n_sp - 1)

        off[block] = off_raw[block].astype(F32) * LOG2E

        @pl.when(s == n_sp - 3)
        def _():
            relay_o(0)
            for copy in o_later:
                copy.start()

        @pl.when(s == n_sp - 2)
        def _():
            for q in (1, 2):
                relay_o(q)

        @pl.when(jnp.logical_and(s == n_sp - 1, jnp.logical_not(edge)))
        def _():
            share_o()

        lax.fori_loop(block * tiles + 1, block * tiles + tiles, convolve, 0)

        def conv_block(u, _):
            target = jnp.where(rising, block, jnp.where(jnp.logical_and(u == 0, s > 0), block + 1, 0))
            convolve(target * tiles, 0)
            ship(1, conv_out, target)
            ship_stat(target)
            return 0

        falling_count = jnp.where(s > 0, 1, 0) + jnp.where(block == 0, 1, 0)
        lax.fori_loop(0, jnp.where(rising, 1, falling_count), conv_block, 0)
        whole = z < n_sp - 1

        def run(u, _):
            query = jnp.where(rising, block, jnp.where(whole, n_sp - 1 - u, block))
            attend(query, query, True)

            def further(t, _):
                attend(jnp.where(whole, query, query + t), jnp.where(whole, query - t, query), False)
                return 0

            lax.fori_loop(1, jnp.where(whole, query, s) + 1, further, 0)
            return 0

        gathered = jnp.where(s == n_sp - 1, n_sp, 0)
        lax.fori_loop(0, jnp.where(z == n_sp - 2, gathered, 1), run, 0)
        return 0

    lax.fori_loop(0, n_sp, step, 0)


    others = [(z + d) % n_sp for d in range(1, n_sp)]

    def stat_from(slot):
        return remote(stat_all.at[slot], stat_all.at[slot], st_s.at[0, z], st_r.at[slot], tp=1 - tp)

    def x_from(k, source):
        ref = x_all.at[k * n_sp + source]
        return remote(ref, ref, x_s.at[k, z], x_r.at[k, source], tp=1 - tp)

    for source in others:
        stat_from(source).wait_recv()
    for source in range(n_sp):
        stat_from(n_sp + source).wait_recv()
    for source in others:
        x_from(1, source).wait_recv()
    kind = lax.broadcasted_iota(jnp.int32, (rows, n * 8), 1) % 8
    for t in range(tiles):
        stats = jnp.transpose(stat_all[:, t].reshape(n * 8, rows))
        mean = jnp.sum(jnp.where(kind == 0, stats, 0.0), axis=1, keepdims=True) / n
        off_mean = stats - mean
        spread = jnp.where(kind == 0, off_mean * off_mean, jnp.where(kind == 1, stats, 0.0))
        scale = lax.rsqrt(jnp.sum(spread, axis=1, keepdims=True) / n + 1e-06)
        at = pl.ds(t * rows, rows)
        for g in range(n_sp):
            x = x_all[n_sp + g, at, :].astype(F32) + off_mean[:, 8 * g : 8 * g + 1]
            y = x * scale * cgain[:, g * width : (g + 1) * width]
            hidden[at, (n_sp + g) * width : (n_sp + g + 1) * width] = (y * jax.nn.sigmoid(y)).astype(BF16)
    for source in others:
        x_from(0, source).wait_recv()
    for g in range(n_sp):
        hidden[:, g * width : (g + 1) * width] = x_all[g]

    sent = []
    for index, owner in enumerate((fs, xn, yn, dg)):
        if owner is xn:
            send_o(xn, 0, 3, 3, fs=xn).wait_recv()
            send_side(xn, 1, 8, xn).wait_recv()
        elif owner is yn:
            send_o(yn, 1, 3, 7, fs=xn).wait_recv()
            send_side(yn, 0, 9, xn).wait_recv()
        elif owner is dg:
            for side in range(2):
                for q in (1, 2):
                    send_o(dg, side, q, 10 + 3 * side + q, fs=xn).wait_recv()
                send_o(dg, side, 3, 16 + side, sp=mate).wait_recv()
        part[index] = jnp.dot(hidden[...], wout[owner], preferred_element_type=F32).astype(BF16)
        cols = aligned(owner * o_cols, o_cols)
        give = remote(
            part.at[index, aligned((1 - tp) * rows, rows)], got_out.at[:, cols],
            part_s.at[index], part_r.at[index], tp=1 - tp,
        )
        give.start()
        own_out[:, cols] = part[index, aligned(tp * rows, rows), :]
        sent.append(give)

    for copy in w_first + w_relay + o_first + o_later + o_share:
        copy.wait_send()
    for pair in o_relay:
        for copy in pair:
            copy.wait_send()
    for dist in range(1, n_sp):
        @pl.when(jnp.logical_and(z < n_sp - 1, z >= dist - 1))
        def _():
            lift_off(z, dist).wait_send()

        @pl.when(jnp.logical_and(z > 0, z + dist - 1 < n_sp))
        def _():
            sink_off(z, dist).wait_send()

    for p in range(2):
        for dist in range(1, n_sp):
            @pl.when(jnp.logical_and(z < n_sp - 1, z >= dist - 1))
            def _():
                lift(z, dist, p).wait_send()

            @pl.when(jnp.logical_and(z > 0, z + dist - 1 < n_sp))
            def _():
                sink(z, dist, p).wait_send()

        for block in range(n_sp):
            across(block, p).wait_send()
    for block in others:
        for k in range(2):
            remote(x_all.at[k], x_all.at[k], x_s.at[k, block], x_r.at[k, z], tp=1 - tp).wait_send()
        remote(stat_all.at[z], stat_all.at[z], st_s.at[0, block], st_r.at[z], tp=1 - tp).wait_send()
    for block in range(n_sp):
        remote(stat_all.at[z], stat_all.at[z], st_s.at[1, block], st_r.at[z], tp=1 - tp).wait_send()
    for copy in sent:
        copy.wait()


def layer_call(n_sp, n_fs, n_tp, width, heads, blk, tokens, gain, w_ins, off, ck, cgain, wa, wc):
    rows, features = tokens.shape
    depth = w_ins[0].shape[0]
    o_rows, o_cols = wa.shape
    length, n = rows * n_sp * n_tp, n_sp * n_tp
    tiles = blk // rows
    dma = pltpu.SemaphoreType.DMA
    vmem = pltpu.VMEM
    result = vmem((rows, n_fs * o_cols), BF16)
    return pl.pallas_call(
        functools.partial(layer_body, n_sp, n_tp, width, heads, ck.shape[0], blk),
        out_shape=[result, result],
        in_specs=[ANY] * 12,
        out_specs=[pl.BlockSpec(memory_space=pltpu.VMEM)] * 2,
        scratch_shapes=[
            vmem((length, features), BF16),
            vmem((n_fs * depth, 5 * width), BF16),
            vmem((n_fs, 2 * o_rows, o_cols), BF16),
            vmem((n_sp,) + off.shape, BF16),
            vmem((n_sp,) + off.shape, F32),
            vmem((ck.shape[0], width), F32),
            vmem(gain.shape, F32),
            vmem(cgain.shape, F32),
            vmem((n_sp, heads * blk, width), BF16),
            vmem((length, width), BF16),
            vmem((length, width), BF16),
            vmem((length + 32, width), F32),
            vmem((n_sp, heads * blk, 1), F32),
            vmem((n_sp, heads * blk, width), F32),
            vmem((length, width), BF16),
            vmem((length, width), BF16),
            vmem((length // rows, 8, rows), F32),
            vmem((2 * n_sp, blk, width), BF16),
            vmem((n, tiles, 8, rows), F32),
            vmem((blk, 2 * n_sp * width), BF16),
            vmem((n_fs, blk, o_cols), BF16),
            dma((12,)),
            dma((n_sp - 1, 2)), dma((n_sp - 1, 2)), dma((n_sp - 1, 2)), dma((n_sp - 1, 2)),
            dma((n_sp, 2)), dma((n_sp, 2)),
            dma((6,)), dma((6,)),
            dma((2, n_sp - 1)), dma((2, n_sp - 1)),
            dma((18,)), dma((18,)),
            dma((2, n_sp)), dma((2, n_sp)),
            dma((2, n_sp)), dma((n,)),
            dma((n_fs,)), dma((n_fs,)),
        ],
        compiler_params=pltpu.CompilerParams(collective_id=0, has_side_effects=True),
        name="layer",
    )(tokens, gain, *w_ins, off, ck, cgain, wa, wc)


def spread_shards(
    tokens,
    norm_gain,
    w_query,
    w_key,
    w_value,
    w_conv_value,
    w_conv_gate,
    key_offset,
    conv_kernel,
    conv_gain,
    w_attn_out,
    w_conv_out,
):
    n_sp, n_fs, n_tp = (lax.axis_size(a) for a in ("sp", "fs", "tp"))
    width = w_query.shape[1] // n_sp
    own, got = layer_call(
        n_sp, n_fs, n_tp, width, width // HD, key_offset.shape[0], tokens[0], norm_gain[None],
        (w_query, w_key, w_value, w_conv_value, w_conv_gate), jnp.transpose(key_offset),
        conv_kernel, conv_gain[None], w_attn_out, w_conv_out,
    )
    return (own.astype(F32) + got.astype(F32)).astype(BF16)[None]


def shifted(block, axis, distance):
    devices = range(lax.axis_size(axis))
    route = [(i - distance, i) for i in devices if i - distance in devices]
    return lax.ppermute(block, axis, route)


def piece_terms(queries, key_rows, value_rows, offsets, carry_log, allowed):
    head_size = queries.shape[2]
    logits = jnp.einsum(
        "qhd,khd->hqk", queries, key_rows, preferred_element_type=jnp.float32
    ) * head_size ** (-0.5)
    logits = logits + jnp.transpose(offsets.astype(jnp.float32))[:, None, :]
    log_keep = jax.nn.log_sigmoid(-logits)
    if allowed is not None:
        log_keep = jnp.where(allowed[None], log_keep, 0.0)
    between = lax.cumsum(log_keep, axis=2, reverse=True) - log_keep
    weights = jnp.exp(jax.nn.log_sigmoid(logits) + between + carry_log[:, :, None])
    if allowed is not None:
        weights = jnp.where(allowed[None], weights, 0.0)
    result = jnp.einsum(
        "hqk,khd->qhd", weights.astype(jnp.bfloat16), value_rows, preferred_element_type=jnp.float32
    )
    return (result, carry_log + jnp.sum(log_keep, axis=2))


def shards(
    tokens,
    norm_gain,
    w_query,
    w_key,
    w_value,
    w_conv_value,
    w_conv_gate,
    key_offset,
    conv_kernel,
    conv_gain,
    w_attn_out,
    w_conv_out,
):
    gathered = (
        lax.all_gather(w_query, "fs", axis=0, tiled=True),
        lax.all_gather(w_key, "fs", axis=0, tiled=True),
        lax.all_gather(w_value, "fs", axis=0, tiled=True),
        lax.all_gather(w_conv_value, "fs", axis=0, tiled=True),
        lax.all_gather(w_conv_gate, "fs", axis=0, tiled=True),
    )
    floats = lax.all_gather(tokens[0], "tp", axis=0, tiled=True).astype(jnp.float32)
    normed = (
        floats * lax.rsqrt(jnp.mean(floats * floats, axis=1, keepdims=True) + 1e-06) * norm_gain
    ).astype(jnp.bfloat16)
    projected = jnp.concatenate(
        [
            jnp.dot(normed, weight, preferred_element_type=jnp.float32).astype(jnp.bfloat16)
            for weight in gathered
        ],
        axis=1,
    )
    head_cols = w_query.shape[1]
    channels = w_conv_value.shape[1]
    block_len = projected.shape[0]
    local_heads = head_cols // HD
    queries = projected[:, :head_cols].reshape(block_len, local_heads, HD)
    key_flat = projected[:, head_cols : 2 * head_cols]
    value_flat = projected[:, 2 * head_cols : 3 * head_cols]
    conv_value = projected[:, 3 * head_cols : 3 * head_cols + channels]
    conv_gate = projected[:, 3 * head_cols + channels :]
    position = lax.axis_index("sp")
    positions = jnp.arange(block_len, dtype=jnp.int32)
    causal = positions[None, :] < positions[:, None]
    start_log = jnp.zeros((local_heads, block_len), jnp.float32)
    totals, carry_log = piece_terms(
        queries,
        key_flat.reshape(block_len, local_heads, HD),
        value_flat.reshape(block_len, local_heads, HD),
        key_offset,
        start_log,
        causal,
    )

    def visit(hop_count, carried):
        running, running_log, moving = carried
        moving = shifted((moving[0], moving[1], moving[2]), "sp", 1)
        result, next_log = piece_terms(
            queries,
            moving[0].reshape(block_len, local_heads, HD),
            moving[1].reshape(block_len, local_heads, HD),
            moving[2],
            running_log,
            None,
        )
        active = position >= hop_count
        running = jnp.where(active, running + result, running)
        running_log = jnp.where(active, next_log, running_log)
        return (running, running_log, moving)

    totals, carry_log, leftover = lax.fori_loop(
        1, lax.axis_size("sp"), visit, (totals, carry_log, (key_flat, value_flat, key_offset))
    )
    attn_heads = totals.reshape(block_len, head_cols).astype(jnp.bfloat16)
    gated_input = (
        conv_value.astype(jnp.float32) * jax.nn.sigmoid(conv_gate.astype(jnp.float32))
    ).astype(jnp.bfloat16)
    kernel_len = conv_kernel.shape[0]
    edge_rows = shifted(gated_input[block_len - (kernel_len - 1) :], "sp", 1)
    extended = jnp.concatenate([edge_rows, gated_input], axis=0).astype(jnp.float32)
    conv_sum = jnp.zeros((block_len, channels), jnp.float32)
    for tap_index in range(kernel_len):
        conv_sum = conv_sum + conv_kernel[tap_index] * extended[tap_index : tap_index + block_len]
    channel_total = lax.psum(jnp.sum(conv_sum, axis=1), "tp")
    centred = conv_sum - (channel_total / CC)[:, None]
    spread = lax.psum(jnp.sum(centred * centred, axis=1), "tp") / CC
    conv_hidden = jax.nn.silu(centred * lax.rsqrt(spread + 1e-06)[:, None] * conv_gain).astype(
        jnp.bfloat16
    )
    attn_weight, conv_weight = (
        lax.all_gather(w_attn_out, "fs", axis=1, tiled=True),
        lax.all_gather(w_conv_out, "fs", axis=1, tiled=True),
    )
    partial_value = jnp.dot(attn_heads, attn_weight, preferred_element_type=jnp.float32)
    partial_value = partial_value + jnp.dot(
        conv_hidden, conv_weight, preferred_element_type=jnp.float32
    )
    mixed = lax.psum_scatter(
        lax.optimization_barrier(partial_value.astype(jnp.bfloat16))
        .astype(jnp.float32)
        .astype(jnp.bfloat16),
        "tp",
        scatter_dimension=0,
        tiled=True,
    )
    return mixed[None]


def solution(mesh):
    placed = (
        P("fs", ("sp", "tp"), None),
        P(),
        P("fs", "tp"),
        P("fs", "tp"),
        P("fs", "tp"),
        P("fs", "tp"),
        P("fs", "tp"),
        P("sp", "tp"),
        P(None, "tp"),
        P("tp"),
        P("tp", "fs"),
        P("tp", "fs"),
    )

    def fits(tokens, norm_gain, w_query, *rest):
        n_sp, n_fs, n_tp = mesh.shape["sp"], mesh.shape["fs"], mesh.shape["tp"]
        cols = w_query.shape[1] // n_tp
        return n_fs == 4 and n_tp == 2 and n_sp == 4 and rest[5].shape[0] <= 33 and cols % (128 * n_sp) == 0 and rest[2].shape[1] == w_query.shape[1] and (
            tokens.shape[1] % (128 * n_sp * n_tp) == 0
        )

    def program(*args):
        body = spread_shards if fits(*args) else shards
        return mapped(body)(*args)

    def mapped(body):
        return jax.shard_map(
            body, mesh=mesh, in_specs=placed, out_specs=P("fs", ("sp", "tp"), None), check_vma=False
        )

    return program
```

```python
import functools

import jax
import jax.numpy as jnp
from jax import lax
from jax.experimental import pallas as pl
from jax.experimental.pallas import tpu as pltpu
from jax.sharding import PartitionSpec as P

HD = 64
CC = 1024
MESH = pl.DeviceIdType.MESH
F32 = jnp.float32
BF16 = jnp.bfloat16


def remote(src, dst, send, recv, **where):
    return pltpu.make_async_remote_copy(
        src_ref=src, dst_ref=dst, send_sem=send, recv_sem=recv, device_id=where, device_id_type=MESH
    )


def greet(peers):
    barrier = pltpu.get_barrier_semaphore()
    for where in peers:
        pl.semaphore_signal(barrier, inc=1, device_id=where, device_id_type=MESH)
    pl.semaphore_wait(barrier, len(peers))


def plane(fs):
    y = (fs + 2) % 4
    return fs + 1 - 2 * (fs % 2), y, y + 1 - 2 * (y % 2)


ANY = pl.BlockSpec(memory_space=pl.ANY)


LOG2E = 1.4426950408889634


def aligned(start, size):
    return pl.ds(pl.multiple_of(start, size), size)


def layer_body(n_sp, n_tp, width, heads, taps, blk, *refs):
    tok_in, gain_in, w_ins, off_in, ck_in, cgain_in, wa_in, wc_in = refs[0], refs[1], refs[2:7], *refs[7:12]
    own_out, got_out = refs[12:14]
    tok, w, wout, off_raw, off, ck, gain, cgain = refs[14:22]
    queries, keys, values, gated, carry, running = refs[22:28]
    attn_out, conv_out, stat_out, x_all, stat_all, hidden, part = refs[28:35]
    ld, up_s, up_r, dn_s, dn_r, par_s, par_r, w_s, w_r, off_s, off_r = refs[35:46]
    o_s, o_r, x_s, x_r, st_s, st_r, part_s, part_r, ready = refs[46:]
    rows = tok_in.shape[0]
    tiles = blk // rows
    sub = rows // 2
    depth = w_ins[0].shape[0]
    half = depth // 2
    o_rows, o_cols = wa_in.shape
    share = o_rows * 9 // 32 // 16 * 16
    small = o_rows // 2 - share
    z, fs, tp = lax.axis_index("sp"), lax.axis_index("fs"), lax.axis_index("tp")
    xn, yn, dg = plane(fs)
    n = n_sp * n_tp
    me = z * n_tp + tp

    own_rows = aligned((z * n_tp + tp) * rows, rows)
    loads = [pltpu.make_async_copy(tok_in, tok.at[own_rows], ld.at[0])]
    loads += [
        pltpu.make_async_copy(
            ref.at[:, aligned(z * width, width)],
            w.at[aligned(fs * depth, depth), pl.ds(k * width, width)],
            ld.at[1 + k],
        )
        for k, ref in enumerate(w_ins)
    ]
    loads += [
        pltpu.make_async_copy(wa_in, wout.at[fs, pl.ds(0, o_rows)], ld.at[6]),
        pltpu.make_async_copy(wc_in, wout.at[fs, pl.ds(o_rows, o_rows)], ld.at[7]),
        pltpu.make_async_copy(off_in, off_raw.at[z], ld.at[8]),
        pltpu.make_async_copy(ck_in.at[:, aligned(z * width, width)], ck, ld.at[9]),
        pltpu.make_async_copy(gain_in, gain, ld.at[10]),
        pltpu.make_async_copy(cgain_in, cgain, ld.at[11]),
    ]
    for copy in loads[:6] + loads[8:]:
        copy.start()
    barrier = pltpu.get_barrier_semaphore()

    def hello(**where):
        pl.semaphore_signal(barrier, inc=1, device_id=where, device_id_type=MESH)

    hello(fs=xn)
    hello(fs=yn)
    hello(tp=1 - tp)


    @pl.when(z < n_sp - 1)
    def _():
        hello(sp=z + 1)

    eager = n_sp // 2

    @pl.when(z > eager)
    def _():
        hello(sp=z - 1)

    pl.semaphore_wait(
        barrier, 3 + jnp.where(z > 0, 1, 0) + jnp.where(jnp.logical_and(z >= eager, z < n_sp - 1), 1, 0)
    )

    @pl.when(jnp.logical_and(z > 0, z <= eager))
    def _():
        pl.semaphore_signal(ready, inc=1, device_id={"sp": z - 1}, device_id_type=MESH)

    def piece_rows(block, core, p):
        return tok.at[aligned((block * n_tp + core) * rows + p * sub, sub)]

    def lift(block, dist, p):
        ref = piece_rows(block, tp, p)
        return remote(ref, ref, up_s.at[dist - 1, p], up_r.at[dist - 1, p], sp=(z + 1) % n_sp)

    def sink(block, dist, p):
        ref = piece_rows(block, tp, p)
        return remote(ref, ref, dn_s.at[dist - 1, p], dn_r.at[dist - 1, p], sp=(z + n_sp - 1) % n_sp)

    def lift_off(block, dist):
        ref = off_raw.at[block]
        return remote(ref, ref, off_s.at[0, dist - 1], off_r.at[0, dist - 1], sp=(z + 1) % n_sp)

    def sink_off(block, dist):
        ref = off_raw.at[block]
        return remote(ref, ref, off_s.at[1, dist - 1], off_r.at[1, dist - 1], sp=(z + n_sp - 1) % n_sp)

    def across(block, p):
        ref = piece_rows(block, tp, p)
        return remote(ref, ref, par_s.at[block, p], par_r.at[block, p], tp=1 - tp)

    def from_partner(block, p):
        ref = piece_rows(block, 1 - tp, p)
        return remote(ref, ref, par_s.at[block, p], par_r.at[block, p], tp=1 - tp)

    def w_part(owner, h):
        return w.at[aligned(owner * depth + h * half, half)]

    def send_w(owner, h, sem, to):
        return remote(w_part(owner, h), w_part(owner, h), w_s.at[sem], w_r.at[sem], fs=to)

    mate = z + 1 - 2 * (z % 2)
    edge = jnp.logical_or(z == 0, z == n_sp - 1)

    def o_piece(owner, side, q):
        far = share + 2 * small
        start = (jnp.where(edge, 0, far), share, share + small, jnp.where(edge, far, 0))[q]
        size = share if q in (0, 3) else small
        return wout.at[owner, pl.ds(pl.multiple_of(side * o_rows + start, 16), size)]

    def send_o(owner, side, q, sem, **to):
        ref = o_piece(owner, side, q)
        return remote(ref, ref, o_s.at[sem], o_r.at[sem], **to)

    def send_side(owner, side, sem, to):
        ref = wout.at[owner, pl.ds(side * o_rows, o_rows)]
        return remote(ref, ref, o_s.at[sem], o_r.at[sem], fs=to)

    loads[0].wait()
    for p in range(2):
        @pl.when(jnp.logical_and(z >= eager, z < n_sp - 1))
        def _():
            lift(z, 1, p).start()

        @pl.when(z > 0)
        def _():
            sink(z, 1, p).start()

    for k in range(5):
        loads[1 + k].wait()
    w_first = [send_w(fs, 0, 0, xn), send_w(fs, 1, 1, yn), send_w(fs, 1, 2, xn), send_w(fs, 0, 3, yn)]
    for copy in w_first:
        copy.start()
    for copy in loads[6:8]:
        copy.start()
    for p in range(2):
        across(z, p).start()
    loads[8].wait()

    @pl.when(z > 0)
    def _():
        sink_off(z, 1).start()

    @pl.when(z < eager)
    def _():
        pl.semaphore_wait(ready, 1)
        for p in range(2):
            lift(z, 1, p).start()

    @pl.when(z < n_sp - 1)
    def _():
        lift_off(z, 1).start()

    w_relay = [send_w(xn, 0, 4, yn), send_w(yn, 1, 5, xn)]
    w_here = [(0, xn, 0), (1, yn, 1), (2, xn, 1), (3, yn, 0), (4, dg, 0), (5, dg, 1)]
    o_first = []
    for q in range(3):
        o_first += [send_o(fs, 0, q, q, fs=xn), send_o(fs, 1, q, 4 + q, fs=yn)]
    o_later = [send_o(fs, 0, 3, 3, fs=xn), send_o(fs, 1, 3, 7, fs=yn), send_side(fs, 1, 8, xn), send_side(fs, 0, 9, yn)]
    o_relay = [(send_o(xn, 0, q, 10 + q, fs=yn), send_o(yn, 1, q, 13 + q, fs=xn)) for q in range(3)]
    o_share = [send_o(dg, side, 0, 16 + side, sp=mate) for side in range(2)]

    def relay_o(q):
        send_o(xn, 0, q, q, fs=xn).wait_recv()
        send_o(yn, 1, q, 4 + q, fs=xn).wait_recv()
        for copy in o_relay[q]:
            copy.start()

    def share_o():
        for side in range(2):
            send_o(dg, side, 0, 10 + 3 * side, fs=xn).wait_recv()
            o_share[side].start()

    def token_hop(dist, p):
        @pl.when(z >= dist)
        def _():
            block = (z - dist + n_sp) % n_sp
            lift(block, dist, p).wait_recv()
            if dist < n_sp - 1:
                @pl.when(z < n_sp - 1)
                def _():
                    lift(block, dist + 1, p).start()
            across(block, p).start()

        @pl.when(z + dist < n_sp)
        def _():
            block = (z + dist) % n_sp
            sink(block, dist, p).wait_recv()
            if dist < n_sp - 1:
                @pl.when(z > 0)
                def _():
                    sink(block, dist + 1, p).start()
            across(block, p).start()

    def offset_hop(dist):
        @pl.when(z >= dist)
        def _():
            block = (z - dist + n_sp) % n_sp
            lift_off(block, dist).wait_recv()
            if dist < n_sp - 1:
                @pl.when(z < n_sp - 1)
                def _():
                    lift_off(block, dist + 1).start()

        @pl.when(z + dist < n_sp)
        def _():
            block = (z + dist) % n_sp
            sink_off(block, dist).wait_recv()
            if dist < n_sp - 1:
                @pl.when(z > 0)
                def _():
                    sink_off(block, dist + 1).start()

    def relay_w():
        for s, owner, h in w_here[:2]:
            send_w(owner, h, s, xn).wait_recv()
            w_relay[s].start()
        for copy in loads[6:8]:
            copy.wait()
        for copy in o_first:
            copy.start()

    gated[pl.ds(0, 32), :] = jnp.zeros((32, width), F32)
    for dist in range(1, n_sp - 1):
        token_hop(dist, 0)
        offset_hop(dist)
        if dist == 1:
            relay_w()
        token_hop(dist, 1)
    if n_sp == 2:
        relay_w()
    for copy in loads[9:]:
        copy.wait()
    for s, owner, h in w_here[2:]:
        send_w(owner, h, s, xn).wait_recv()

    lane = lax.broadcasted_iota(jnp.int32, (rows, width), 1)

    def project(block, p):
        def spots(c):
            return c * rows + p * sub

        x = jnp.concatenate(
            [tok[aligned(block * blk + spots(c), sub), :] for c in range(n_tp)], axis=0
        ).astype(F32)
        normed = (x * lax.rsqrt(jnp.mean(x * x, axis=1, keepdims=True) + 1e-06) * gain[...]).astype(BF16)
        out = jnp.dot(normed, w[...], preferred_element_type=F32).astype(BF16)
        q = out[:, :width].astype(F32) * HD ** (-0.5)
        masked = [
            jnp.where(jnp.logical_and(lane >= h * HD, lane < (h + 1) * HD), q, 0.0).astype(BF16) for h in range(heads)
        ]
        value = out[:, 3 * width : 4 * width].astype(F32)
        gate = out[:, 4 * width :].astype(F32)
        fresh = (value * jax.nn.sigmoid(gate)).astype(BF16).astype(F32)
        for c in range(n_tp):
            part_of = slice(c * sub, (c + 1) * sub)
            at = aligned(block * blk + spots(c), sub)
            for h in range(heads):
                queries[block, aligned(h * blk + spots(c), sub), :] = masked[h][part_of]
            keys[at, :] = out[part_of, width : 2 * width]
            values[at, :] = out[part_of, 2 * width : 3 * width]
            gated[pl.ds(pl.multiple_of(block * blk + spots(c) + 32, 32), sub), :] = fresh[part_of]

    def convolve(tile, _):
        base = pl.multiple_of(tile * rows, rows)
        total = jnp.zeros((rows, width), F32)
        for phase in range(8):
            span = rows + 8 if phase else rows
            lined = jnp.zeros((span, width), F32)
            for tap in range((phase + taps - 33) % 8, taps, 8):
                lined = lined + ck[tap : tap + 1, :] * gated[pl.ds(base + (33 - taps + tap - phase), span), :]
            total = total + lined[phase : phase + rows]
        mean = jnp.mean(total, axis=1, keepdims=True)
        local = total - mean
        conv_out[pl.ds(base, rows), :] = local.astype(BF16)
        spread = jnp.mean(local * local, axis=1, keepdims=True)
        stat_out[tile] = jnp.transpose(jnp.where(lane == 0, mean, spread))[:8]
        return 0

    def block_rows(i):
        return aligned(i * blk, blk)


    def ship(k, source, block):
        at = source.at[block_rows(block)]

        @pl.when(block == z)
        def _():
            x_all[k * n_sp + z] = at[...]

        @pl.when(block != z)
        def _():
            remote(at, x_all.at[k * n_sp + z], x_s.at[k, block], x_r.at[k, z], sp=block).start()


    def ship_stat(block):
        at = stat_out.at[pl.ds(block * tiles, tiles)]

        @pl.when(block == z)
        def _():
            stat_all[z] = at[...]

        @pl.when(block != z)
        def _():
            remote(at, stat_all.at[z], st_s.at[0, block], st_r.at[z], sp=block).start()

        remote(at, stat_all.at[n_sp + z], st_s.at[1, block], st_r.at[n_sp + z], sp=block, tp=1 - tp).start()

    wide = lax.broadcasted_iota(jnp.int32, (blk, width), 1)
    row = lax.broadcasted_iota(jnp.int32, (blk, blk), 0)
    col = lax.broadcasted_iota(jnp.int32, (blk, blk), 1)
    stacked = (heads, blk, blk)
    earlier = lax.broadcasted_iota(jnp.int32, stacked, 2) < lax.broadcasted_iota(jnp.int32, stacked, 1)
    earlier = earlier.reshape(heads * blk, blk)

    def attend(i, j, diagonal):
        k = keys[block_rows(j), :]
        v = values[block_rows(j), :]
        after = jnp.where(row >= col, 1.0, 0.0).astype(BF16)
        s = lax.dot_general(queries[i], k, (((1,), (1,)), ((), ())), preferred_element_type=F32)
        shift = jnp.concatenate(
            [jnp.broadcast_to(off[j, pl.ds(z * heads + h, 1), :], (blk, blk)) for h in range(heads)], axis=0
        )
        s = s * LOG2E + shift
        keep = jnp.minimum(-s, 0.0) - jnp.log2(1.0 + jnp.exp2(-jnp.abs(s)))
        if diagonal:
            keep = jnp.where(earlier, keep, 0.0)
        suffix = jnp.dot(keep.astype(BF16), after, preferred_element_type=F32)
        if diagonal:
            weights = jnp.where(earlier, jnp.exp2(s + suffix), 0.0)
            carry[i] = suffix[:, :1]
            running[i] = jnp.dot(weights.astype(BF16), v, preferred_element_type=F32)
        else:
            before = carry[i]
            weights = jnp.exp2(s + suffix + before)
            carry[i] = before + suffix[:, :1]
            running[i] += jnp.dot(weights.astype(BF16), v, preferred_element_type=F32)

        @pl.when(j == 0)
        def _():
            merged = running[i, :blk]
            for h in range(1, heads):
                merged = jnp.where(wide >= h * HD, running[i, h * blk : (h + 1) * blk], merged)
            attn_out[block_rows(i), :] = merged.astype(BF16)
            ship(0, attn_out, i)

    def step(s, _):
        rising = z < n_sp - 2
        block = jnp.where(rising, s, n_sp - 1 - s)

        def half_block(p, _):
            @pl.when(jnp.logical_and(s == n_sp - 1, edge))
            def _():
                @pl.when(p == 1)
                def _():
                    share_o()

                token_hop(n_sp - 1, p)

            from_partner(block, p).wait_recv()
            project(block, p)
            return 0

        lax.fori_loop(0, 2, half_block, 0)

        @pl.when(jnp.logical_and(s == n_sp - 1, edge))
        def _():
            offset_hop(n_sp - 1)

        off[block] = off_raw[block].astype(F32) * LOG2E

        @pl.when(s == n_sp - 3)
        def _():
            relay_o(0)
            for copy in o_later:
                copy.start()

        @pl.when(s == n_sp - 2)
        def _():
            for q in (1, 2):
                relay_o(q)

        @pl.when(jnp.logical_and(s == n_sp - 1, jnp.logical_not(edge)))
        def _():
            share_o()

        lax.fori_loop(block * tiles + 1, block * tiles + tiles, convolve, 0)

        def conv_block(u, _):
            target = jnp.where(rising, block, jnp.where(jnp.logical_and(u == 0, s > 0), block + 1, 0))
            convolve(target * tiles, 0)
            ship(1, conv_out, target)
            ship_stat(target)
            return 0

        falling_count = jnp.where(s > 0, 1, 0) + jnp.where(block == 0, 1, 0)
        lax.fori_loop(0, jnp.where(rising, 1, falling_count), conv_block, 0)
        whole = z < n_sp - 1

        def run(u, _):
            query = jnp.where(rising, block, jnp.where(whole, (n_sp - u) % n_sp, block))
            attend(query, query, True)

            def further(t, _):
                attend(jnp.where(whole, query, query + t), jnp.where(whole, query - t, query), False)
                return 0

            lax.fori_loop(1, jnp.where(whole, query, s) + 1, further, 0)
            return 0

        gathered = jnp.where(s == n_sp - 1, n_sp, 0)
        lax.fori_loop(0, jnp.where(z == n_sp - 2, gathered, 1), run, 0)
        return 0

    lax.fori_loop(0, n_sp, step, 0)


    others = [(z + d) % n_sp for d in range(1, n_sp)]

    def stat_from(slot):
        return remote(stat_all.at[slot], stat_all.at[slot], st_s.at[0, z], st_r.at[slot], tp=1 - tp)

    def x_from(k, source):
        ref = x_all.at[k * n_sp + source]
        return remote(ref, ref, x_s.at[k, z], x_r.at[k, source], tp=1 - tp)

    for source in others:
        stat_from(source).wait_recv()
    for source in range(n_sp):
        stat_from(n_sp + source).wait_recv()
    for source in others:
        x_from(1, source).wait_recv()
    kind = lax.broadcasted_iota(jnp.int32, (rows, n * 8), 1) % 8
    for t in range(tiles):
        stats = jnp.transpose(stat_all[:, t].reshape(n * 8, rows))
        mean = jnp.sum(jnp.where(kind == 0, stats, 0.0), axis=1, keepdims=True) / n
        off_mean = stats - mean
        spread = jnp.where(kind == 0, off_mean * off_mean, jnp.where(kind == 1, stats, 0.0))
        scale = lax.rsqrt(jnp.sum(spread, axis=1, keepdims=True) / n + 1e-06)
        at = pl.ds(t * rows, rows)
        for g in range(n_sp):
            x = x_all[n_sp + g, at, :].astype(F32) + off_mean[:, 8 * g : 8 * g + 1]
            y = x * scale * cgain[:, g * width : (g + 1) * width]
            hidden[at, (n_sp + g) * width : (n_sp + g + 1) * width] = (y * jax.nn.sigmoid(y)).astype(BF16)
    for source in others:
        x_from(0, source).wait_recv()
    for g in range(n_sp):
        hidden[:, g * width : (g + 1) * width] = x_all[g]

    sent = []
    for index, owner in enumerate((fs, xn, yn, dg)):
        if owner is xn:
            send_o(xn, 0, 3, 3, fs=xn).wait_recv()
            send_side(xn, 1, 8, xn).wait_recv()
        elif owner is yn:
            send_o(yn, 1, 3, 7, fs=xn).wait_recv()
            send_side(yn, 0, 9, xn).wait_recv()
        elif owner is dg:
            for side in range(2):
                for q in (1, 2):
                    send_o(dg, side, q, 10 + 3 * side + q, fs=xn).wait_recv()
                send_o(dg, side, 3, 16 + side, sp=mate).wait_recv()
        part[index] = jnp.dot(hidden[...], wout[owner], preferred_element_type=F32).astype(BF16)
        cols = aligned(owner * o_cols, o_cols)
        give = remote(
            part.at[index, aligned((1 - tp) * rows, rows)], got_out.at[:, cols],
            part_s.at[index], part_r.at[index], tp=1 - tp,
        )
        give.start()
        own_out[:, cols] = part[index, aligned(tp * rows, rows), :]
        sent.append(give)

    for copy in w_first + w_relay + o_first + o_later + o_share:
        copy.wait_send()
    for pair in o_relay:
        for copy in pair:
            copy.wait_send()
    for dist in range(1, n_sp):
        @pl.when(jnp.logical_and(z < n_sp - 1, z >= dist - 1))
        def _():
            lift_off(z, dist).wait_send()

        @pl.when(jnp.logical_and(z > 0, z + dist - 1 < n_sp))
        def _():
            sink_off(z, dist).wait_send()

    for p in range(2):
        for dist in range(1, n_sp):
            @pl.when(jnp.logical_and(z < n_sp - 1, z >= dist - 1))
            def _():
                lift(z, dist, p).wait_send()

            @pl.when(jnp.logical_and(z > 0, z + dist - 1 < n_sp))
            def _():
                sink(z, dist, p).wait_send()

        for block in range(n_sp):
            across(block, p).wait_send()
    for block in others:
        for k in range(2):
            remote(x_all.at[k], x_all.at[k], x_s.at[k, block], x_r.at[k, z], tp=1 - tp).wait_send()
        remote(stat_all.at[z], stat_all.at[z], st_s.at[0, block], st_r.at[z], tp=1 - tp).wait_send()
    for block in range(n_sp):
        remote(stat_all.at[z], stat_all.at[z], st_s.at[1, block], st_r.at[z], tp=1 - tp).wait_send()
    for copy in sent:
        copy.wait()


def layer_call(n_sp, n_fs, n_tp, width, heads, blk, tokens, gain, w_ins, off, ck, cgain, wa, wc):
    rows, features = tokens.shape
    depth = w_ins[0].shape[0]
    o_rows, o_cols = wa.shape
    length, n = rows * n_sp * n_tp, n_sp * n_tp
    tiles = blk // rows
    dma = pltpu.SemaphoreType.DMA
    vmem = pltpu.VMEM
    result = vmem((rows, n_fs * o_cols), BF16)
    return pl.pallas_call(
        functools.partial(layer_body, n_sp, n_tp, width, heads, ck.shape[0], blk),
        out_shape=[result, result],
        in_specs=[ANY] * 12,
        out_specs=[pl.BlockSpec(memory_space=pltpu.VMEM)] * 2,
        scratch_shapes=[
            vmem((length, features), BF16),
            vmem((n_fs * depth, 5 * width), BF16),
            vmem((n_fs, 2 * o_rows, o_cols), BF16),
            vmem((n_sp,) + off.shape, BF16),
            vmem((n_sp,) + off.shape, F32),
            vmem((ck.shape[0], width), F32),
            vmem(gain.shape, F32),
            vmem(cgain.shape, F32),
            vmem((n_sp, heads * blk, width), BF16),
            vmem((length, width), BF16),
            vmem((length, width), BF16),
            vmem((length + 32, width), F32),
            vmem((n_sp, heads * blk, 1), F32),
            vmem((n_sp, heads * blk, width), F32),
            vmem((length, width), BF16),
            vmem((length, width), BF16),
            vmem((length // rows, 8, rows), F32),
            vmem((2 * n_sp, blk, width), BF16),
            vmem((n, tiles, 8, rows), F32),
            vmem((blk, 2 * n_sp * width), BF16),
            vmem((n_fs, blk, o_cols), BF16),
            dma((12,)),
            dma((n_sp - 1, 2)), dma((n_sp - 1, 2)), dma((n_sp - 1, 2)), dma((n_sp - 1, 2)),
            dma((n_sp, 2)), dma((n_sp, 2)),
            dma((6,)), dma((6,)),
            dma((2, n_sp - 1)), dma((2, n_sp - 1)),
            dma((18,)), dma((18,)),
            dma((2, n_sp)), dma((2, n_sp)),
            dma((2, n_sp)), dma((n,)),
            dma((n_fs,)), dma((n_fs,)),
            pltpu.SemaphoreType.REGULAR,
        ],
        compiler_params=pltpu.CompilerParams(collective_id=0, has_side_effects=True),
        name="layer",
    )(tokens, gain, *w_ins, off, ck, cgain, wa, wc)


def spread_shards(
    tokens,
    norm_gain,
    w_query,
    w_key,
    w_value,
    w_conv_value,
    w_conv_gate,
    key_offset,
    conv_kernel,
    conv_gain,
    w_attn_out,
    w_conv_out,
):
    n_sp, n_fs, n_tp = (lax.axis_size(a) for a in ("sp", "fs", "tp"))
    width = w_query.shape[1] // n_sp
    own, got = layer_call(
        n_sp, n_fs, n_tp, width, width // HD, key_offset.shape[0], tokens[0], norm_gain[None],
        (w_query, w_key, w_value, w_conv_value, w_conv_gate), jnp.transpose(key_offset),
        conv_kernel, conv_gain[None], w_attn_out, w_conv_out,
    )
    return (own.astype(F32) + got.astype(F32)).astype(BF16)[None]


def shifted(block, axis, distance):
    devices = range(lax.axis_size(axis))
    route = [(i - distance, i) for i in devices if i - distance in devices]
    return lax.ppermute(block, axis, route)


def piece_terms(queries, key_rows, value_rows, offsets, carry_log, allowed):
    head_size = queries.shape[2]
    logits = jnp.einsum(
        "qhd,khd->hqk", queries, key_rows, preferred_element_type=jnp.float32
    ) * head_size ** (-0.5)
    logits = logits + jnp.transpose(offsets.astype(jnp.float32))[:, None, :]
    log_keep = jax.nn.log_sigmoid(-logits)
    if allowed is not None:
        log_keep = jnp.where(allowed[None], log_keep, 0.0)
    between = lax.cumsum(log_keep, axis=2, reverse=True) - log_keep
    weights = jnp.exp(jax.nn.log_sigmoid(logits) + between + carry_log[:, :, None])
    if allowed is not None:
        weights = jnp.where(allowed[None], weights, 0.0)
    result = jnp.einsum(
        "hqk,khd->qhd", weights.astype(jnp.bfloat16), value_rows, preferred_element_type=jnp.float32
    )
    return (result, carry_log + jnp.sum(log_keep, axis=2))


def shards(
    tokens,
    norm_gain,
    w_query,
    w_key,
    w_value,
    w_conv_value,
    w_conv_gate,
    key_offset,
    conv_kernel,
    conv_gain,
    w_attn_out,
    w_conv_out,
):
    gathered = (
        lax.all_gather(w_query, "fs", axis=0, tiled=True),
        lax.all_gather(w_key, "fs", axis=0, tiled=True),
        lax.all_gather(w_value, "fs", axis=0, tiled=True),
        lax.all_gather(w_conv_value, "fs", axis=0, tiled=True),
        lax.all_gather(w_conv_gate, "fs", axis=0, tiled=True),
    )
    floats = lax.all_gather(tokens[0], "tp", axis=0, tiled=True).astype(jnp.float32)
    normed = (
        floats * lax.rsqrt(jnp.mean(floats * floats, axis=1, keepdims=True) + 1e-06) * norm_gain
    ).astype(jnp.bfloat16)
    projected = jnp.concatenate(
        [
            jnp.dot(normed, weight, preferred_element_type=jnp.float32).astype(jnp.bfloat16)
            for weight in gathered
        ],
        axis=1,
    )
    head_cols = w_query.shape[1]
    channels = w_conv_value.shape[1]
    block_len = projected.shape[0]
    local_heads = head_cols // HD
    queries = projected[:, :head_cols].reshape(block_len, local_heads, HD)
    key_flat = projected[:, head_cols : 2 * head_cols]
    value_flat = projected[:, 2 * head_cols : 3 * head_cols]
    conv_value = projected[:, 3 * head_cols : 3 * head_cols + channels]
    conv_gate = projected[:, 3 * head_cols + channels :]
    position = lax.axis_index("sp")
    positions = jnp.arange(block_len, dtype=jnp.int32)
    causal = positions[None, :] < positions[:, None]
    start_log = jnp.zeros((local_heads, block_len), jnp.float32)
    totals, carry_log = piece_terms(
        queries,
        key_flat.reshape(block_len, local_heads, HD),
        value_flat.reshape(block_len, local_heads, HD),
        key_offset,
        start_log,
        causal,
    )

    def visit(hop_count, carried):
        running, running_log, moving = carried
        moving = shifted((moving[0], moving[1], moving[2]), "sp", 1)
        result, next_log = piece_terms(
            queries,
            moving[0].reshape(block_len, local_heads, HD),
            moving[1].reshape(block_len, local_heads, HD),
            moving[2],
            running_log,
            None,
        )
        active = position >= hop_count
        running = jnp.where(active, running + result, running)
        running_log = jnp.where(active, next_log, running_log)
        return (running, running_log, moving)

    totals, carry_log, leftover = lax.fori_loop(
        1, lax.axis_size("sp"), visit, (totals, carry_log, (key_flat, value_flat, key_offset))
    )
    attn_heads = totals.reshape(block_len, head_cols).astype(jnp.bfloat16)
    gated_input = (
        conv_value.astype(jnp.float32) * jax.nn.sigmoid(conv_gate.astype(jnp.float32))
    ).astype(jnp.bfloat16)
    kernel_len = conv_kernel.shape[0]
    edge_rows = shifted(gated_input[block_len - (kernel_len - 1) :], "sp", 1)
    extended = jnp.concatenate([edge_rows, gated_input], axis=0).astype(jnp.float32)
    conv_sum = jnp.zeros((block_len, channels), jnp.float32)
    for tap_index in range(kernel_len):
        conv_sum = conv_sum + conv_kernel[tap_index] * extended[tap_index : tap_index + block_len]
    channel_total = lax.psum(jnp.sum(conv_sum, axis=1), "tp")
    centred = conv_sum - (channel_total / CC)[:, None]
    spread = lax.psum(jnp.sum(centred * centred, axis=1), "tp") / CC
    conv_hidden = jax.nn.silu(centred * lax.rsqrt(spread + 1e-06)[:, None] * conv_gain).astype(
        jnp.bfloat16
    )
    attn_weight, conv_weight = (
        lax.all_gather(w_attn_out, "fs", axis=1, tiled=True),
        lax.all_gather(w_conv_out, "fs", axis=1, tiled=True),
    )
    partial_value = jnp.dot(attn_heads, attn_weight, preferred_element_type=jnp.float32)
    partial_value = partial_value + jnp.dot(
        conv_hidden, conv_weight, preferred_element_type=jnp.float32
    )
    mixed = lax.psum_scatter(
        lax.optimization_barrier(partial_value.astype(jnp.bfloat16))
        .astype(jnp.float32)
        .astype(jnp.bfloat16),
        "tp",
        scatter_dimension=0,
        tiled=True,
    )
    return mixed[None]


def solution(mesh):
    placed = (
        P("fs", ("sp", "tp"), None),
        P(),
        P("fs", "tp"),
        P("fs", "tp"),
        P("fs", "tp"),
        P("fs", "tp"),
        P("fs", "tp"),
        P("sp", "tp"),
        P(None, "tp"),
        P("tp"),
        P("tp", "fs"),
        P("tp", "fs"),
    )

    def fits(tokens, norm_gain, w_query, *rest):
        n_sp, n_fs, n_tp = mesh.shape["sp"], mesh.shape["fs"], mesh.shape["tp"]
        cols = w_query.shape[1] // n_tp
        return n_fs == 4 and n_tp == 2 and n_sp == 4 and rest[5].shape[0] <= 33 and cols % (128 * n_sp) == 0 and rest[2].shape[1] == w_query.shape[1] and (
            tokens.shape[1] % (128 * n_sp * n_tp) == 0
        )

    def program(*args):
        body = spread_shards if fits(*args) else shards
        return mapped(body)(*args)

    def mapped(body):
        return jax.shard_map(
            body, mesh=mesh, in_specs=placed, out_specs=P("fs", ("sp", "tp"), None), check_vma=False
        )

    return program
```

```python
import functools

import jax
import jax.numpy as jnp
from jax import lax
from jax.experimental import pallas as pl
from jax.experimental.pallas import tpu as pltpu
from jax.sharding import PartitionSpec as P

HD = 64
CC = 1024
MESH = pl.DeviceIdType.MESH
F32 = jnp.float32
BF16 = jnp.bfloat16


def remote(src, dst, send, recv, **where):
    return pltpu.make_async_remote_copy(
        src_ref=src, dst_ref=dst, send_sem=send, recv_sem=recv, device_id=where, device_id_type=MESH
    )


def greet(peers):
    barrier = pltpu.get_barrier_semaphore()
    for where in peers:
        pl.semaphore_signal(barrier, inc=1, device_id=where, device_id_type=MESH)
    pl.semaphore_wait(barrier, len(peers))


def plane(fs):
    y = (fs + 2) % 4
    return fs + 1 - 2 * (fs % 2), y, y + 1 - 2 * (y % 2)


ANY = pl.BlockSpec(memory_space=pl.ANY)


LOG2E = 1.4426950408889634


def aligned(start, size):
    return pl.ds(pl.multiple_of(start, size), size)


def layer_body(n_sp, n_tp, width, heads, taps, blk, *refs):
    tok_in, gain_in, w_ins, off_in, ck_in, cgain_in, wa_in, wc_in = refs[0], refs[1], refs[2:7], *refs[7:12]
    own_out, got_out = refs[12:14]
    tok, w, wout, off_raw, off, ck, gain, cgain = refs[14:22]
    queries, keys, values, gated, carry, running = refs[22:28]
    attn_out, conv_out, stat_out, x_all, stat_all, hidden, part = refs[28:35]
    ld, up_s, up_r, dn_s, dn_r, par_s, par_r, w_s, w_r, off_s, off_r = refs[35:46]
    o_s, o_r, x_s, x_r, st_s, st_r, part_s, part_r, ready = refs[46:]
    rows = tok_in.shape[0]
    tiles = blk // rows
    sub = rows // 2
    depth = w_ins[0].shape[0]
    half = depth // 2
    o_rows, o_cols = wa_in.shape
    share = o_rows * 9 // 32 // 16 * 16
    small = o_rows // 2 - share
    z, fs, tp = lax.axis_index("sp"), lax.axis_index("fs"), lax.axis_index("tp")
    xn, yn, dg = plane(fs)
    n = n_sp * n_tp
    me = z * n_tp + tp

    own_rows = aligned((z * n_tp + tp) * rows, rows)
    loads = [pltpu.make_async_copy(tok_in, tok.at[own_rows], ld.at[0])]
    loads += [
        pltpu.make_async_copy(
            ref.at[:, aligned(z * width, width)],
            w.at[aligned(fs * depth, depth), pl.ds(k * width, width)],
            ld.at[1 + k],
        )
        for k, ref in enumerate(w_ins)
    ]
    loads += [
        pltpu.make_async_copy(wa_in, wout.at[fs, pl.ds(0, o_rows)], ld.at[6]),
        pltpu.make_async_copy(wc_in, wout.at[fs, pl.ds(o_rows, o_rows)], ld.at[7]),
        pltpu.make_async_copy(off_in, off_raw.at[z], ld.at[8]),
        pltpu.make_async_copy(ck_in.at[:, aligned(z * width, width)], ck, ld.at[9]),
        pltpu.make_async_copy(gain_in, gain, ld.at[10]),
        pltpu.make_async_copy(cgain_in, cgain, ld.at[11]),
    ]
    for copy in loads[:6] + loads[8:]:
        copy.start()
    barrier = pltpu.get_barrier_semaphore()

    def hello(**where):
        pl.semaphore_signal(barrier, inc=1, device_id=where, device_id_type=MESH)

    hello(fs=xn)
    hello(fs=yn)
    hello(tp=1 - tp)


    @pl.when(z < n_sp - 1)
    def _():
        hello(sp=z + 1)

    eager = n_sp // 2

    @pl.when(z > eager)
    def _():
        hello(sp=z - 1)

    pl.semaphore_wait(
        barrier, 3 + jnp.where(z > 0, 1, 0) + jnp.where(jnp.logical_and(z >= eager, z < n_sp - 1), 1, 0)
    )

    @pl.when(jnp.logical_and(z > 0, z <= eager))
    def _():
        pl.semaphore_signal(ready, inc=1, device_id={"sp": z - 1}, device_id_type=MESH)

    def piece_rows(block, core, p):
        return tok.at[aligned((block * n_tp + core) * rows + p * sub, sub)]

    def lift(block, dist, p):
        ref = piece_rows(block, tp, p)
        return remote(ref, ref, up_s.at[dist - 1, p], up_r.at[dist - 1, p], sp=(z + 1) % n_sp)

    def sink(block, dist, p):
        ref = piece_rows(block, tp, p)
        return remote(ref, ref, dn_s.at[dist - 1, p], dn_r.at[dist - 1, p], sp=(z + n_sp - 1) % n_sp)

    def lift_off(block, dist):
        ref = off_raw.at[block]
        return remote(ref, ref, off_s.at[0, dist - 1], off_r.at[0, dist - 1], sp=(z + 1) % n_sp)

    def sink_off(block, dist):
        ref = off_raw.at[block]
        return remote(ref, ref, off_s.at[1, dist - 1], off_r.at[1, dist - 1], sp=(z + n_sp - 1) % n_sp)

    def across(block, p):
        ref = piece_rows(block, tp, p)
        return remote(ref, ref, par_s.at[block, p], par_r.at[block, p], tp=1 - tp)

    def from_partner(block, p):
        ref = piece_rows(block, 1 - tp, p)
        return remote(ref, ref, par_s.at[block, p], par_r.at[block, p], tp=1 - tp)

    def w_part(owner, h):
        return w.at[aligned(owner * depth + h * half, half)]

    def send_w(owner, h, sem, to):
        return remote(w_part(owner, h), w_part(owner, h), w_s.at[sem], w_r.at[sem], fs=to)

    mate = z + 1 - 2 * (z % 2)
    edge = jnp.logical_or(z == 0, z == n_sp - 1)

    def o_piece(owner, side, q):
        far = share + 2 * small
        start = (jnp.where(edge, 0, far), share, share + small, jnp.where(edge, far, 0))[q]
        size = share if q in (0, 3) else small
        return wout.at[owner, pl.ds(pl.multiple_of(side * o_rows + start, 16), size)]

    def send_o(owner, side, q, sem, **to):
        ref = o_piece(owner, side, q)
        return remote(ref, ref, o_s.at[sem], o_r.at[sem], **to)

    def send_side(owner, side, sem, to):
        ref = wout.at[owner, pl.ds(side * o_rows, o_rows)]
        return remote(ref, ref, o_s.at[sem], o_r.at[sem], fs=to)

    loads[0].wait()
    for p in range(2):
        @pl.when(jnp.logical_and(z >= eager, z < n_sp - 1))
        def _():
            lift(z, 1, p).start()

        @pl.when(z > 0)
        def _():
            sink(z, 1, p).start()

    for k in range(5):
        loads[1 + k].wait()
    w_first = [send_w(fs, 0, 0, xn), send_w(fs, 1, 1, yn), send_w(fs, 1, 2, xn), send_w(fs, 0, 3, yn)]
    for copy in w_first:
        copy.start()
    for copy in loads[6:8]:
        copy.start()
    for p in range(2):
        across(z, p).start()
    loads[8].wait()

    @pl.when(z > 0)
    def _():
        sink_off(z, 1).start()

    @pl.when(z < eager)
    def _():
        pl.semaphore_wait(ready, 1)
        for p in range(2):
            lift(z, 1, p).start()

    @pl.when(z < n_sp - 1)
    def _():
        lift_off(z, 1).start()

    w_relay = [send_w(xn, 0, 4, yn), send_w(yn, 1, 5, xn)]
    w_here = [(0, xn, 0), (1, yn, 1), (2, xn, 1), (3, yn, 0), (4, dg, 0), (5, dg, 1)]
    o_first = []
    for q in range(3):
        o_first += [send_o(fs, 0, q, q, fs=xn), send_o(fs, 1, q, 4 + q, fs=yn)]
    o_later = [send_o(fs, 0, 3, 3, fs=xn), send_o(fs, 1, 3, 7, fs=yn), send_side(fs, 1, 8, xn), send_side(fs, 0, 9, yn)]
    o_relay = [(send_o(xn, 0, q, 10 + q, fs=yn), send_o(yn, 1, q, 13 + q, fs=xn)) for q in range(3)]
    o_share = [send_o(dg, side, 0, 16 + side, sp=mate) for side in range(2)]

    def relay_o(q):
        send_o(xn, 0, q, q, fs=xn).wait_recv()
        send_o(yn, 1, q, 4 + q, fs=xn).wait_recv()
        for copy in o_relay[q]:
            copy.start()

    def share_o():
        for side in range(2):
            send_o(dg, side, 0, 10 + 3 * side, fs=xn).wait_recv()
            o_share[side].start()

    def token_hop(dist, p):
        @pl.when(z >= dist)
        def _():
            block = (z - dist + n_sp) % n_sp
            lift(block, dist, p).wait_recv()
            if dist < n_sp - 1:
                @pl.when(z < n_sp - 1)
                def _():
                    lift(block, dist + 1, p).start()
            across(block, p).start()

        @pl.when(z + dist < n_sp)
        def _():
            block = (z + dist) % n_sp
            sink(block, dist, p).wait_recv()
            if dist < n_sp - 1:
                @pl.when(z > 0)
                def _():
                    sink(block, dist + 1, p).start()
            across(block, p).start()

    def offset_hop(dist):
        @pl.when(z >= dist)
        def _():
            block = (z - dist + n_sp) % n_sp
            lift_off(block, dist).wait_recv()
            if dist < n_sp - 1:
                @pl.when(z < n_sp - 1)
                def _():
                    lift_off(block, dist + 1).start()

        @pl.when(z + dist < n_sp)
        def _():
            block = (z + dist) % n_sp
            sink_off(block, dist).wait_recv()
            if dist < n_sp - 1:
                @pl.when(z > 0)
                def _():
                    sink_off(block, dist + 1).start()

    def relay_w():
        for s, owner, h in w_here[:2]:
            send_w(owner, h, s, xn).wait_recv()
            w_relay[s].start()
        for copy in loads[6:8]:
            copy.wait()
        for copy in o_first:
            copy.start()

    gated[pl.ds(0, 32), :] = jnp.zeros((32, width), F32)
    for dist in range(1, n_sp - 1):
        token_hop(dist, 0)
        offset_hop(dist)
        if dist == 1:
            relay_w()
        token_hop(dist, 1)
    if n_sp == 2:
        relay_w()
    for copy in loads[9:]:
        copy.wait()
    for s, owner, h in w_here[2:]:
        send_w(owner, h, s, xn).wait_recv()

    lane = lax.broadcasted_iota(jnp.int32, (rows, width), 1)

    def project(block, p):
        def spots(c):
            return c * rows + p * sub

        x = jnp.concatenate(
            [tok[aligned(block * blk + spots(c), sub), :] for c in range(n_tp)], axis=0
        ).astype(F32)
        normed = (x * lax.rsqrt(jnp.mean(x * x, axis=1, keepdims=True) + 1e-06) * gain[...]).astype(BF16)
        out = jnp.dot(normed, w[...], preferred_element_type=F32).astype(BF16)
        q = out[:, :width].astype(F32) * HD ** (-0.5)
        masked = [
            jnp.where(jnp.logical_and(lane >= h * HD, lane < (h + 1) * HD), q, 0.0).astype(BF16) for h in range(heads)
        ]
        value = out[:, 3 * width : 4 * width].astype(F32)
        gate = out[:, 4 * width :].astype(F32)
        fresh = (value * jax.nn.sigmoid(gate)).astype(BF16).astype(F32)
        for c in range(n_tp):
            part_of = slice(c * sub, (c + 1) * sub)
            at = aligned(block * blk + spots(c), sub)
            for h in range(heads):
                queries[block, aligned(h * blk + spots(c), sub), :] = masked[h][part_of]
            keys[at, :] = out[part_of, width : 2 * width]
            values[at, :] = out[part_of, 2 * width : 3 * width]
            gated[pl.ds(pl.multiple_of(block * blk + spots(c) + 32, 32), sub), :] = fresh[part_of]

    def convolve(tile, _):
        base = pl.multiple_of(tile * rows, rows)
        total = jnp.zeros((rows, width), F32)
        for phase in range(8):
            span = rows + 8 if phase else rows
            lined = jnp.zeros((span, width), F32)
            for tap in range((phase + taps - 33) % 8, taps, 8):
                lined = lined + ck[tap : tap + 1, :] * gated[pl.ds(base + (33 - taps + tap - phase), span), :]
            total = total + lined[phase : phase + rows]
        mean = jnp.mean(total, axis=1, keepdims=True)
        local = total - mean
        conv_out[pl.ds(base, rows), :] = local.astype(BF16)
        spread = jnp.mean(local * local, axis=1, keepdims=True)
        stats = jnp.transpose(jnp.where(lane % 2 == 0, mean, spread))[:8]
        pair = lax.broadcasted_iota(jnp.int32, (8, rows), 0) // 2
        stat_out[tile // tiles] = jnp.where(pair == tile % tiles, stats, stat_out[tile // tiles])
        return 0

    def block_rows(i):
        return aligned(i * blk, blk)


    def ship(k, source, block):
        at = source.at[block_rows(block)]

        @pl.when(block == z)
        def _():
            x_all[k * n_sp + z] = at[...]

        @pl.when(block != z)
        def _():
            remote(at, x_all.at[k * n_sp + z], x_s.at[k, block], x_r.at[k, z], sp=block).start()


    def ship_stat(block):
        at = stat_out.at[block]

        @pl.when(block == z)
        def _():
            stat_all[z] = at[...]

        @pl.when(block != z)
        def _():
            remote(at, stat_all.at[z], st_s.at[0, block], st_r.at[z], sp=block).start()

        remote(at, stat_all.at[n_sp + z], st_s.at[1, block], st_r.at[n_sp + z], sp=block, tp=1 - tp).start()

    wide = lax.broadcasted_iota(jnp.int32, (blk, width), 1)
    row = lax.broadcasted_iota(jnp.int32, (blk, blk), 0)
    col = lax.broadcasted_iota(jnp.int32, (blk, blk), 1)
    stacked = (heads, blk, blk)
    earlier = lax.broadcasted_iota(jnp.int32, stacked, 2) < lax.broadcasted_iota(jnp.int32, stacked, 1)
    earlier = earlier.reshape(heads * blk, blk)

    def attend(i, j, diagonal):
        k = keys[block_rows(j), :]
        v = values[block_rows(j), :]
        after = jnp.where(row >= col, 1.0, 0.0).astype(BF16)
        s = lax.dot_general(queries[i], k, (((1,), (1,)), ((), ())), preferred_element_type=F32)
        shift = jnp.concatenate(
            [jnp.broadcast_to(off[j, pl.ds(z * heads + h, 1), :], (blk, blk)) for h in range(heads)], axis=0
        )
        s = s * LOG2E + shift
        keep = jnp.minimum(-s, 0.0) - jnp.log2(1.0 + jnp.exp2(-jnp.abs(s)))
        if diagonal:
            keep = jnp.where(earlier, keep, 0.0)
        suffix = jnp.dot(keep.astype(BF16), after, preferred_element_type=F32)
        if diagonal:
            weights = jnp.where(earlier, jnp.exp2(s + suffix), 0.0)
            carry[i] = suffix[:, :1]
            running[i] = jnp.dot(weights.astype(BF16), v, preferred_element_type=F32)
        else:
            before = carry[i]
            weights = jnp.exp2(s + suffix + before)
            carry[i] = before + suffix[:, :1]
            running[i] += jnp.dot(weights.astype(BF16), v, preferred_element_type=F32)

        @pl.when(j == 0)
        def _():
            merged = running[i, :blk]
            for h in range(1, heads):
                merged = jnp.where(wide >= h * HD, running[i, h * blk : (h + 1) * blk], merged)
            attn_out[block_rows(i), :] = merged.astype(BF16)
            ship(0, attn_out, i)

    def step(s, _):
        rising = z < n_sp - 2
        block = jnp.where(rising, s, n_sp - 1 - s)

        def half_block(p, _):
            @pl.when(jnp.logical_and(s == n_sp - 1, edge))
            def _():
                @pl.when(p == 1)
                def _():
                    share_o()

                token_hop(n_sp - 1, p)

            from_partner(block, p).wait_recv()
            project(block, p)
            return 0

        lax.fori_loop(0, 2, half_block, 0)

        @pl.when(jnp.logical_and(s == n_sp - 1, edge))
        def _():
            offset_hop(n_sp - 1)

        off[block] = off_raw[block].astype(F32) * LOG2E

        @pl.when(s == n_sp - 3)
        def _():
            relay_o(0)
            for copy in o_later:
                copy.start()

        @pl.when(s == n_sp - 2)
        def _():
            for q in (1, 2):
                relay_o(q)

        @pl.when(jnp.logical_and(s == n_sp - 1, jnp.logical_not(edge)))
        def _():
            share_o()

        lax.fori_loop(block * tiles + 1, block * tiles + tiles, convolve, 0)

        def conv_block(u, _):
            target = jnp.where(rising, block, jnp.where(jnp.logical_and(u == 0, s > 0), block + 1, 0))
            convolve(target * tiles, 0)
            ship(1, conv_out, target)
            ship_stat(target)
            return 0

        falling_count = jnp.where(s > 0, 1, 0) + jnp.where(block == 0, 1, 0)
        lax.fori_loop(0, jnp.where(rising, 1, falling_count), conv_block, 0)
        whole = z < n_sp - 1

        def run(u, _):
            query = jnp.where(rising, block, jnp.where(whole, (n_sp - u) % n_sp, block))
            attend(query, query, True)

            def further(t, _):
                attend(jnp.where(whole, query, query + t), jnp.where(whole, query - t, query), False)
                return 0

            lax.fori_loop(1, jnp.where(whole, query, s) + 1, further, 0)
            return 0

        gathered = jnp.where(s == n_sp - 1, n_sp, 0)
        lax.fori_loop(0, jnp.where(z == n_sp - 2, gathered, 1), run, 0)
        return 0

    lax.fori_loop(0, n_sp, step, 0)


    others = [(z + d) % n_sp for d in range(1, n_sp)]

    def stat_from(slot):
        return remote(stat_all.at[slot], stat_all.at[slot], st_s.at[0, z], st_r.at[slot], tp=1 - tp)

    def x_from(k, source):
        ref = x_all.at[k * n_sp + source]
        return remote(ref, ref, x_s.at[k, z], x_r.at[k, source], tp=1 - tp)

    for source in others:
        stat_from(source).wait_recv()
    for source in range(n_sp):
        stat_from(n_sp + source).wait_recv()
    for source in others:
        x_from(1, source).wait_recv()
    kind = lax.broadcasted_iota(jnp.int32, (rows, n * 8), 1) % 8
    for t in range(tiles):
        stats = jnp.transpose(stat_all[...].reshape(n * 8, rows))
        mean = jnp.sum(jnp.where(kind == 2 * t, stats, 0.0), axis=1, keepdims=True) / n
        off_mean = stats - mean
        spread = jnp.where(kind == 2 * t, off_mean * off_mean, jnp.where(kind == 2 * t + 1, stats, 0.0))
        scale = lax.rsqrt(jnp.sum(spread, axis=1, keepdims=True) / n + 1e-06)
        at = pl.ds(t * rows, rows)
        for g in range(n_sp):
            x = x_all[n_sp + g, at, :].astype(F32) + off_mean[:, 8 * g + 2 * t : 8 * g + 2 * t + 1]
            y = x * scale * cgain[:, g * width : (g + 1) * width]
            hidden[at, (n_sp + g) * width : (n_sp + g + 1) * width] = (y * jax.nn.sigmoid(y)).astype(BF16)
    for source in others:
        x_from(0, source).wait_recv()
    for g in range(n_sp):
        hidden[:, g * width : (g + 1) * width] = x_all[g]

    sent = []
    for index, owner in enumerate((fs, xn, yn, dg)):
        if owner is xn:
            send_o(xn, 0, 3, 3, fs=xn).wait_recv()
            send_side(xn, 1, 8, xn).wait_recv()
        elif owner is yn:
            send_o(yn, 1, 3, 7, fs=xn).wait_recv()
            send_side(yn, 0, 9, xn).wait_recv()
        elif owner is dg:
            for side in range(2):
                for q in (1, 2):
                    send_o(dg, side, q, 10 + 3 * side + q, fs=xn).wait_recv()
                send_o(dg, side, 3, 16 + side, sp=mate).wait_recv()
        part[index] = jnp.dot(hidden[...], wout[owner], preferred_element_type=F32).astype(BF16)
        cols = aligned(owner * o_cols, o_cols)
        give = remote(
            part.at[index, aligned((1 - tp) * rows, rows)], got_out.at[:, cols],
            part_s.at[index], part_r.at[index], tp=1 - tp,
        )
        give.start()
        own_out[:, cols] = part[index, aligned(tp * rows, rows), :]
        sent.append(give)

    for copy in w_first + w_relay + o_first + o_later + o_share:
        copy.wait_send()
    for pair in o_relay:
        for copy in pair:
            copy.wait_send()
    for dist in range(1, n_sp):
        @pl.when(jnp.logical_and(z < n_sp - 1, z >= dist - 1))
        def _():
            lift_off(z, dist).wait_send()

        @pl.when(jnp.logical_and(z > 0, z + dist - 1 < n_sp))
        def _():
            sink_off(z, dist).wait_send()

    for p in range(2):
        for dist in range(1, n_sp):
            @pl.when(jnp.logical_and(z < n_sp - 1, z >= dist - 1))
            def _():
                lift(z, dist, p).wait_send()

            @pl.when(jnp.logical_and(z > 0, z + dist - 1 < n_sp))
            def _():
                sink(z, dist, p).wait_send()

        for block in range(n_sp):
            across(block, p).wait_send()
    for block in others:
        for k in range(2):
            remote(x_all.at[k], x_all.at[k], x_s.at[k, block], x_r.at[k, z], tp=1 - tp).wait_send()
        remote(stat_all.at[z], stat_all.at[z], st_s.at[0, block], st_r.at[z], tp=1 - tp).wait_send()
    for block in range(n_sp):
        remote(stat_all.at[z], stat_all.at[z], st_s.at[1, block], st_r.at[z], tp=1 - tp).wait_send()
    for copy in sent:
        copy.wait()


def layer_call(n_sp, n_fs, n_tp, width, heads, blk, tokens, gain, w_ins, off, ck, cgain, wa, wc):
    rows, features = tokens.shape
    depth = w_ins[0].shape[0]
    o_rows, o_cols = wa.shape
    length, n = rows * n_sp * n_tp, n_sp * n_tp
    tiles = blk // rows
    dma = pltpu.SemaphoreType.DMA
    vmem = pltpu.VMEM
    result = vmem((rows, n_fs * o_cols), BF16)
    return pl.pallas_call(
        functools.partial(layer_body, n_sp, n_tp, width, heads, ck.shape[0], blk),
        out_shape=[result, result],
        in_specs=[ANY] * 12,
        out_specs=[pl.BlockSpec(memory_space=pltpu.VMEM)] * 2,
        scratch_shapes=[
            vmem((length, features), BF16),
            vmem((n_fs * depth, 5 * width), BF16),
            vmem((n_fs, 2 * o_rows, o_cols), BF16),
            vmem((n_sp,) + off.shape, BF16),
            vmem((n_sp,) + off.shape, F32),
            vmem((ck.shape[0], width), F32),
            vmem(gain.shape, F32),
            vmem(cgain.shape, F32),
            vmem((n_sp, heads * blk, width), BF16),
            vmem((length, width), BF16),
            vmem((length, width), BF16),
            vmem((length + 32, width), F32),
            vmem((n_sp, heads * blk, 1), F32),
            vmem((n_sp, heads * blk, width), F32),
            vmem((length, width), BF16),
            vmem((length, width), BF16),
            vmem((n_sp, 8, rows), F32),
            vmem((2 * n_sp, blk, width), BF16),
            vmem((n, 8, rows), F32),
            vmem((blk, 2 * n_sp * width), BF16),
            vmem((n_fs, blk, o_cols), BF16),
            dma((12,)),
            dma((n_sp - 1, 2)), dma((n_sp - 1, 2)), dma((n_sp - 1, 2)), dma((n_sp - 1, 2)),
            dma((n_sp, 2)), dma((n_sp, 2)),
            dma((6,)), dma((6,)),
            dma((2, n_sp - 1)), dma((2, n_sp - 1)),
            dma((18,)), dma((18,)),
            dma((2, n_sp)), dma((2, n_sp)),
            dma((2, n_sp)), dma((n,)),
            dma((n_fs,)), dma((n_fs,)),
            pltpu.SemaphoreType.REGULAR,
        ],
        compiler_params=pltpu.CompilerParams(collective_id=0, has_side_effects=True),
        name="layer",
    )(tokens, gain, *w_ins, off, ck, cgain, wa, wc)


def spread_shards(
    tokens,
    norm_gain,
    w_query,
    w_key,
    w_value,
    w_conv_value,
    w_conv_gate,
    key_offset,
    conv_kernel,
    conv_gain,
    w_attn_out,
    w_conv_out,
):
    n_sp, n_fs, n_tp = (lax.axis_size(a) for a in ("sp", "fs", "tp"))
    width = w_query.shape[1] // n_sp
    own, got = layer_call(
        n_sp, n_fs, n_tp, width, width // HD, key_offset.shape[0], tokens[0], norm_gain[None],
        (w_query, w_key, w_value, w_conv_value, w_conv_gate), jnp.transpose(key_offset),
        conv_kernel, conv_gain[None], w_attn_out, w_conv_out,
    )
    return (own.astype(F32) + got.astype(F32)).astype(BF16)[None]


def shifted(block, axis, distance):
    devices = range(lax.axis_size(axis))
    route = [(i - distance, i) for i in devices if i - distance in devices]
    return lax.ppermute(block, axis, route)


def piece_terms(queries, key_rows, value_rows, offsets, carry_log, allowed):
    head_size = queries.shape[2]
    logits = jnp.einsum(
        "qhd,khd->hqk", queries, key_rows, preferred_element_type=jnp.float32
    ) * head_size ** (-0.5)
    logits = logits + jnp.transpose(offsets.astype(jnp.float32))[:, None, :]
    log_keep = jax.nn.log_sigmoid(-logits)
    if allowed is not None:
        log_keep = jnp.where(allowed[None], log_keep, 0.0)
    between = lax.cumsum(log_keep, axis=2, reverse=True) - log_keep
    weights = jnp.exp(jax.nn.log_sigmoid(logits) + between + carry_log[:, :, None])
    if allowed is not None:
        weights = jnp.where(allowed[None], weights, 0.0)
    result = jnp.einsum(
        "hqk,khd->qhd", weights.astype(jnp.bfloat16), value_rows, preferred_element_type=jnp.float32
    )
    return (result, carry_log + jnp.sum(log_keep, axis=2))


def shards(
    tokens,
    norm_gain,
    w_query,
    w_key,
    w_value,
    w_conv_value,
    w_conv_gate,
    key_offset,
    conv_kernel,
    conv_gain,
    w_attn_out,
    w_conv_out,
):
    gathered = (
        lax.all_gather(w_query, "fs", axis=0, tiled=True),
        lax.all_gather(w_key, "fs", axis=0, tiled=True),
        lax.all_gather(w_value, "fs", axis=0, tiled=True),
        lax.all_gather(w_conv_value, "fs", axis=0, tiled=True),
        lax.all_gather(w_conv_gate, "fs", axis=0, tiled=True),
    )
    floats = lax.all_gather(tokens[0], "tp", axis=0, tiled=True).astype(jnp.float32)
    normed = (
        floats * lax.rsqrt(jnp.mean(floats * floats, axis=1, keepdims=True) + 1e-06) * norm_gain
    ).astype(jnp.bfloat16)
    projected = jnp.concatenate(
        [
            jnp.dot(normed, weight, preferred_element_type=jnp.float32).astype(jnp.bfloat16)
            for weight in gathered
        ],
        axis=1,
    )
    head_cols = w_query.shape[1]
    channels = w_conv_value.shape[1]
    block_len = projected.shape[0]
    local_heads = head_cols // HD
    queries = projected[:, :head_cols].reshape(block_len, local_heads, HD)
    key_flat = projected[:, head_cols : 2 * head_cols]
    value_flat = projected[:, 2 * head_cols : 3 * head_cols]
    conv_value = projected[:, 3 * head_cols : 3 * head_cols + channels]
    conv_gate = projected[:, 3 * head_cols + channels :]
    position = lax.axis_index("sp")
    positions = jnp.arange(block_len, dtype=jnp.int32)
    causal = positions[None, :] < positions[:, None]
    start_log = jnp.zeros((local_heads, block_len), jnp.float32)
    totals, carry_log = piece_terms(
        queries,
        key_flat.reshape(block_len, local_heads, HD),
        value_flat.reshape(block_len, local_heads, HD),
        key_offset,
        start_log,
        causal,
    )

    def visit(hop_count, carried):
        running, running_log, moving = carried
        moving = shifted((moving[0], moving[1], moving[2]), "sp", 1)
        result, next_log = piece_terms(
            queries,
            moving[0].reshape(block_len, local_heads, HD),
            moving[1].reshape(block_len, local_heads, HD),
            moving[2],
            running_log,
            None,
        )
        active = position >= hop_count
        running = jnp.where(active, running + result, running)
        running_log = jnp.where(active, next_log, running_log)
        return (running, running_log, moving)

    totals, carry_log, leftover = lax.fori_loop(
        1, lax.axis_size("sp"), visit, (totals, carry_log, (key_flat, value_flat, key_offset))
    )
    attn_heads = totals.reshape(block_len, head_cols).astype(jnp.bfloat16)
    gated_input = (
        conv_value.astype(jnp.float32) * jax.nn.sigmoid(conv_gate.astype(jnp.float32))
    ).astype(jnp.bfloat16)
    kernel_len = conv_kernel.shape[0]
    edge_rows = shifted(gated_input[block_len - (kernel_len - 1) :], "sp", 1)
    extended = jnp.concatenate([edge_rows, gated_input], axis=0).astype(jnp.float32)
    conv_sum = jnp.zeros((block_len, channels), jnp.float32)
    for tap_index in range(kernel_len):
        conv_sum = conv_sum + conv_kernel[tap_index] * extended[tap_index : tap_index + block_len]
    channel_total = lax.psum(jnp.sum(conv_sum, axis=1), "tp")
    centred = conv_sum - (channel_total / CC)[:, None]
    spread = lax.psum(jnp.sum(centred * centred, axis=1), "tp") / CC
    conv_hidden = jax.nn.silu(centred * lax.rsqrt(spread + 1e-06)[:, None] * conv_gain).astype(
        jnp.bfloat16
    )
    attn_weight, conv_weight = (
        lax.all_gather(w_attn_out, "fs", axis=1, tiled=True),
        lax.all_gather(w_conv_out, "fs", axis=1, tiled=True),
    )
    partial_value = jnp.dot(attn_heads, attn_weight, preferred_element_type=jnp.float32)
    partial_value = partial_value + jnp.dot(
        conv_hidden, conv_weight, preferred_element_type=jnp.float32
    )
    mixed = lax.psum_scatter(
        lax.optimization_barrier(partial_value.astype(jnp.bfloat16))
        .astype(jnp.float32)
        .astype(jnp.bfloat16),
        "tp",
        scatter_dimension=0,
        tiled=True,
    )
    return mixed[None]


def solution(mesh):
    placed = (
        P("fs", ("sp", "tp"), None),
        P(),
        P("fs", "tp"),
        P("fs", "tp"),
        P("fs", "tp"),
        P("fs", "tp"),
        P("fs", "tp"),
        P("sp", "tp"),
        P(None, "tp"),
        P("tp"),
        P("tp", "fs"),
        P("tp", "fs"),
    )

    def fits(tokens, norm_gain, w_query, *rest):
        n_sp, n_fs, n_tp = mesh.shape["sp"], mesh.shape["fs"], mesh.shape["tp"]
        cols = w_query.shape[1] // n_tp
        return n_fs == 4 and n_tp == 2 and n_sp == 4 and rest[5].shape[0] <= 33 and cols % (128 * n_sp) == 0 and rest[2].shape[1] == w_query.shape[1] and (
            tokens.shape[1] % (128 * n_sp * n_tp) == 0
        )

    def program(*args):
        body = spread_shards if fits(*args) else shards
        return mapped(body)(*args)

    def mapped(body):
        return jax.shard_map(
            body, mesh=mesh, in_specs=placed, out_specs=P("fs", ("sp", "tp"), None), check_vma=False
        )

    return program
```
